512 devices in a mesh: sp: 32 (over z, core), tp: 16 (over y, x).
Axes of the slice: x: 4, y: 4, z: 16, core: 2. Of those that a mesh axis runs over, the one named last changes fastest.
Arguments:
- residual_in: bfloat16 [4096, 2048], P('sp'), may hold values from -6 to 6
- queries: bfloat16 [4096, 2048], P('sp', 'tp'), may hold values from -6 to 6
- keys: bfloat16 [4096, 2048], P('sp', 'tp'), may hold values from -6 to 6
- values: bfloat16 [4096, 2048], P('sp', 'tp'), may hold values from -6 to 6
- out_gate: bfloat16 [4096, 2048], P('sp', 'tp'), may hold values from -6 to 6
- beta_logit: bfloat16 [16, 4096], P('tp', 'sp'), may hold values from -6 to -2
- decay_logit: bfloat16 [16, 4096], P('tp', 'sp'), may hold values from -4.5 to 4.5
- decay_log: float32 [16], P('tp'), may hold values from -11 to -3.2
- head_gain: float32 [128], replicated, may hold values from 0.1 to 1.9
- out_weight: bfloat16 [2048, 2048], P('tp'), may hold values from -0.125 to 0.125
- norm_gain: float32 [2048], replicated, may hold values from 0.1 to 1.9
- final_gain: float32 [2048], replicated, may hold values from 0.1 to 1.9
- expert_index: int32 [4096, 2], P('sp'), may hold values from 0 to 31, all different within a row; in each aligned block of 8 rows (0 to 7, 8 to 15, ...) no two rows name the same one
- route_weights: float32 [4096, 2], P('sp'), may hold values from 0.2 to 1
- expert_gate: bfloat16 [32, 2048, 6144], P('sp', None, 'tp'), may hold values from -0.125 to 0.125
- expert_up: bfloat16 [32, 2048, 6144], P('sp', None, 'tp'), may hold values from -0.125 to 0.125
- expert_down: bfloat16 [32, 6144, 2048], P('sp', 'tp'), may hold values from -0.078125 to 0.078125
Outputs:
- layer_out: bfloat16 [4096, 2048], P('sp')
The draws below stay inside these ranges and needn't reach their ends.
Inputs may be any that keep to these rules, and one draw needn't show every extreme that they name: `expert_index`: in each aligned block of 8 rows no expert is named by more than 1 row, a bound that some block reaches; a row names 2 different experts.
All inputs are finite; a program needn't handle non-finite values.
Results may differ from the reference program's by a relative error of at most 0.015.
Values may be sent and summed in bfloat16 or wider, within the bound.
No kernel may reach another device: no remote copies, remote signals or barrier semaphores. Data moves between devices by JAX's collectives and lax.ppermute only.
A program may use at most 64 MiB of HBM per device.

```python
import math
import jax
import jax.numpy as jnp
import numpy as np
from jax import lax

D = 2048
HEADS = 16
HEAD_FEATURES = 128
FF = 6144
TOP = 2
BLOCK = 64
TOKENS = 4096
EXPERTS = 32
ROWS_TP = 8
CAP = 1
N_SP = 32
N_TP = 16


def draw_decay_logit(key, part):
    noise_key, level_key = jax.random.split(key)
    noise = jax.random.truncated_normal(noise_key, -3.0, 3.0, (HEADS, TOKENS), jnp.float32)
    levels = jax.random.uniform(level_key, (HEADS, TOKENS // 128), jnp.float32, -1.5, 1.5)
    return (noise + jnp.repeat(levels, 128, axis=1)).astype(jnp.bfloat16)


def draw_decay_log(key, part):
    pick_key, slow_key, fast_key = jax.random.split(key, 3)
    share = 0.5
    slow = jax.random.uniform(pick_key, (HEADS,), jnp.float32) < share
    slow_value = jax.random.uniform(slow_key, (HEADS,), jnp.float32, -11.0, -9.5)
    fast_value = jax.random.uniform(fast_key, (HEADS,), jnp.float32, -4.2, -3.2)
    return jnp.where(slow, slow_value, fast_value)


def steps_of(own_key, dims, cuts, smallest, top_value):
    def one(position, shards_of):
        steps = jax.random.uniform(jax.random.fold_in(jax.random.fold_in(own_key, 6), position), (shards_of,), jnp.float32, smallest / len(cuts), top_value / len(cuts))
        return jnp.repeat(jnp.exp(steps), dims[position] // shards_of).reshape((-1,) + (1,) * (len(dims) - position - 1))

    factor_of = one(*cuts[0])
    for cut in cuts[1:]:
        factor_of = factor_of * one(*cut)
    return factor_of


def deal_out(rng, own, number, rows, number_of, top, reach, slope):
    sequence = jax.random.permutation(rng, number_of)
    crowded, ordinary = shares(number_of, rows * top, reach, slope, True), shares(number_of, rows * top, reach, slope, False)
    places = jnp.arange(number_of)

    def named(sizes, turn):
        used = int((sizes > 0).sum())
        fixed = max(1, used // 4)
        shifted = fixed + (places - fixed + turn * (used - fixed)) % max(1, number_of - fixed)
        return jnp.zeros((number_of,), jnp.int32).at[sequence[jnp.where(places < fixed, places, shifted)]].set(jnp.asarray(sizes, jnp.int32))

    sizes = jnp.where(number % 4 == 0, named(crowded, number // 4), named(ordinary, number - number // 4 - 1))
    mixed = jax.random.permutation(jax.random.fold_in(own, 3), number_of)
    donor, receiver = mixed[0:number_of // 2 * 2:2], mixed[1:number_of // 2 * 2:2]
    room = jnp.minimum(sizes[donor] - 1, reach - sizes[receiver]) // 2
    room = jnp.where((donor == sequence[0]) | (receiver == sequence[0]) | (sizes[receiver] == 0), 0, jnp.maximum(room, 0))
    shifted = jax.random.randint(jax.random.fold_in(own, 4), (number_of // 2,), 0, 1 << 20) % (room + 1)
    sizes = sizes.at[donor].add(-shifted).at[receiver].add(shifted)
    items = jnp.searchsorted(jnp.cumsum(sizes), jnp.arange(rows * top), side="right").astype(jnp.int32)
    table = items.reshape(top, rows).T
    table = table[jax.random.permutation(jax.random.fold_in(own, 1), rows)]
    turn = jax.random.randint(jax.random.fold_in(own, 2), (rows, 1), 0, top)
    return jnp.take_along_axis(table, (jnp.arange(top)[None, :] + turn) % top, axis=1)


def shares(count, total, bound, slope, full):
    weights = [(1 << 20) // math.isqrt(standing ** slope) + 1 for standing in range(1, count + 1)]
    largest = bound if full else min(bound, max(-(-total // count), total * weights[0] // sum(weights)))
    least = 1 if total - largest >= count - 1 else 0
    holding, surplus = [largest] + [least] * (count - 1), total - largest - least * (count - 1)
    while surplus > 0:
        candidates = [i for i in range(1, count) if holding[i] < largest] or [i for i in range(1, count) if holding[i] < bound]
        whole, budget = sum([weights[i] for i in candidates]), surplus
        for i in candidates:
            extra = min(bound - holding[i], max(1, budget * weights[i] // whole), surplus)
            holding[i] = holding[i] + extra
            surplus = surplus - extra
    return np.array(holding)


def scatter_about(rng, shape, scale, reach, pieces=(), kind=jnp.bfloat16):
    array = jax.random.normal(rng, shape, jnp.float32) * scale
    if len(pieces) > 0:
        array = steps_of(rng, shape, pieces, -0.22, 0.18) * array
    return jnp.clip(array, min=-reach, max=reach).astype(kind)


def setup_inputs(seed: int = 0) -> dict:
    splits = jax.random.split(jax.random.key(seed), 18)
    residual_in = scatter_about(splits[0], (TOKENS, D), 1.0, 6.0, ((0, 32),))
    queries = scatter_about(splits[1], (TOKENS, HEADS * HEAD_FEATURES), 1.0, 6.0, ((0, 32), (1, 16)))
    keys = scatter_about(splits[2], (TOKENS, HEADS * HEAD_FEATURES), 1.0, 6.0, ((0, 32), (1, 16)))
    values = scatter_about(splits[3], (TOKENS, HEADS * HEAD_FEATURES), 1.0, 6.0, ((0, 32), (1, 16)))
    out_gate = scatter_about(splits[4], (TOKENS, HEADS * HEAD_FEATURES), 1.0, 6.0, ((0, 32), (1, 16)))
    beta_logit = jnp.clip(-6.0 + 4.0 * jax.random.uniform(splits[5], (HEADS, TOKENS), jnp.float32) ** steps_of(splits[5], (HEADS, TOKENS), ((0, 16), (1, 32)), -0.2, 0.2), -6.0, -2.0).astype(jnp.bfloat16)
    decay_logit = draw_decay_logit(jax.random.fold_in(splits[17], 71), 0)
    decay_log = draw_decay_log(jax.random.fold_in(splits[17], 71), 0)
    head_gain = jnp.clip(1.0 + 0.18 * jax.random.normal(splits[8], (HEAD_FEATURES,), jnp.float32), 0.1, 1.9)
    out_weight = scatter_about(splits[9], (HEADS * HEAD_FEATURES, D), (HEADS * HEAD_FEATURES) ** -0.5, 0.125, ((0, 16),))
    norm_gain = jnp.clip(1.0 + 0.18 * jax.random.normal(splits[10], (D,), jnp.float32), 0.1, 1.9)
    final_gain = jnp.clip(1.0 + 0.18 * jax.random.normal(splits[11], (D,), jnp.float32), 0.1, 1.9)
    expert_index_keys = jax.random.split(jax.random.fold_in(splits[12], 1), TOKENS // ROWS_TP)
    expert_index_turns = jax.random.permutation(jax.random.fold_in(splits[12], 3), TOKENS // ROWS_TP)
    expert_index = jax.vmap(lambda own, number: deal_out(jax.random.fold_in(splits[12], 2), own, number, ROWS_TP, EXPERTS, TOP, CAP, 1))(expert_index_keys, expert_index_turns).reshape((TOKENS, TOP))
    route_weights = jnp.clip(0.2 + 0.8 * jax.random.uniform(splits[13], (TOKENS, TOP), jnp.float32) ** steps_of(splits[13], (TOKENS, TOP), ((0, 32),), -0.2, 0.2), 0.2, 1.0)
    expert_gate = scatter_about(splits[14], (EXPERTS, D, FF), D ** -0.5, 0.125, ((0, 32), (2, 16)))
    expert_up = scatter_about(splits[15], (EXPERTS, D, FF), D ** -0.5, 0.125, ((0, 32), (2, 16)))
    expert_down = scatter_about(splits[16], (EXPERTS, FF, D), FF ** -0.5, 0.078125, ((0, 32), (1, 16)))
    return dict(residual_in=residual_in, queries=queries, keys=keys, values=values, out_gate=out_gate, beta_logit=beta_logit, decay_logit=decay_logit, decay_log=decay_log, head_gain=head_gain, out_weight=out_weight, norm_gain=norm_gain, final_gain=final_gain, expert_index=expert_index, route_weights=route_weights, expert_gate=expert_gate, expert_up=expert_up, expert_down=expert_down)


highest_precision = lax.Precision.HIGHEST
residual_scale = 2.0 ** 0.5

def unit_rows(data):
    return data * lax.rsqrt(lax.optimization_barrier(jnp.sum(data * data, -1, keepdims=True)) + 1e-06)

def layer_norm(data, gain):
    center = data - lax.optimization_barrier(jnp.mean(data, -1, keepdims=True))
    return center * lax.rsqrt(lax.optimization_barrier(jnp.mean(center * center, -1, keepdims=True)) + 1e-05) * gain

def rounded(data):
    return lax.optimization_barrier(data.astype(jnp.bfloat16)).astype(jnp.float32)

def delta_blocks(query, key, value, beta, decay):
    heads, length, width = query.shape
    count = length // BLOCK
    shape = (heads, count, BLOCK, width)
    query = query.reshape(shape)
    key = key.reshape(shape)
    value = value.reshape(shape)
    beta = beta.reshape(heads, count, BLOCK)
    running = jnp.cumsum(decay.reshape(heads, count, BLOCK), axis=-1)
    causal = jnp.tril(jnp.ones((BLOCK, BLOCK), bool))
    strict = jnp.tril(jnp.ones((BLOCK, BLOCK), bool), -1)
    within = jnp.exp(jnp.where(causal, running[..., :, None] - running[..., None, :], -jnp.inf))
    key_beta = key * beta[..., None]
    lower = jnp.where(strict, jnp.einsum('hnid,hnjd->hnij', key_beta, key, precision=highest_precision) * within, 0.0)
    system = jnp.eye(BLOCK, dtype=jnp.float32) + lower
    fresh = jax.scipy.linalg.solve_triangular(system, value * beta[..., None], lower=True, unit_diagonal=True)
    weighted = jax.scipy.linalg.solve_triangular(system, key_beta * jnp.exp(running)[..., None], lower=True, unit_diagonal=True)
    scores = jnp.einsum('hnid,hnjd->hnij', query, key, precision=highest_precision) * within
    query_decayed = query * jnp.exp(running)[..., None]
    key_decayed = key * jnp.exp(running[..., -1:] - running)[..., None]
    block_decay = jnp.exp(running[..., -1])

    def advance(recurrent_state, inputs):
        fresh_value_block, block_weighted_values, block_queries, block_keys, block_scores, block_decay_factor = inputs
        corrected_value = fresh_value_block - jnp.einsum('nya,nag->nyg', block_weighted_values, recurrent_state, precision=highest_precision)
        final_output = jnp.einsum('nya,nag->nyg', block_queries, recurrent_state, precision=highest_precision) + jnp.einsum('emp,epk->emk', block_scores, corrected_value, precision=highest_precision)
        recurrent_state = block_decay_factor[:, None, None] * recurrent_state + jnp.einsum('iyp,iyu->ipu', block_keys, corrected_value, precision=highest_precision)
        return (recurrent_state, final_output)
    start = jnp.zeros((heads, width, width), jnp.float32)
    inputs = tuple((jnp.moveaxis(item, 1, 0) for item in (fresh, weighted, query_decayed, key_decayed, scores, block_decay)))
    _, output_list = lax.scan(advance, start, inputs)
    return jnp.moveaxis(output_list, 0, 1).reshape(heads, length, width)

def reference(residual_in, queries, keys, values, out_gate, beta_logit, decay_logit, decay_log, head_gain, out_weight, norm_gain, final_gain, expert_index, route_weights, expert_gate, expert_up, expert_down):
    length, width = residual_in.shape
    heads = beta_logit.shape[0]

    def split_heads(data):
        return data.astype(jnp.float32).reshape(length, heads, HEAD_FEATURES).transpose(1, 0, 2)
    query = unit_rows(split_heads(queries)) * HEAD_FEATURES ** (-0.5)
    key = unit_rows(split_heads(keys))
    value = split_heads(values)
    beta = jax.nn.sigmoid(beta_logit.astype(jnp.float32))
    decay = -jnp.exp(decay_log)[:, None] * jax.nn.softplus(decay_logit.astype(jnp.float32))
    mixed = delta_blocks(query, key, value, beta, decay)
    normalized = mixed * lax.rsqrt(lax.optimization_barrier(jnp.mean(mixed * mixed, -1, keepdims=True)) + 1e-06) * head_gain
    gated = (normalized * jax.nn.silu(split_heads(out_gate))).transpose(1, 0, 2).reshape(length, heads * HEAD_FEATURES).astype(jnp.bfloat16)
    group = heads * HEAD_FEATURES // N_TP
    projected = jnp.zeros((length, width), jnp.float32)
    for index in range(N_TP):
        projected = projected + rounded(jnp.dot(gated[:, index * group:(index + 1) * group].astype(jnp.float32), out_weight[index * group:(index + 1) * group].astype(jnp.float32), preferred_element_type=jnp.float32))
    hidden_in = layer_norm(residual_scale * residual_in.astype(jnp.float32) + projected, norm_gain).astype(jnp.bfloat16)
    total = length * TOP
    flat = expert_index.reshape(total).astype(jnp.int32)
    largest = N_SP * N_TP * CAP
    slice_width = FF // N_TP

    def one_expert(inputs):
        index, gate_matrix, up_matrix, down_matrix = inputs
        positions = jnp.nonzero(flat == index, size=largest, fill_value=total)[0].astype(jnp.int32)
        rows = hidden_in[jnp.minimum(positions, total - 1) // TOP]
        gate = jnp.dot(rows.astype(jnp.float32), gate_matrix.astype(jnp.float32), preferred_element_type=jnp.float32)
        up = jnp.dot(rows.astype(jnp.float32), up_matrix.astype(jnp.float32), preferred_element_type=jnp.float32)
        inner = (jax.nn.silu(gate) * up).astype(jnp.bfloat16)
        summed = jnp.zeros((largest, width), jnp.float32)
        for part in range(N_TP):
            summed = summed + rounded(jnp.dot(inner[:, part * slice_width:(part + 1) * slice_width].astype(jnp.float32), down_matrix[part * slice_width:(part + 1) * slice_width].astype(jnp.float32), preferred_element_type=jnp.float32))
        return (summed.astype(jnp.bfloat16), positions)
    output_list, positions = lax.map(one_expert, (jnp.arange(EXPERTS, dtype=jnp.int32), expert_gate, expert_up, expert_down))
    placed = jnp.zeros((total + 1, width), jnp.bfloat16).at[positions.reshape(-1)].set(output_list.reshape(-1, width))
    chosen = placed[:total].reshape(length, TOP, width).astype(jnp.float32)
    routed = lax.optimization_barrier(jnp.sum(route_weights[..., None] * chosen, 1))
    return layer_norm(residual_scale * hidden_in.astype(jnp.float32) + routed, final_gain).astype(jnp.bfloat16)
```

```python
import jax
import jax.numpy as jnp
from jax import lax
from jax.sharding import Mesh
from jax.sharding import PartitionSpec as P

HEAD_FEATURES = 128
TOP = 2
BLOCK = 64
Z = ("zh", "zl")
SP = ("zh", "zl", "c")
PLANE = ("c", "tp")


highest_precision = lax.Precision.HIGHEST
residual_scale = 2.0**0.5


def mm(a, b):
    return jnp.dot(a, b, precision=highest_precision)


def entering(map_here, state_here):
    kind = jnp.bfloat16
    zh, zl, c = (lax.axis_index(axis) for axis in SP)
    own = jnp.concatenate([map_here, state_here], 0).astype(kind)
    near = lax.all_gather(own, ("zl", "c")).astype(jnp.float32)
    width = map_here.shape[-1]
    map_in, state_in = (jnp.eye(width, dtype=jnp.float32), jnp.zeros((width, width), jnp.float32))
    map_all, state_all = (near[0, :width], near[0, width:])
    for k in range(1, 4):
        inside = k == 2 * zl + c
        map_in = jnp.where(inside, map_all, map_in)
        state_in = jnp.where(inside, state_all, state_in)
        map_k, state_k = (near[k, :width], near[k, width:])
        state_all = mm(map_k, state_all) + state_k
        map_all = mm(map_k, map_all)
    group = jnp.concatenate([map_all, state_all], 0).astype(kind)
    quarter = lax.dynamic_slice_in_dim(group, (2 * zl + c) * (width // 2), width // 2, 0)
    count = lax.axis_size(Z)
    far = lax.all_to_all(jnp.broadcast_to(quarter[None], (count, *quarter.shape)), Z, 0, 0, tiled=True)
    far = lax.all_gather(far, "c")
    far = far.reshape(2, count // 2, 2, width // 2, width).transpose(1, 2, 0, 3, 4)
    far = far.reshape(count // 2, 2 * width, width).astype(jnp.float32)
    state = jnp.zeros((width, width), jnp.float32)
    for k in range(count // 2 - 1):
        state = jnp.where(k < zh, mm(far[k, :width], state) + far[k, width:], state)
    return mm(map_in, state) + state_in


def in_blocks(x, dim, length):
    shape = x.shape
    blocks = x.reshape(*shape[:dim], length, shape[dim] // length, *shape[dim + 1 :])
    return jnp.moveaxis(blocks, dim, 0)


def sum_at_owner(x, axis, dim):
    length = lax.axis_size(axis)
    blocks = lax.all_to_all(in_blocks(x, dim, length), axis, 0, 0, tiled=True)
    return jnp.sum(blocks.astype(jnp.float32), axis=0)


def copy_for_each(x, axis):
    length = lax.axis_size(axis)
    return lax.all_to_all(jnp.broadcast_to(x[None], (length, *x.shape)), axis, 0, 0, tiled=True)


def in_order(blocks, dim):
    shape = list(blocks.shape[1:])
    shape[dim] *= blocks.shape[0]
    return jnp.moveaxis(blocks, 0, dim).reshape(shape)


def collect(x, axis, dim):
    blocks = copy_for_each(x, axis)
    return in_order(blocks, dim)


def unit_rows(data):
    return data * lax.rsqrt(jnp.sum(data * data, -1, keepdims=True) + 1e-06)


def layer_norm(data, gain):
    center = data - jnp.mean(data, -1, keepdims=True)
    return center * lax.rsqrt(jnp.mean(center * center, -1, keepdims=True) + 1e-05) * gain


def block_terms(query, key, beta, decay):
    heads, length, width = query.shape
    count = length // BLOCK
    shape = (heads, count, BLOCK, width)
    query = query.reshape(shape)
    key = key.reshape(shape)
    beta = beta.reshape(heads, count, BLOCK)
    running = jnp.cumsum(decay.reshape(heads, count, BLOCK), axis=-1)
    causal = jnp.tril(jnp.ones((BLOCK, BLOCK), bool))
    strict = jnp.tril(jnp.ones((BLOCK, BLOCK), bool), -1)
    within = jnp.exp(jnp.where(causal, running[..., :, None] - running[..., None, :], -jnp.inf))
    key_beta = key * beta[..., None]
    lower = jnp.where(
        strict,
        jnp.einsum("hnid,hnjd->hnij", key_beta, key, precision=highest_precision) * within,
        0.0,
    )
    system = jnp.eye(BLOCK, dtype=jnp.float32) + lower
    weighted = jax.scipy.linalg.solve_triangular(
        system, key_beta * jnp.exp(running)[..., None], lower=True, unit_diagonal=True
    )
    scores = jnp.einsum("hnid,hnjd->hnij", query, key, precision=highest_precision) * within
    query_decayed = query * jnp.exp(running)[..., None]
    key_decayed = key * jnp.exp(running[..., -1:] - running)[..., None]
    block_decay = jnp.exp(running[..., -1])
    return (system, beta, weighted, query_decayed, key_decayed, scores, block_decay)


def run_blocks(terms, value, start):
    system, beta, weighted, query_decayed, key_decayed, scores, block_decay = terms
    heads, count = (beta.shape[0], beta.shape[1])
    fresh = jax.scipy.linalg.solve_triangular(
        system,
        value.reshape(heads, count, BLOCK, -1) * beta[..., None],
        lower=True,
        unit_diagonal=True,
    )
    missing = start.shape[-1] - fresh.shape[-1]
    fresh = jnp.concatenate([fresh, jnp.zeros(fresh.shape[:-1] + (missing,), jnp.float32)], -1)

    def advance(recurrent_state, inputs):
        (
            fresh_value_block,
            block_weighted_values,
            block_queries,
            block_keys,
            block_scores,
            block_decay_factor,
        ) = inputs
        corrected_value = fresh_value_block - jnp.einsum(
            "nya,nag->nyg", block_weighted_values, recurrent_state, precision=highest_precision
        )
        state_next = block_decay_factor[:, None, None] * recurrent_state + jnp.einsum(
            "iyp,iyu->ipu", block_keys, corrected_value, precision=highest_precision
        )
        final_output = jnp.einsum(
            "nya,nag->nyg", block_queries, recurrent_state, precision=highest_precision
        ) + jnp.einsum("emp,epk->emk", block_scores, corrected_value, precision=highest_precision)
        return (state_next, final_output)

    inputs = tuple(
        (
            jnp.moveaxis(item, 1, 0)
            for item in (fresh, weighted, query_decayed, key_decayed, scores, block_decay)
        )
    )
    final, output_list = lax.scan(advance, start, inputs)
    return (jnp.moveaxis(output_list, 0, 1).reshape(heads, count * BLOCK, -1), final)


def per_device(
    residual_in,
    queries,
    keys,
    values,
    out_gate,
    beta_logit,
    decay_logit,
    decay_log,
    head_gain,
    out_weight,
    norm_gain,
    final_gain,
    expert_index,
    route_weights,
    expert_gate,
    expert_up,
    expert_down,
):
    length, width = residual_in.shape
    heads = beta_logit.shape[0]

    def split_heads(data):
        return data.astype(jnp.float32).reshape(length, heads, HEAD_FEATURES).transpose(1, 0, 2)

    query = unit_rows(split_heads(queries)) * HEAD_FEATURES ** (-0.5)
    key = unit_rows(split_heads(keys))
    value = split_heads(values)
    beta = jax.nn.sigmoid(beta_logit.astype(jnp.float32))
    decay = -jnp.exp(decay_log)[:, None] * jax.nn.softplus(decay_logit.astype(jnp.float32))
    terms = block_terms(query, key, beta, decay)
    identity_map = jnp.broadcast_to(
        jnp.eye(HEAD_FEATURES, dtype=jnp.float32), (heads, HEAD_FEATURES, HEAD_FEATURES)
    )
    blank = jnp.zeros((heads, HEAD_FEATURES, HEAD_FEATURES), jnp.float32)
    extended = jnp.concatenate([blank, identity_map], -1)
    output_list, final = run_blocks(terms, value, extended)
    entry_value = entering(final[0, :, HEAD_FEATURES:], final[0, :, :HEAD_FEATURES])[None]
    mixed = output_list[..., :HEAD_FEATURES] + jnp.einsum(
        "apj,ajz->apz", output_list[..., HEAD_FEATURES:], entry_value, precision=highest_precision
    )
    normalized = mixed * lax.rsqrt(jnp.mean(mixed * mixed, -1, keepdims=True) + 1e-06) * head_gain
    gated = (
        (normalized * jax.nn.silu(split_heads(out_gate)))
        .transpose(1, 0, 2)
        .reshape(length, heads * HEAD_FEATURES)
        .astype(jnp.bfloat16)
    )
    split_count = lax.axis_size("tp")
    expert_count = lax.axis_size(SP) * expert_gate.shape[0]
    rows = length // split_count
    first = lax.axis_index("tp") * rows
    projected = sum_at_owner(
        jnp.dot(gated, out_weight, preferred_element_type=jnp.float32).astype(jnp.bfloat16), "tp", 0
    )
    residual = lax.dynamic_slice_in_dim(residual_in, first, rows, 0)
    routes = lax.dynamic_slice_in_dim(expert_index, first, rows, 0)
    weights = lax.dynamic_slice_in_dim(route_weights, first, rows, 0)
    hidden_in = layer_norm(
        residual_scale * residual.astype(jnp.float32) + projected, norm_gain
    ).astype(jnp.bfloat16)
    chips = lax.axis_size(Z)
    table = (routes[:, :, None] == jnp.arange(expert_count, dtype=jnp.int32)).astype(jnp.bfloat16)
    send = jnp.einsum(
        "rs,rd->sd", jnp.sum(table, 1), hidden_in, preferred_element_type=jnp.float32
    ).astype(jnp.bfloat16)

    def along_z(x):
        out = lax.all_to_all(x.reshape(chips, 16, width // 8), Z, 0, 0, tiled=True)
        return out.reshape(chips, 2, width)

    def in_plane(x):
        return lax.all_to_all(x, PLANE, 0, 0, tiled=True)

    arrived = along_z(send).transpose(1, 0, 2)
    arrived = jnp.broadcast_to(arrived[:, None], (2, split_count, chips, width))
    piece = in_plane(arrived.reshape(2 * split_count, chips, width)).reshape(-1, width)
    gate_matrix, up_matrix, down_matrix = (expert_gate[0], expert_up[0], expert_down[0])
    gate = jnp.dot(piece, gate_matrix, preferred_element_type=jnp.float32)
    up = jnp.dot(piece, up_matrix, preferred_element_type=jnp.float32)
    inner = (jax.nn.silu(gate) * up).astype(jnp.bfloat16)
    partial_value = jnp.dot(inner, down_matrix, preferred_element_type=jnp.float32)
    parts = in_plane(partial_value.astype(jnp.bfloat16).reshape(2 * split_count, chips, width))
    parts = parts.reshape(2, split_count, chips, width)
    result = jnp.sum(parts.astype(jnp.float32), axis=1).astype(jnp.bfloat16)
    back = along_z(result.transpose(1, 0, 2)).reshape(expert_count, width)
    gathered = jnp.einsum("rks,sd->rkd", table, back, preferred_element_type=jnp.float32)
    routed = jnp.sum(weights[..., None] * gathered, 1)
    layer_out = layer_norm(
        residual_scale * hidden_in.astype(jnp.float32) + routed, final_gain
    ).astype(jnp.bfloat16)
    layer_out = collect(layer_out, "tp", 0)
    return layer_out


def solution(mesh):
    split = Mesh(
        mesh.devices.reshape(8, 2, 2, mesh.shape["tp"]), ("zh", "zl", "c", "tp")
    )
    placed = (
        P(SP, None),
        P(SP, "tp"),
        P(SP, "tp"),
        P(SP, "tp"),
        P(SP, "tp"),
        P("tp", SP),
        P("tp", SP),
        P("tp"),
        P(),
        P("tp", None),
        P(),
        P(),
        P(SP, None),
        P(SP, None),
        P(SP, None, "tp"),
        P(SP, None, "tp"),
        P(SP, "tp", None),
    )
    return jax.shard_map(
        per_device, mesh=split, in_specs=placed, out_specs=P(SP, None), check_vma=False
    )
```

```python
import jax
import jax.numpy as jnp
from jax import lax
from jax.experimental import pallas as pl
from jax.experimental.pallas import tpu as pltpu
from jax.sharding import Mesh
from jax.sharding import PartitionSpec as P

HEAD_FEATURES = 128
TOP = 2
Z = ("zh", "zl")
SP = ("zh", "zl", "c")
PLANE = ("c", "tp")


highest_precision = lax.Precision.HIGHEST
residual_scale = 2.0**0.5


def mm(a, b):
    return jnp.dot(a, b, precision=highest_precision)


def entering(own):
    kind = jnp.bfloat16
    zh, zl, c = (lax.axis_index(axis) for axis in SP)
    near = lax.all_gather(own, ("zl", "c")).astype(jnp.float32)
    width = own.shape[-1]
    map_in, state_in = (jnp.eye(width, dtype=jnp.float32), jnp.zeros((width, width), jnp.float32))
    map_all, state_all = (near[0, :width], near[0, width:])
    for k in range(1, 4):
        inside = k == 2 * zl + c
        map_in = jnp.where(inside, map_all, map_in)
        state_in = jnp.where(inside, state_all, state_in)
        map_k, state_k = (near[k, :width], near[k, width:])
        state_all = mm(map_k, state_all) + state_k
        map_all = mm(map_k, map_all)
    group = jnp.concatenate([map_all, state_all], 0).astype(kind)
    quarter = lax.dynamic_slice_in_dim(group, (2 * zl + c) * (width // 2), width // 2, 0)
    count = lax.axis_size(Z)
    far = lax.all_to_all(jnp.broadcast_to(quarter[None], (count, *quarter.shape)), Z, 0, 0, tiled=True)
    far = lax.all_gather(far, "c")
    far = far.reshape(2, count // 2, 2, width // 2, width).transpose(1, 2, 0, 3, 4)
    far = far.reshape(count // 2, 2 * width, width).astype(jnp.float32)
    state = jnp.zeros((width, width), jnp.float32)
    for k in range(count // 2 - 1):
        state = jnp.where(k < zh, mm(far[k, :width], state) + far[k, width:], state)
    return mm(map_in, state) + state_in


def in_blocks(x, dim, length):
    shape = x.shape
    blocks = x.reshape(*shape[:dim], length, shape[dim] // length, *shape[dim + 1 :])
    return jnp.moveaxis(blocks, dim, 0)


def sum_at_owner(x, axis, dim):
    length = lax.axis_size(axis)
    blocks = lax.all_to_all(in_blocks(x, dim, length), axis, 0, 0, tiled=True)
    return jnp.sum(blocks.astype(jnp.float32), axis=0)


def copy_for_each(x, axis):
    length = lax.axis_size(axis)
    return lax.all_to_all(jnp.broadcast_to(x[None], (length, *x.shape)), axis, 0, 0, tiled=True)


def in_order(blocks, dim):
    shape = list(blocks.shape[1:])
    shape[dim] *= blocks.shape[0]
    return jnp.moveaxis(blocks, 0, dim).reshape(shape)


def collect(x, axis, dim):
    blocks = copy_for_each(x, axis)
    return in_order(blocks, dim)


def layer_norm(data, gain):
    center = data - jnp.mean(data, -1, keepdims=True)
    return center * lax.rsqrt(jnp.mean(center * center, -1, keepdims=True) + 1e-05) * gain


def local_span(q_ref, k_ref, v_ref, beta_ref, decay_ref, rate_ref, both_ref, mix_ref, out_ref):
    size = HEAD_FEATURES
    row = lax.broadcasted_iota(jnp.int32, (size, size), 0)
    col = lax.broadcasted_iota(jnp.int32, (size, size), 1)
    eye = row == col
    causal = col <= row

    def to_column(data):
        return jnp.sum(jnp.where(eye, data, 0.0), 1, keepdims=True)

    def to_row(data):
        return jnp.sum(jnp.where(eye, data, 0.0), 0, keepdims=True)

    def dot(a, b, dims=((1,), (0,))):
        return lax.dot_general(
            a.astype(jnp.bfloat16),
            b.astype(jnp.bfloat16),
            (dims, ((), ())),
            preferred_element_type=jnp.float32,
        )

    beta = to_column(jax.nn.sigmoid(beta_ref[...].astype(jnp.float32)))
    logit = decay_ref[...].astype(jnp.float32)
    softplus = jnp.maximum(logit, 0.0) + jnp.log(1.0 + jnp.exp(-jnp.abs(logit)))
    decay = -jnp.exp(jnp.full((1, size), rate_ref[0], jnp.float32)) * softplus
    running = jnp.sum(jnp.where(causal, decay, 0.0), 1, keepdims=True)
    last = jnp.sum(decay, 1, keepdims=True)
    within = jnp.exp(jnp.where(causal, running - to_row(running), -1e30))
    query = q_ref[...].astype(jnp.float32)
    key = k_ref[...].astype(jnp.float32)
    value = v_ref[...].astype(jnp.float32)
    query_scale = lax.rsqrt(jnp.sum(query * query, 1, keepdims=True) + 1e-06) * size ** (-0.5)
    key_scale = lax.rsqrt(jnp.sum(key * key, 1, keepdims=True) + 1e-06)
    key_scale_row = to_row(key_scale)
    across = within * key_scale_row
    lower = jnp.where(
        col < row, dot(k_ref[...], k_ref[...], ((1,), (1,))) * across * (beta * key_scale), 0.0
    )
    scores = dot(q_ref[...], k_ref[...], ((1,), (1,))) * across * query_scale
    differ = row ^ col
    inverse = jnp.where(eye, 1.0, 0.0) - jnp.where(differ == 1, lower, 0.0)
    for level in range(1, 7):
        part = jnp.where((differ >> level) == 1, lower, 0.0)
        inverse = inverse - dot(dot(inverse, part), inverse)
    grown = jnp.exp(running)
    key = key * key_scale
    right = jnp.concatenate([key * (beta * grown), value * beta], 1)
    solved = dot(inverse, right)
    leaving = dot(key * jnp.exp(last - running), solved, ((0,), (0,)))
    passed = jnp.where(eye, jnp.exp(last), 0.0) - leaving[:, :size]
    both_ref[...] = jnp.concatenate([passed, leaving[:, size:]], 0).astype(both_ref.dtype)
    seen = dot(scores, solved)
    mix_ref[...] = query * (query_scale * grown) - seen[:, :size]
    out_ref[...] = seen[:, size:]


def per_device(
    residual_in,
    queries,
    keys,
    values,
    out_gate,
    beta_logit,
    decay_logit,
    decay_log,
    head_gain,
    out_weight,
    norm_gain,
    final_gain,
    expert_index,
    route_weights,
    expert_gate,
    expert_up,
    expert_down,
):
    length, width = residual_in.shape

    vmem = pl.BlockSpec(memory_space=pltpu.VMEM)
    both, mix, local = pl.pallas_call(
        local_span,
        out_shape=(
            jax.ShapeDtypeStruct((2 * HEAD_FEATURES, HEAD_FEATURES), jnp.bfloat16),
            jax.ShapeDtypeStruct((length, HEAD_FEATURES), jnp.float32),
            jax.ShapeDtypeStruct((length, HEAD_FEATURES), jnp.float32),
        ),
        in_specs=[vmem] * 5 + [pl.BlockSpec(memory_space=pltpu.SMEM)],
        out_specs=(vmem,) * 3,
        name="local_span",
    )(queries, keys, values, beta_logit, decay_logit, decay_log)
    mixed = local + mm(mix, entering(both))
    normalized = mixed * lax.rsqrt(jnp.mean(mixed * mixed, -1, keepdims=True) + 1e-06) * head_gain
    gated = (normalized * jax.nn.silu(out_gate.astype(jnp.float32))).astype(jnp.bfloat16)
    split_count = lax.axis_size("tp")
    expert_count = lax.axis_size(SP) * expert_gate.shape[0]
    rows = length // split_count
    first = lax.axis_index("tp") * rows
    projected = sum_at_owner(
        jnp.dot(gated, out_weight, preferred_element_type=jnp.float32).astype(jnp.bfloat16), "tp", 0
    )
    residual = lax.dynamic_slice_in_dim(residual_in, first, rows, 0)
    routes = lax.dynamic_slice_in_dim(expert_index, first, rows, 0)
    weights = lax.dynamic_slice_in_dim(route_weights, first, rows, 0)
    hidden_in = layer_norm(
        residual_scale * residual.astype(jnp.float32) + projected, norm_gain
    ).astype(jnp.bfloat16)
    chips = lax.axis_size(Z)
    table = (routes[:, :, None] == jnp.arange(expert_count, dtype=jnp.int32)).astype(jnp.bfloat16)
    send = jnp.einsum(
        "rs,rd->sd", jnp.sum(table, 1), hidden_in, preferred_element_type=jnp.float32
    ).astype(jnp.bfloat16)

    def along_z(x):
        out = lax.all_to_all(x.reshape(chips, 16, width // 8), Z, 0, 0, tiled=True)
        return out.reshape(chips, 2, width)

    def in_plane(x):
        return lax.all_to_all(x, PLANE, 0, 0, tiled=True)

    arrived = along_z(send).transpose(1, 0, 2)
    arrived = jnp.broadcast_to(arrived[:, None], (2, split_count, chips, width))
    piece = in_plane(arrived.reshape(2 * split_count, chips, width)).reshape(-1, width)
    gate_matrix, up_matrix, down_matrix = (expert_gate[0], expert_up[0], expert_down[0])
    gate = jnp.dot(piece, gate_matrix, preferred_element_type=jnp.float32)
    up = jnp.dot(piece, up_matrix, preferred_element_type=jnp.float32)
    inner = (jax.nn.silu(gate) * up).astype(jnp.bfloat16)
    partial_value = jnp.dot(inner, down_matrix, preferred_element_type=jnp.float32)
    parts = in_plane(partial_value.astype(jnp.bfloat16).reshape(2 * split_count, chips, width))
    parts = parts.reshape(2, split_count, chips, width)
    result = jnp.sum(parts.astype(jnp.float32), axis=1).astype(jnp.bfloat16)
    back = along_z(result.transpose(1, 0, 2)).reshape(expert_count, width)
    gathered = jnp.einsum("rks,sd->rkd", table, back, preferred_element_type=jnp.float32)
    routed = jnp.sum(weights[..., None] * gathered, 1)
    layer_out = layer_norm(
        residual_scale * hidden_in.astype(jnp.float32) + routed, final_gain
    ).astype(jnp.bfloat16)
    layer_out = collect(layer_out, "tp", 0)
    return layer_out


def solution(mesh):
    split = Mesh(
        mesh.devices.reshape(8, 2, 2, mesh.shape["tp"]), ("zh", "zl", "c", "tp")
    )
    placed = (
        P(SP, None),
        P(SP, "tp"),
        P(SP, "tp"),
        P(SP, "tp"),
        P(SP, "tp"),
        P("tp", SP),
        P("tp", SP),
        P("tp"),
        P(),
        P("tp", None),
        P(),
        P(),
        P(SP, None),
        P(SP, None),
        P(SP, None, "tp"),
        P(SP, None, "tp"),
        P(SP, "tp", None),
    )
    return jax.shard_map(
        per_device, mesh=split, in_specs=placed, out_specs=P(SP, None), check_vma=False
    )
```

```python
import jax
import jax.numpy as jnp
from jax import lax
from jax.experimental import pallas as pl
from jax.experimental.pallas import tpu as pltpu
from jax.sharding import Mesh
from jax.sharding import PartitionSpec as P


HEAD_FEATURES = 128
Z = ("zh", "zl")
SP = ("zh", "zl", "c")
PLANE = ("c", "tp")


highest_precision = lax.Precision.HIGHEST
residual_scale = 2.0**0.5


def held(x):
    return pltpu.with_memory_space_constraint(x, pltpu.VMEM)


def mm(a, b):
    return jnp.dot(a, b, precision=highest_precision)


def pack_thirds(gate_ref, up_ref, down_ref, first_ref, second_ref, third_ref, sems):
    share = down_ref.shape[0] // 3
    copies = []
    for part, ref in enumerate((first_ref, second_ref, third_ref)):
        cut = pl.ds(part * share, share)
        moves = [(gate_ref.at[:, cut], ref.at[:, pl.ds(0, share)])]
        moves.append((up_ref.at[:, cut], ref.at[:, pl.ds(share, share)]))
        for k in range(0, ref.shape[0], share):
            source = down_ref.at[cut, pl.ds(k, share)]
            moves.append((source, ref.at[pl.ds(k, share), pl.ds(2 * share, share)]))
        copies += moves
    copies = [pltpu.make_async_copy(x, y, sems.at[k]) for k, (x, y) in enumerate(copies)]
    for copy in copies:
        copy.start()
    for copy in copies:
        copy.wait()


def spread(gate, up, down, side):
    width, share = gate.shape
    share //= 3
    packed = jax.ShapeDtypeStruct((width, 3 * share), gate.dtype)
    anywhere = pl.BlockSpec(memory_space=pl.ANY)
    thirds = pl.pallas_call(
        pack_thirds,
        out_shape=(packed,) * 3,
        in_specs=[anywhere] * 3,
        out_specs=(anywhere,) * 3,
        scratch_shapes=[pltpu.SemaphoreType.DMA((3 * (2 + width // share),))],
        name="pack_thirds",
    )(gate, up, down)
    out = []
    for third, (dy, dx) in zip(thirds, ((0, 1), (0, side - 1), (1, 0))):
        pairs = [
            (y * side + x, (y + dy) % side * side + (x + dx) % side)
            for y in range(side)
            for x in range(side)
        ]
        out.append(lax.ppermute(third, "tp", pairs))
    return out


def entering(own, weights, side):
    kind = jnp.bfloat16
    zh, zl, c = (lax.axis_index(axis) for axis in SP)
    near = lax.all_gather(own, ("zl", "c")).astype(jnp.float32)
    width = own.shape[-1]
    map_in, state_in = (jnp.eye(width, dtype=jnp.float32), jnp.zeros((width, width), jnp.float32))
    map_all, state_all = (near[0, :width], near[0, width:])
    for k in range(1, 4):
        inside = k == 2 * zl + c
        map_in = jnp.where(inside, map_all, map_in)
        state_in = jnp.where(inside, state_all, state_in)
        map_k, state_k = (near[k, :width], near[k, width:])
        state_all = mm(map_k, state_all) + state_k
        map_all = mm(map_k, map_all)
    group = jnp.concatenate([map_all, state_all], 0).astype(kind)
    quarter = lax.dynamic_slice_in_dim(group, (2 * zl + c) * (width // 2), width // 2, 0)
    count = lax.axis_size(Z)
    quarter, weights = lax.optimization_barrier((quarter, weights))
    thirds = spread(*weights, side)
    far = jnp.broadcast_to(quarter[None], (count, *quarter.shape))
    far = lax.all_to_all(far, Z, 0, 0, tiled=True)
    far = lax.all_gather(far, "c")
    far = far.reshape(2, count // 2, 2, width // 2, width).transpose(1, 2, 0, 3, 4)
    far = far.reshape(count // 2, 2 * width, width).astype(jnp.float32)
    state = jnp.zeros((width, width), jnp.float32)
    for k in range(count // 2 - 1):
        state = jnp.where(k < zh, mm(far[k, :width], state) + far[k, width:], state)
    return mm(map_in, state) + state_in, thirds


def in_blocks(x, dim, length):
    shape = x.shape
    blocks = x.reshape(*shape[:dim], length, shape[dim] // length, *shape[dim + 1 :])
    return jnp.moveaxis(blocks, dim, 0)


def sum_at_owner(x, axis, dim):
    length = lax.axis_size(axis)
    blocks = lax.all_to_all(in_blocks(x, dim, length), axis, 0, 0, tiled=True)
    return jnp.sum(blocks.astype(jnp.float32), axis=0)


def copy_for_each(x, axis):
    length = lax.axis_size(axis)
    return lax.all_to_all(jnp.broadcast_to(x[None], (length, *x.shape)), axis, 0, 0, tiled=True)


def in_order(blocks, dim):
    shape = list(blocks.shape[1:])
    shape[dim] *= blocks.shape[0]
    return jnp.moveaxis(blocks, 0, dim).reshape(shape)


def collect(x, axis, dim):
    blocks = copy_for_each(x, axis)
    return in_order(blocks, dim)


def layer_norm(data, gain):
    center = data - jnp.mean(data, -1, keepdims=True)
    return center * lax.rsqrt(jnp.mean(center * center, -1, keepdims=True) + 1e-05) * gain


def local_span(q_ref, k_ref, v_ref, beta_ref, decay_ref, rate_ref, both_ref, mix_ref, out_ref):
    size = HEAD_FEATURES
    row = lax.broadcasted_iota(jnp.int32, (size, size), 0)
    col = lax.broadcasted_iota(jnp.int32, (size, size), 1)
    eye = row == col
    causal = col <= row

    def to_column(data):
        return jnp.sum(jnp.where(eye, data, 0.0), 1, keepdims=True)

    def to_row(data):
        return jnp.sum(jnp.where(eye, data, 0.0), 0, keepdims=True)

    def dot(a, b, dims=((1,), (0,))):
        return lax.dot_general(
            a.astype(jnp.bfloat16),
            b.astype(jnp.bfloat16),
            (dims, ((), ())),
            preferred_element_type=jnp.float32,
        )

    beta = to_column(jax.nn.sigmoid(beta_ref[...].astype(jnp.float32)))
    logit = decay_ref[...].astype(jnp.float32)
    softplus = jnp.maximum(logit, 0.0) + jnp.log(1.0 + jnp.exp(-jnp.abs(logit)))
    decay = -jnp.exp(jnp.full((1, size), rate_ref[0], jnp.float32)) * softplus
    running = jnp.sum(jnp.where(causal, decay, 0.0), 1, keepdims=True)
    last = jnp.sum(decay, 1, keepdims=True)
    within = jnp.exp(jnp.where(causal, running - to_row(running), -1e30))
    query = q_ref[...].astype(jnp.float32)
    key = k_ref[...].astype(jnp.float32)
    value = v_ref[...].astype(jnp.float32)
    query_scale = lax.rsqrt(jnp.sum(query * query, 1, keepdims=True) + 1e-06) * size ** (-0.5)
    key_scale = lax.rsqrt(jnp.sum(key * key, 1, keepdims=True) + 1e-06)
    key_scale_row = to_row(key_scale)
    across = within * key_scale_row
    lower = jnp.where(
        col < row, dot(k_ref[...], k_ref[...], ((1,), (1,))) * across * (beta * key_scale), 0.0
    )
    scores = dot(q_ref[...], k_ref[...], ((1,), (1,))) * across * query_scale
    differ = row ^ col
    inverse = jnp.where(eye, 1.0, 0.0) - jnp.where(differ == 1, lower, 0.0)
    for level in range(1, 7):
        part = jnp.where((differ >> level) == 1, lower, 0.0)
        inverse = inverse - dot(dot(inverse, part), inverse)
    grown = jnp.exp(running)
    key = key * key_scale
    right = jnp.concatenate([key * (beta * grown), value * beta], 1)
    solved = dot(inverse, right)
    leaving = dot(key * jnp.exp(last - running), solved, ((0,), (0,)))
    passed = jnp.where(eye, jnp.exp(last), 0.0) - leaving[:, :size]
    both_ref[...] = jnp.concatenate([passed, leaving[:, size:]], 0).astype(both_ref.dtype)
    seen = dot(scores, solved)
    mix_ref[...] = query * (query_scale * grown) - seen[:, :size]
    out_ref[...] = seen[:, size:]


def run_experts(rows_ref, *refs):
    out_ref, bufs, sems = refs[6], refs[7:13], refs[13]
    copies = [pltpu.make_async_copy(refs[k], bufs[k], sems.at[k]) for k in range(6)]
    for copy in copies:
        copy.start()
    gate_ref, up_ref, down_ref = bufs[:3]
    rows = rows_ref[...]
    share = bufs[3].shape[1] // 3

    def dot(a, b):
        return jnp.dot(a, b, preferred_element_type=jnp.float32)

    copies[0].wait()
    gate = dot(rows, gate_ref[...])
    copies[1].wait()
    inner = (jax.nn.silu(gate) * dot(rows, up_ref[...])).astype(jnp.bfloat16)
    copies[2].wait()
    total = dot(inner, down_ref[...])
    for copy, ref in zip(copies[3:], bufs[3:]):
        copy.wait()
        both = dot(rows, ref[:, : 2 * share])
        inner = (jax.nn.silu(both[:, :share]) * both[:, share:]).astype(jnp.bfloat16)
        down = [ref[k : k + share, 2 * share :] for k in range(0, ref.shape[0], share)]
        total = total + dot(inner, jnp.concatenate(down, 1))
    out_ref[...] = total.astype(out_ref.dtype)


def per_device(
    residual_in,
    queries,
    keys,
    values,
    out_gate,
    beta_logit,
    decay_logit,
    decay_log,
    head_gain,
    out_weight,
    norm_gain,
    final_gain,
    expert_index,
    route_weights,
    expert_gate,
    expert_up,
    expert_down,
):
    length, width = residual_in.shape

    vmem = pl.BlockSpec(memory_space=pltpu.VMEM)
    both, mix, local = pl.pallas_call(
        local_span,
        out_shape=(
            pltpu.VMEM((2 * HEAD_FEATURES, HEAD_FEATURES), jnp.bfloat16),
            pltpu.VMEM((length, HEAD_FEATURES), jnp.float32),
            pltpu.VMEM((length, HEAD_FEATURES), jnp.float32),
        ),
        in_specs=[vmem] * 5 + [pl.BlockSpec(memory_space=pltpu.SMEM)],
        out_specs=(vmem,) * 3,
        name="local_span",
    )(queries, keys, values, beta_logit, decay_logit, decay_log)
    split_count = lax.axis_size("tp")
    side = round(split_count**0.5)
    gate_matrix, up_matrix, down_matrix = (expert_gate[0], expert_up[0], expert_down[0])
    state, thirds = entering(both, (gate_matrix, up_matrix, down_matrix), side)
    mixed = local + mm(mix, state)
    normalized = mixed * lax.rsqrt(jnp.mean(mixed * mixed, -1, keepdims=True) + 1e-06) * head_gain
    gated = (normalized * jax.nn.silu(out_gate.astype(jnp.float32))).astype(jnp.bfloat16)
    expert_count = lax.axis_size(SP) * expert_gate.shape[0]
    rows = length // split_count
    first = lax.axis_index("tp") * rows
    projected = sum_at_owner(
        jnp.dot(gated, out_weight, preferred_element_type=jnp.float32).astype(jnp.bfloat16), "tp", 0
    )
    residual = lax.dynamic_slice_in_dim(residual_in, first, rows, 0)
    routes = lax.dynamic_slice_in_dim(expert_index, first, rows, 0)
    weights = lax.dynamic_slice_in_dim(route_weights, first, rows, 0)
    hidden_in = layer_norm(
        residual_scale * residual.astype(jnp.float32) + projected, norm_gain
    ).astype(jnp.bfloat16)
    chips = lax.axis_size(Z)
    table = (routes[:, :, None] == jnp.arange(expert_count, dtype=jnp.int32)).astype(jnp.bfloat16)
    send = jnp.einsum(
        "rs,rd->sd", jnp.sum(table, 1), hidden_in, preferred_element_type=jnp.float32
    ).astype(jnp.bfloat16)

    def along_z(x):
        out = lax.all_to_all(x.reshape(chips, 16, width // 8), Z, 0, 0, tiled=True)
        return out.reshape(chips, 2, width)

    def in_plane(x):
        return lax.all_to_all(x, PLANE, 0, 0, tiled=True)

    half = chips // 2
    arrived = along_z(send).transpose(1, 0, 2).reshape(2, 2, half, width)
    swapped = arrived[:, ::-1]
    turns = jnp.stack([arrived, swapped], 1)[:, None, :, None]
    turns = jnp.broadcast_to(turns, (2, side // 2, 2, side // 2, 2, half, width))
    piece = in_plane(turns.reshape(2 * split_count, half, width)).reshape(-1, width)
    tables = (gate_matrix, up_matrix, down_matrix, *thirds)
    partial_value = pl.pallas_call(
        run_experts,
        out_shape=pltpu.VMEM(piece.shape, jnp.bfloat16),
        in_specs=[vmem] + [pl.BlockSpec(memory_space=pl.ANY)] * 6,
        out_specs=vmem,
        scratch_shapes=[pltpu.VMEM(x.shape, x.dtype) for x in tables]
        + [pltpu.SemaphoreType.DMA((6,))],
        name="run_experts",
    )(held(piece), *tables)
    parts = in_plane(partial_value.reshape(2 * split_count, half, width))
    parts = parts.reshape(2, side // 2, 2, side // 2, 2, half, width).astype(jnp.float32)
    parts = jnp.sum(parts, axis=(1, 3))
    result = jnp.stack([parts[:, 0, 0] + parts[:, 1, 1], parts[:, 0, 1] + parts[:, 1, 0]], 1)
    result = result.reshape(2, chips, width).astype(jnp.bfloat16)
    back = along_z(result.transpose(1, 0, 2)).reshape(expert_count, width)
    gathered = jnp.einsum("rks,sd->rkd", table, back, preferred_element_type=jnp.float32)
    routed = jnp.sum(weights[..., None] * gathered, 1)
    layer_out = layer_norm(
        residual_scale * hidden_in.astype(jnp.float32) + routed, final_gain
    ).astype(jnp.bfloat16)
    layer_out = collect(layer_out, "tp", 0)
    return layer_out


def solution(mesh):
    split = Mesh(
        mesh.devices.reshape(8, 2, 2, mesh.shape["tp"]), ("zh", "zl", "c", "tp")
    )
    placed = (
        P(SP, None),
        P(SP, "tp"),
        P(SP, "tp"),
        P(SP, "tp"),
        P(SP, "tp"),
        P("tp", SP),
        P("tp", SP),
        P("tp"),
        P(),
        P("tp", None),
        P(),
        P(),
        P(SP, None),
        P(SP, None),
        P(SP, None, "tp"),
        P(SP, None, "tp"),
        P(SP, "tp", None),
    )

    return jax.shard_map(per_device, mesh=split, in_specs=placed, out_specs=P(SP, None), check_vma=False)
```

```python
import jax
import jax.numpy as jnp
from jax import lax
from jax.experimental import pallas as pl
from jax.experimental.pallas import tpu as pltpu
from jax.sharding import Mesh
from jax.sharding import PartitionSpec as P


HEAD_FEATURES = 128
Z = ("zh", "zl")
SP = ("zh", "zl", "c")
PLANE = ("c", "tp")


highest_precision = lax.Precision.HIGHEST
residual_scale = 2.0**0.5


def held(x):
    return pltpu.with_memory_space_constraint(x, pltpu.VMEM)


def mm(a, b):
    return jnp.dot(a, b, precision=highest_precision)


def pack_thirds(gate_ref, up_ref, down_ref, *refs):
    outs, bufs, sems = refs[:3], refs[3:6], refs[6]
    copies = [
        pltpu.make_async_copy(x, y, sems.at[k])
        for k, (x, y) in enumerate(zip((gate_ref, up_ref, down_ref), bufs))
    ]
    for copy in copies:
        copy.start()
    share = down_ref.shape[0] // 3
    for kind, (copy, buf) in enumerate(zip(copies, bufs)):
        copy.wait()
        for part, out in enumerate(outs):
            cut = slice(part * share, (part + 1) * share)
            rows = slice(kind * share, (kind + 1) * share)
            if kind == 2:
                out[rows] = buf[cut]
            else:
                for k in range(0, buf.shape[0], share):
                    out[rows, k : k + share] = buf[k : k + share, cut]


def spread(gate, up, down, side):
    packed = jax.ShapeDtypeStruct(down.shape, down.dtype)
    thirds = pl.pallas_call(
        pack_thirds,
        out_shape=(packed,) * 3,
        in_specs=[pl.BlockSpec(memory_space=pl.ANY)] * 3,
        out_specs=(pl.BlockSpec(memory_space=pltpu.VMEM),) * 3,
        scratch_shapes=[pltpu.VMEM(x.shape, x.dtype) for x in (gate, up, down)]
        + [pltpu.SemaphoreType.DMA((3,))],
        name="pack_thirds",
    )(gate, up, down)
    out = []
    for third, (dy, dx) in zip(thirds, ((0, 1), (0, side - 1), (1, 0))):
        pairs = [
            (y * side + x, (y + dy) % side * side + (x + dx) % side)
            for y in range(side)
            for x in range(side)
        ]
        out.append(lax.ppermute(third, "tp", pairs))
    return out


def entering(own, weights, side):
    kind = jnp.bfloat16
    zh, zl, c = (lax.axis_index(axis) for axis in SP)
    near = lax.all_gather(own, ("zl", "c")).astype(jnp.float32)
    width = own.shape[-1]
    map_in, state_in = (jnp.eye(width, dtype=jnp.float32), jnp.zeros((width, width), jnp.float32))
    map_all, state_all = (near[0, :width], near[0, width:])
    for k in range(1, 4):
        inside = k == 2 * zl + c
        map_in = jnp.where(inside, map_all, map_in)
        state_in = jnp.where(inside, state_all, state_in)
        map_k, state_k = (near[k, :width], near[k, width:])
        state_all = mm(map_k, state_all) + state_k
        map_all = mm(map_k, map_all)
    group = jnp.concatenate([map_all, state_all], 0).astype(kind)
    quarter = lax.dynamic_slice_in_dim(group, (2 * zl + c) * (width // 2), width // 2, 0)
    count = lax.axis_size(Z)
    quarter, weights = lax.optimization_barrier((quarter, weights))
    thirds = spread(*weights, side)
    far = jnp.broadcast_to(quarter[None], (count, *quarter.shape))
    far = lax.all_to_all(far, Z, 0, 0, tiled=True)
    far = lax.all_gather(far, "c")
    far = far.reshape(2, count // 2, 2, width // 2, width).transpose(1, 2, 0, 3, 4)
    far = far.reshape(count // 2, 2 * width, width).astype(jnp.float32)
    state = jnp.zeros((width, width), jnp.float32)
    for k in range(count // 2 - 1):
        state = jnp.where(k < zh, mm(far[k, :width], state) + far[k, width:], state)
    return mm(map_in, state) + state_in, thirds


def in_blocks(x, dim, length):
    shape = x.shape
    blocks = x.reshape(*shape[:dim], length, shape[dim] // length, *shape[dim + 1 :])
    return jnp.moveaxis(blocks, dim, 0)


def sum_at_owner(x, axis, dim):
    length = lax.axis_size(axis)
    blocks = lax.all_to_all(in_blocks(x, dim, length), axis, 0, 0, tiled=True)
    return jnp.sum(blocks.astype(jnp.float32), axis=0)


def copy_for_each(x, axis):
    length = lax.axis_size(axis)
    return lax.all_to_all(jnp.broadcast_to(x[None], (length, *x.shape)), axis, 0, 0, tiled=True)


def in_order(blocks, dim):
    shape = list(blocks.shape[1:])
    shape[dim] *= blocks.shape[0]
    return jnp.moveaxis(blocks, 0, dim).reshape(shape)


def collect(x, axis, dim):
    blocks = copy_for_each(x, axis)
    return in_order(blocks, dim)


def layer_norm(data, gain):
    center = data - jnp.mean(data, -1, keepdims=True)
    return center * lax.rsqrt(jnp.mean(center * center, -1, keepdims=True) + 1e-05) * gain


def local_span(q_ref, k_ref, v_ref, beta_ref, decay_ref, rate_ref, both_ref, mix_ref, out_ref):
    size = HEAD_FEATURES
    row = lax.broadcasted_iota(jnp.int32, (size, size), 0)
    col = lax.broadcasted_iota(jnp.int32, (size, size), 1)
    eye = row == col
    causal = col <= row

    def to_column(data):
        return jnp.sum(jnp.where(eye, data, 0.0), 1, keepdims=True)

    def to_row(data):
        return jnp.sum(jnp.where(eye, data, 0.0), 0, keepdims=True)

    def dot(a, b, dims=((1,), (0,))):
        return lax.dot_general(
            a.astype(jnp.bfloat16),
            b.astype(jnp.bfloat16),
            (dims, ((), ())),
            preferred_element_type=jnp.float32,
        )

    beta = to_column(jax.nn.sigmoid(beta_ref[...].astype(jnp.float32)))
    logit = decay_ref[...].astype(jnp.float32)
    softplus = jnp.maximum(logit, 0.0) + jnp.log(1.0 + jnp.exp(-jnp.abs(logit)))
    decay = -jnp.exp(jnp.full((1, size), rate_ref[0], jnp.float32)) * softplus
    running = jnp.sum(jnp.where(causal, decay, 0.0), 1, keepdims=True)
    last = jnp.sum(decay, 1, keepdims=True)
    within = jnp.exp(jnp.where(causal, running - to_row(running), -1e30))
    query = q_ref[...].astype(jnp.float32)
    key = k_ref[...].astype(jnp.float32)
    value = v_ref[...].astype(jnp.float32)
    query_scale = lax.rsqrt(jnp.sum(query * query, 1, keepdims=True) + 1e-06) * size ** (-0.5)
    key_scale = lax.rsqrt(jnp.sum(key * key, 1, keepdims=True) + 1e-06)
    key_scale_row = to_row(key_scale)
    across = within * key_scale_row
    lower = jnp.where(
        col < row, dot(k_ref[...], k_ref[...], ((1,), (1,))) * across * (beta * key_scale), 0.0
    )
    scores = dot(q_ref[...], k_ref[...], ((1,), (1,))) * across * query_scale
    differ = row ^ col
    inverse = jnp.where(eye, 1.0, 0.0) - jnp.where(differ == 1, lower, 0.0)
    for level in range(1, 7):
        part = jnp.where((differ >> level) == 1, lower, 0.0)
        inverse = inverse - dot(dot(inverse, part), inverse)
    grown = jnp.exp(running)
    key = key * key_scale
    right = jnp.concatenate([key * (beta * grown), value * beta], 1)
    solved = dot(inverse, right)
    leaving = dot(key * jnp.exp(last - running), solved, ((0,), (0,)))
    passed = jnp.where(eye, jnp.exp(last), 0.0) - leaving[:, :size]
    both_ref[...] = jnp.concatenate([passed, leaving[:, size:]], 0).astype(both_ref.dtype)
    seen = dot(scores, solved)
    mix_ref[...] = query * (query_scale * grown) - seen[:, :size]
    out_ref[...] = seen[:, size:]


def run_experts(rows_ref, *refs):
    out_ref, bufs, sems = refs[6], refs[7:13], refs[13]
    copies = [pltpu.make_async_copy(refs[k], bufs[k], sems.at[k]) for k in range(6)]
    for copy in copies:
        copy.start()
    gate_ref, up_ref, down_ref = bufs[:3]
    rows = rows_ref[...]
    share = down_ref.shape[0] // 3
    width = rows.shape[1]

    def dot(a, b):
        return jnp.dot(a, b, preferred_element_type=jnp.float32)

    copies[0].wait()
    gate = dot(rows, gate_ref[...])
    copies[1].wait()
    inners = [(jax.nn.silu(gate) * dot(rows, up_ref[...])).astype(jnp.bfloat16)]
    for copy, ref in zip(copies[3:], bufs[3:]):
        copy.wait()
        both = [
            jnp.concatenate([ref[:share, k : k + share], ref[share : 2 * share, k : k + share]], 1)
            for k in range(0, width, share)
        ]
        both = dot(rows, jnp.concatenate(both, 0))
        inners.append((jax.nn.silu(both[:, :share]) * both[:, share:]).astype(jnp.bfloat16))
    copies[2].wait()
    step = 2 * share
    for k in range(0, width, step):
        total = dot(inners[0], down_ref[:, k : k + step])
        for inner, ref in zip(inners[1:], bufs[3:]):
            total = total + dot(inner, ref[2 * share :, k : k + step])
        out_ref[:, k : k + step] = total.astype(out_ref.dtype)


def per_device(
    residual_in,
    queries,
    keys,
    values,
    out_gate,
    beta_logit,
    decay_logit,
    decay_log,
    head_gain,
    out_weight,
    norm_gain,
    final_gain,
    expert_index,
    route_weights,
    expert_gate,
    expert_up,
    expert_down,
):
    length, width = residual_in.shape

    vmem = pl.BlockSpec(memory_space=pltpu.VMEM)
    both, mix, local = pl.pallas_call(
        local_span,
        out_shape=(
            pltpu.VMEM((2 * HEAD_FEATURES, HEAD_FEATURES), jnp.bfloat16),
            pltpu.VMEM((length, HEAD_FEATURES), jnp.float32),
            pltpu.VMEM((length, HEAD_FEATURES), jnp.float32),
        ),
        in_specs=[vmem] * 5 + [pl.BlockSpec(memory_space=pltpu.SMEM)],
        out_specs=(vmem,) * 3,
        name="local_span",
    )(queries, keys, values, beta_logit, decay_logit, decay_log)
    split_count = lax.axis_size("tp")
    side = round(split_count**0.5)
    gate_matrix, up_matrix, down_matrix = (expert_gate[0], expert_up[0], expert_down[0])
    state, thirds = entering(both, (gate_matrix, up_matrix, down_matrix), side)
    mixed = local + mm(mix, state)
    normalized = mixed * lax.rsqrt(jnp.mean(mixed * mixed, -1, keepdims=True) + 1e-06) * head_gain
    gated = (normalized * jax.nn.silu(out_gate.astype(jnp.float32))).astype(jnp.bfloat16)
    expert_count = lax.axis_size(SP) * expert_gate.shape[0]
    rows = length // split_count
    first = lax.axis_index("tp") * rows
    projected = sum_at_owner(
        jnp.dot(gated, out_weight, preferred_element_type=jnp.float32).astype(jnp.bfloat16), "tp", 0
    )
    residual = lax.dynamic_slice_in_dim(residual_in, first, rows, 0)
    routes = lax.dynamic_slice_in_dim(expert_index, first, rows, 0)
    weights = lax.dynamic_slice_in_dim(route_weights, first, rows, 0)
    hidden_in = layer_norm(
        residual_scale * residual.astype(jnp.float32) + projected, norm_gain
    ).astype(jnp.bfloat16)
    chips = lax.axis_size(Z)
    table = (routes[:, :, None] == jnp.arange(expert_count, dtype=jnp.int32)).astype(jnp.bfloat16)
    send = jnp.einsum(
        "rs,rd->sd", jnp.sum(table, 1), hidden_in, preferred_element_type=jnp.float32
    ).astype(jnp.bfloat16)

    def along_z(x):
        out = lax.all_to_all(x.reshape(chips, 16, width // 8), Z, 0, 0, tiled=True)
        return out.reshape(chips, 2, width)

    def in_plane(x):
        return lax.all_to_all(x, PLANE, 0, 0, tiled=True)

    half = chips // 2
    arrived = along_z(send).transpose(1, 0, 2).reshape(2, 2, half, width)
    swapped = arrived[:, ::-1]
    turns = jnp.stack([arrived, swapped], 1)[:, None, :, None]
    turns = jnp.broadcast_to(turns, (2, side // 2, 2, side // 2, 2, half, width))
    piece = in_plane(turns.reshape(2 * split_count, half, width)).reshape(-1, width)
    tables = (gate_matrix, up_matrix, down_matrix, *thirds)
    partial_value = pl.pallas_call(
        run_experts,
        out_shape=pltpu.VMEM(piece.shape, jnp.bfloat16),
        in_specs=[vmem] + [pl.BlockSpec(memory_space=pl.ANY)] * 6,
        out_specs=vmem,
        scratch_shapes=[pltpu.VMEM(x.shape, x.dtype) for x in tables]
        + [pltpu.SemaphoreType.DMA((6,))],
        name="run_experts",
    )(held(piece), *tables)
    parts = in_plane(partial_value.reshape(2 * split_count, half, width))
    parts = parts.reshape(2, side // 2, 2, side // 2, 2, half, width).astype(jnp.float32)
    parts = jnp.sum(parts, axis=(1, 3))
    result = jnp.stack([parts[:, 0, 0] + parts[:, 1, 1], parts[:, 0, 1] + parts[:, 1, 0]], 1)
    result = result.reshape(2, chips, width).astype(jnp.bfloat16)
    back = along_z(result.transpose(1, 0, 2)).reshape(expert_count, width)
    gathered = jnp.einsum("rks,sd->rkd", table, back, preferred_element_type=jnp.float32)
    routed = jnp.sum(weights[..., None] * gathered, 1)
    layer_out = layer_norm(
        residual_scale * hidden_in.astype(jnp.float32) + routed, final_gain
    ).astype(jnp.bfloat16)
    layer_out = collect(layer_out, "tp", 0)
    return layer_out


def solution(mesh):
    split = Mesh(
        mesh.devices.reshape(8, 2, 2, mesh.shape["tp"]), ("zh", "zl", "c", "tp")
    )
    placed = (
        P(SP, None),
        P(SP, "tp"),
        P(SP, "tp"),
        P(SP, "tp"),
        P(SP, "tp"),
        P("tp", SP),
        P("tp", SP),
        P("tp"),
        P(),
        P("tp", None),
        P(),
        P(),
        P(SP, None),
        P(SP, None),
        P(SP, None, "tp"),
        P(SP, None, "tp"),
        P(SP, "tp", None),
    )

    return jax.shard_map(per_device, mesh=split, in_specs=placed, out_specs=P(SP, None), check_vma=False)
```

```python
import jax
import jax.numpy as jnp
from jax import lax
from jax.experimental import pallas as pl
from jax.experimental.pallas import tpu as pltpu
from jax.sharding import Mesh
from jax.sharding import PartitionSpec as P


HEAD_FEATURES = 128
LANES = 128
Z = ("zh", "zl")
SP = ("zh", "zl", "c")
PLANE = ("c", "tp")


highest_precision = lax.Precision.HIGHEST
residual_scale = 2.0**0.5


def held(x):
    return pltpu.with_memory_space_constraint(x, pltpu.VMEM)


def mm(a, b):
    return jnp.dot(a, b, precision=highest_precision)


def regroup(lanes):
    row = lax.broadcasted_iota(jnp.int32, (16 * lanes, 16 * lanes), 0)
    col = lax.broadcasted_iota(jnp.int32, (16 * lanes, 16 * lanes), 1)
    row_kind, row_part = (row // (4 * lanes), row // lanes % 4)
    col_part, col_kind = (col // (4 * lanes), col // lanes % 4)
    same = (row_kind == col_kind) & (row_part == col_part) & (row % lanes == col % lanes)
    return jnp.where(same, 1.0, 0.0).astype(jnp.bfloat16)


def pack_parts(gate_ref, up_ref, down_ref, outs):
    depth, hidden = gate_ref.shape
    half, lanes = (depth // 2, LANES // 4)
    order = regroup(lanes)
    for block in range(hidden // LANES):
        cut = slice(block * LANES, (block + 1) * LANES)
        kinds = [ref[k : k + half, cut] for ref in (gate_ref, up_ref) for k in (0, half)]
        parts = jnp.dot(jnp.concatenate(kinds, 1), order, preferred_element_type=jnp.float32)
        parts = parts.astype(jnp.bfloat16)
        for part, out in enumerate(outs):
            out[block * half : (block + 1) * half] = parts[:, part * LANES : (part + 1) * LANES]
            first = block * LANES + part * lanes
            for k in range(depth // LANES):
                row = hidden // LANES * (half + k * lanes) + block * lanes
                out[row : row + lanes] = down_ref[first : first + lanes, k * LANES : (k + 1) * LANES]


def spread(parts, side):
    out = []
    for part, (dy, dx) in zip(parts, ((0, 1), (0, side - 1), (1, 0), (side - 1, 0))):
        pairs = [
            (y * side + x, (y + dy) % side * side + (x + dx) % side)
            for y in range(side)
            for x in range(side)
        ]
        out.append(lax.ppermute(part, "tp", pairs))
    return out


def entering(own, parts, side):
    kind = jnp.bfloat16
    zh, zl, c = (lax.axis_index(axis) for axis in SP)
    near = lax.all_gather(own, ("zl", "c")).astype(jnp.float32)
    width = own.shape[-1]
    map_in, state_in = (jnp.eye(width, dtype=jnp.float32), jnp.zeros((width, width), jnp.float32))
    map_all, state_all = (near[0, :width], near[0, width:])
    for k in range(1, 4):
        inside = k == 2 * zl + c
        map_in = jnp.where(inside, map_all, map_in)
        state_in = jnp.where(inside, state_all, state_in)
        map_k, state_k = (near[k, :width], near[k, width:])
        state_all = mm(map_k, state_all) + state_k
        map_all = mm(map_k, map_all)
    group = jnp.concatenate([map_all, state_all], 0).astype(kind)
    quarter = lax.dynamic_slice_in_dim(group, (2 * zl + c) * (width // 2), width // 2, 0)
    count = lax.axis_size(Z)
    quarter, parts = lax.optimization_barrier((quarter, parts))
    parts = spread(parts, side)
    far = jnp.broadcast_to(quarter[None], (count, *quarter.shape))
    far = lax.all_to_all(far, Z, 0, 0, tiled=True)
    far = lax.all_gather(far, "c")
    far = far.reshape(2, count // 2, 2, width // 2, width).transpose(1, 2, 0, 3, 4)
    far = far.reshape(count // 2, 2 * width, width).astype(jnp.float32)
    state = jnp.zeros((width, width), jnp.float32)
    for k in range(count // 2 - 1):
        state = jnp.where(k < zh, mm(far[k, :width], state) + far[k, width:], state)
    return mm(map_in, state) + state_in, parts


def in_blocks(x, dim, length):
    shape = x.shape
    blocks = x.reshape(*shape[:dim], length, shape[dim] // length, *shape[dim + 1 :])
    return jnp.moveaxis(blocks, dim, 0)


def sum_at_owner(x, axis, dim):
    length = lax.axis_size(axis)
    blocks = lax.all_to_all(in_blocks(x, dim, length), axis, 0, 0, tiled=True)
    return jnp.sum(blocks.astype(jnp.float32), axis=0)


def copy_for_each(x, axis):
    length = lax.axis_size(axis)
    return lax.all_to_all(jnp.broadcast_to(x[None], (length, *x.shape)), axis, 0, 0, tiled=True)


def in_order(blocks, dim):
    shape = list(blocks.shape[1:])
    shape[dim] *= blocks.shape[0]
    return jnp.moveaxis(blocks, 0, dim).reshape(shape)


def collect(x, axis, dim):
    blocks = copy_for_each(x, axis)
    return in_order(blocks, dim)


def layer_norm(data, gain):
    center = data - jnp.mean(data, -1, keepdims=True)
    return center * lax.rsqrt(jnp.mean(center * center, -1, keepdims=True) + 1e-05) * gain


def local_span(q_ref, k_ref, v_ref, beta_ref, decay_ref, rate_ref, *refs):
    tables, (both_ref, mix_ref, out_ref), outs = refs[:3], refs[3:6], refs[6:10]
    bufs, part_bufs, sems = refs[10:13], refs[13:17], refs[17]
    copies = [pltpu.make_async_copy(x, y, sems.at[k]) for k, (x, y) in enumerate(zip(tables, bufs))]
    for copy in copies:
        copy.start()
    size = HEAD_FEATURES
    row = lax.broadcasted_iota(jnp.int32, (size, size), 0)
    col = lax.broadcasted_iota(jnp.int32, (size, size), 1)
    eye = row == col
    causal = col <= row

    def to_column(data):
        return jnp.sum(jnp.where(eye, data, 0.0), 1, keepdims=True)

    def to_row(data):
        return jnp.sum(jnp.where(eye, data, 0.0), 0, keepdims=True)

    def dot(a, b, dims=((1,), (0,))):
        return lax.dot_general(
            a.astype(jnp.bfloat16),
            b.astype(jnp.bfloat16),
            (dims, ((), ())),
            preferred_element_type=jnp.float32,
        )

    beta = to_column(jax.nn.sigmoid(beta_ref[...].astype(jnp.float32)))
    logit = decay_ref[...].astype(jnp.float32)
    softplus = jnp.maximum(logit, 0.0) + jnp.log(1.0 + jnp.exp(-jnp.abs(logit)))
    decay = -jnp.exp(jnp.full((1, size), rate_ref[0], jnp.float32)) * softplus
    running = jnp.sum(jnp.where(causal, decay, 0.0), 1, keepdims=True)
    last = jnp.sum(decay, 1, keepdims=True)
    within = jnp.exp(jnp.where(causal, running - to_row(running), -1e30))
    query = q_ref[...].astype(jnp.float32)
    key = k_ref[...].astype(jnp.float32)
    value = v_ref[...].astype(jnp.float32)
    query_scale = lax.rsqrt(jnp.sum(query * query, 1, keepdims=True) + 1e-06) * size ** (-0.5)
    key_scale = lax.rsqrt(jnp.sum(key * key, 1, keepdims=True) + 1e-06)
    key_scale_row = to_row(key_scale)
    across = within * key_scale_row
    lower = jnp.where(
        col < row, dot(k_ref[...], k_ref[...], ((1,), (1,))) * across * (beta * key_scale), 0.0
    )
    scores = dot(q_ref[...], k_ref[...], ((1,), (1,))) * across * query_scale
    for copy in copies:
        copy.wait()
    pack_parts(*bufs, part_bufs)
    copies = [
        pltpu.make_async_copy(x, y, sems.at[3 + k]) for k, (x, y) in enumerate(zip(part_bufs, outs))
    ]
    for copy in copies:
        copy.start()
    differ = row ^ col
    inverse = jnp.where(eye, 1.0, 0.0) - jnp.where(differ == 1, lower, 0.0)
    for level in range(1, 7):
        part = jnp.where((differ >> level) == 1, lower, 0.0)
        inverse = inverse - dot(dot(inverse, part), inverse)
    grown = jnp.exp(running)
    key = key * key_scale
    right = jnp.concatenate([key * (beta * grown), value * beta], 1)
    solved = dot(inverse, right)
    leaving = dot(key * jnp.exp(last - running), solved, ((0,), (0,)))
    passed = jnp.where(eye, jnp.exp(last), 0.0) - leaving[:, :size]
    both_ref[...] = jnp.concatenate([passed, leaving[:, size:]], 0).astype(both_ref.dtype)
    seen = dot(scores, solved)
    mix_ref[...] = query * (query_scale * grown) - seen[:, :size]
    out_ref[...] = seen[:, size:]
    for copy in copies:
        copy.wait()


def run_experts(rows_ref, *refs):
    out_ref, bufs, sems = refs[7], refs[8:15], refs[15]
    copies = [pltpu.make_async_copy(refs[k], bufs[k], sems.at[k]) for k in range(7)]
    for copy in (*copies[:2], *copies[3:], copies[2]):
        copy.start()
    gate_ref, up_ref, down_ref = bufs[:3]
    rows = rows_ref[...]
    width = rows.shape[1]
    half, lanes, blocks = (width // 2, LANES // 4, down_ref.shape[0] // LANES)

    def dot(a, b):
        return jnp.dot(a, b, preferred_element_type=jnp.float32)

    copies[0].wait()
    gate = dot(rows, gate_ref[...])
    copies[1].wait()
    inner = (jax.nn.silu(gate) * dot(rows, up_ref[...])).astype(jnp.bfloat16)
    place = lax.broadcasted_iota(jnp.int32, (rows.shape[0], LANES), 1) // lanes
    arrived = [jnp.zeros((rows.shape[0], LANES), jnp.float32)] * blocks
    for part, (copy, ref) in enumerate(zip(copies[3:], bufs[3:])):
        copy.wait()
        table = jnp.concatenate([ref[k * half : (k + 1) * half] for k in range(blocks)], 1)
        low, high = (dot(rows[:, :half], table), dot(rows[:, half:], table))
        for k in range(blocks):
            cut = slice(k * LANES, (k + 1) * LANES)
            sums = low[:, cut] + pltpu.roll(high[:, cut], LANES - lanes, 1)
            acts = jax.nn.silu(sums) * pltpu.roll(sums, LANES - 2 * lanes, 1)
            if part > 0:
                acts = pltpu.roll(acts, part * lanes, 1)
            arrived[k] = jnp.where(place == part, acts, arrived[k])
    arrived = jnp.concatenate(arrived, 1).astype(jnp.bfloat16)
    copies[2].wait()

    def down_block(k):
        row = blocks * (half + k * lanes)
        runs = [ref[row + b * lanes : row + (b + 1) * lanes] for b in range(blocks) for ref in bufs[3:]]
        return jnp.concatenate(runs, 0)

    for k in range(0, width // LANES, 2):
        cut = slice(k * LANES, (k + 2) * LANES)
        other = jnp.concatenate([down_block(k), down_block(k + 1)], 1)
        out_ref[:, cut] = (dot(inner, down_ref[:, cut]) + dot(arrived, other)).astype(out_ref.dtype)


def per_device(
    residual_in,
    queries,
    keys,
    values,
    out_gate,
    beta_logit,
    decay_logit,
    decay_log,
    head_gain,
    out_weight,
    norm_gain,
    final_gain,
    expert_index,
    route_weights,
    expert_gate,
    expert_up,
    expert_down,
):
    length, width = residual_in.shape

    vmem = pl.BlockSpec(memory_space=pltpu.VMEM)
    anywhere = pl.BlockSpec(memory_space=pl.ANY)
    split_count = lax.axis_size("tp")
    side = round(split_count**0.5)
    tables = (expert_gate[0], expert_up[0], expert_down[0])
    packed = (3 * tables[0].size // 4 // LANES, LANES)
    both, mix, local, *parts = pl.pallas_call(
        local_span,
        out_shape=(
            pltpu.VMEM((2 * HEAD_FEATURES, HEAD_FEATURES), jnp.bfloat16),
            pltpu.VMEM((length, HEAD_FEATURES), jnp.float32),
            pltpu.VMEM((length, HEAD_FEATURES), jnp.float32),
        )
        + (jax.ShapeDtypeStruct(packed, jnp.bfloat16),) * 4,
        in_specs=[vmem] * 5 + [pl.BlockSpec(memory_space=pltpu.SMEM)] + [anywhere] * 3,
        out_specs=(vmem,) * 3 + (anywhere,) * 4,
        scratch_shapes=[pltpu.VMEM(x.shape, x.dtype) for x in tables]
        + [pltpu.VMEM(packed, jnp.bfloat16)] * 4
        + [pltpu.SemaphoreType.DMA((7,))],
        name="local_span",
    )(queries, keys, values, beta_logit, decay_logit, decay_log, *tables)
    state, parts = entering(both, parts, side)
    mixed = local + mm(mix, state)
    normalized = mixed * lax.rsqrt(jnp.mean(mixed * mixed, -1, keepdims=True) + 1e-06) * head_gain
    gated = (normalized * jax.nn.silu(out_gate.astype(jnp.float32))).astype(jnp.bfloat16)
    expert_count = lax.axis_size(SP) * expert_gate.shape[0]
    rows = length // split_count
    first = lax.axis_index("tp") * rows
    projected = sum_at_owner(
        jnp.dot(gated, out_weight, preferred_element_type=jnp.float32).astype(jnp.bfloat16), "tp", 0
    )
    residual = lax.dynamic_slice_in_dim(residual_in, first, rows, 0)
    routes = lax.dynamic_slice_in_dim(expert_index, first, rows, 0)
    weights = lax.dynamic_slice_in_dim(route_weights, first, rows, 0)
    hidden_in = layer_norm(
        residual_scale * residual.astype(jnp.float32) + projected, norm_gain
    ).astype(jnp.bfloat16)
    chips = lax.axis_size(Z)
    table = (routes[:, :, None] == jnp.arange(expert_count, dtype=jnp.int32)).astype(jnp.bfloat16)
    send = jnp.einsum(
        "rs,rd->sd", jnp.sum(table, 1), hidden_in, preferred_element_type=jnp.float32
    ).astype(jnp.bfloat16)

    def along_z(x):
        out = lax.all_to_all(x.reshape(chips, 16, width // 8), Z, 0, 0, tiled=True)
        return out.reshape(chips, 2, width)

    def in_plane(x):
        return lax.all_to_all(x, PLANE, 0, 0, tiled=True)

    half = chips // 2
    arrived = along_z(send).transpose(1, 0, 2).reshape(2, 2, half, width)
    swapped = arrived[:, ::-1]
    turns = jnp.stack([arrived, swapped], 1)[:, None, :, None]
    turns = jnp.broadcast_to(turns, (2, side // 2, 2, side // 2, 2, half, width))
    piece = in_plane(turns.reshape(2 * split_count, half, width)).reshape(-1, width)
    tables += tuple(parts)
    partial_value = pl.pallas_call(
        run_experts,
        out_shape=pltpu.VMEM(piece.shape, jnp.bfloat16),
        in_specs=[vmem] + [anywhere] * 7,
        out_specs=vmem,
        scratch_shapes=[pltpu.VMEM(x.shape, x.dtype) for x in tables]
        + [pltpu.SemaphoreType.DMA((7,))],
        name="run_experts",
    )(held(piece), *tables)
    shares = in_plane(partial_value.reshape(2 * split_count, half, width))
    shares = shares.reshape(2, side // 2, 2, side // 2, 2, half, width).astype(jnp.float32)
    shares = jnp.sum(shares, axis=(1, 3))
    result = jnp.stack([shares[:, 0, 0] + shares[:, 1, 1], shares[:, 0, 1] + shares[:, 1, 0]], 1)
    result = result.reshape(2, chips, width).astype(jnp.bfloat16)
    back = along_z(result.transpose(1, 0, 2)).reshape(expert_count, width)
    gathered = jnp.einsum("rks,sd->rkd", table, back, preferred_element_type=jnp.float32)
    routed = jnp.sum(weights[..., None] * gathered, 1)
    layer_out = layer_norm(
        residual_scale * hidden_in.astype(jnp.float32) + routed, final_gain
    ).astype(jnp.bfloat16)
    layer_out = collect(layer_out, "tp", 0)
    return layer_out


def solution(mesh):
    split = Mesh(
        mesh.devices.reshape(8, 2, 2, mesh.shape["tp"]), ("zh", "zl", "c", "tp")
    )
    placed = (
        P(SP, None),
        P(SP, "tp"),
        P(SP, "tp"),
        P(SP, "tp"),
        P(SP, "tp"),
        P("tp", SP),
        P("tp", SP),
        P("tp"),
        P(),
        P("tp", None),
        P(),
        P(),
        P(SP, None),
        P(SP, None),
        P(SP, None, "tp"),
        P(SP, None, "tp"),
        P(SP, "tp", None),
    )

    return jax.shard_map(per_device, mesh=split, in_specs=placed, out_specs=P(SP, None), check_vma=False)
```

```python
import jax
import jax.numpy as jnp
from jax import lax
from jax.experimental import pallas as pl
from jax.experimental.pallas import tpu as pltpu
from jax.sharding import Mesh
from jax.sharding import PartitionSpec as P


HEAD_FEATURES = 128
LANES = 128
Z = ("zh", "zl")
SP = ("zh", "zl", "c")
PLANE = ("c", "tp")


highest_precision = lax.Precision.HIGHEST
residual_scale = 2.0**0.5


def held(x):
    return pltpu.with_memory_space_constraint(x, pltpu.VMEM)


def mm(a, b):
    return jnp.dot(a, b, precision=highest_precision)


def regroup(lanes):
    row = lax.broadcasted_iota(jnp.int32, (16 * lanes, 16 * lanes), 0)
    col = lax.broadcasted_iota(jnp.int32, (16 * lanes, 16 * lanes), 1)
    row_kind, row_part = (row // (4 * lanes), row // lanes % 4)
    col_part, col_kind = (col // (4 * lanes), col // lanes % 4)
    same = (row_kind == col_kind) & (row_part == col_part) & (row % lanes == col % lanes)
    return jnp.where(same, 1.0, 0.0).astype(jnp.bfloat16)


def pack_parts(gate_ref, up_ref, down_ref, bufs, outs, sems):
    depth, hidden = gate_ref.shape
    half, lanes, blocks = (depth // 2, LANES // 4, hidden // LANES)
    copies = []

    def leave(rows):
        for buf, out in zip(bufs, outs):
            copies.append(pltpu.make_async_copy(buf.at[rows], out.at[rows], sems.at[len(copies)]))
            copies[-1].start()

    for part, buf in enumerate(bufs):
        for block in range(blocks):
            first = block * LANES + part * lanes
            for k in range(depth // LANES):
                row = blocks * (half + k * lanes) + block * lanes
                buf[row : row + lanes] = down_ref[first : first + lanes, k * LANES : (k + 1) * LANES]
    leave(pl.ds(blocks * half, blocks * lanes * (depth // LANES)))
    order = regroup(lanes)
    for block in range(blocks):
        cut = slice(block * LANES, (block + 1) * LANES)
        kinds = [ref[k : k + half, cut] for ref in (gate_ref, up_ref) for k in (0, half)]
        parts = jnp.dot(jnp.concatenate(kinds, 1), order, preferred_element_type=jnp.float32)
        parts = parts.astype(jnp.bfloat16)
        for part, buf in enumerate(bufs):
            buf[block * half : (block + 1) * half] = parts[:, part * LANES : (part + 1) * LANES]
        leave(pl.ds(block * half, half))
    for copy in copies:
        copy.wait()


def spread(parts, side):
    out = []
    for part, (dy, dx) in zip(parts, ((0, 1), (0, side - 1), (1, 0), (side - 1, 0))):
        pairs = [
            (y * side + x, (y + dy) % side * side + (x + dx) % side)
            for y in range(side)
            for x in range(side)
        ]
        out.append(lax.ppermute(part, "tp", pairs))
    return out


def entering(own, parts, side):
    kind = jnp.bfloat16
    zh, zl, c = (lax.axis_index(axis) for axis in SP)
    near = lax.all_gather(own, ("zl", "c")).astype(jnp.float32)
    width = own.shape[-1]
    map_in, state_in = (jnp.eye(width, dtype=jnp.float32), jnp.zeros((width, width), jnp.float32))
    map_all, state_all = (near[0, :width], near[0, width:])
    for k in range(1, 4):
        inside = k == 2 * zl + c
        map_in = jnp.where(inside, map_all, map_in)
        state_in = jnp.where(inside, state_all, state_in)
        map_k, state_k = (near[k, :width], near[k, width:])
        state_all = mm(map_k, state_all) + state_k
        map_all = mm(map_k, map_all)
    group = jnp.concatenate([map_all, state_all], 0).astype(kind)
    quarter = lax.dynamic_slice_in_dim(group, (2 * zl + c) * (width // 2), width // 2, 0)
    count = lax.axis_size(Z)
    quarter, parts = lax.optimization_barrier((quarter, parts))
    parts = spread(parts, side)
    far = jnp.broadcast_to(quarter[None], (count, *quarter.shape))
    far = lax.all_to_all(far, Z, 0, 0, tiled=True)
    far = lax.all_gather(far, "c")
    far = far.reshape(2, count // 2, 2, width // 2, width).transpose(1, 2, 0, 3, 4)
    far = far.reshape(count // 2, 2 * width, width).astype(jnp.float32)
    state = jnp.zeros((width, width), jnp.float32)
    for k in range(count // 2 - 1):
        state = jnp.where(k < zh, mm(far[k, :width], state) + far[k, width:], state)
    return mm(map_in, state) + state_in, parts


def in_blocks(x, dim, length):
    shape = x.shape
    blocks = x.reshape(*shape[:dim], length, shape[dim] // length, *shape[dim + 1 :])
    return jnp.moveaxis(blocks, dim, 0)


def sum_at_owner(x, axis, dim):
    length = lax.axis_size(axis)
    blocks = lax.all_to_all(in_blocks(x, dim, length), axis, 0, 0, tiled=True)
    return jnp.sum(blocks.astype(jnp.float32), axis=0)


def copy_for_each(x, axis):
    length = lax.axis_size(axis)
    return lax.all_to_all(jnp.broadcast_to(x[None], (length, *x.shape)), axis, 0, 0, tiled=True)


def in_order(blocks, dim):
    shape = list(blocks.shape[1:])
    shape[dim] *= blocks.shape[0]
    return jnp.moveaxis(blocks, 0, dim).reshape(shape)


def collect(x, axis, dim):
    blocks = copy_for_each(x, axis)
    return in_order(blocks, dim)


def layer_norm(data, gain):
    center = data - jnp.mean(data, -1, keepdims=True)
    return center * lax.rsqrt(jnp.mean(center * center, -1, keepdims=True) + 1e-05) * gain


def local_span(q_ref, k_ref, v_ref, beta_ref, decay_ref, rate_ref, *refs):
    tables, (both_ref, mix_ref, out_ref), outs = refs[:3], refs[3:6], refs[6:10]
    bufs, part_bufs, sems = refs[10:13], refs[13:17], refs[17]
    copies = [pltpu.make_async_copy(x, y, sems.at[k]) for k, (x, y) in enumerate(zip(tables, bufs))]
    for copy in copies:
        copy.start()
    size = HEAD_FEATURES
    row = lax.broadcasted_iota(jnp.int32, (size, size), 0)
    col = lax.broadcasted_iota(jnp.int32, (size, size), 1)
    eye = row == col
    causal = col <= row

    def to_column(data):
        return jnp.sum(jnp.where(eye, data, 0.0), 1, keepdims=True)

    def to_row(data):
        return jnp.sum(jnp.where(eye, data, 0.0), 0, keepdims=True)

    def dot(a, b, dims=((1,), (0,))):
        return lax.dot_general(
            a.astype(jnp.bfloat16),
            b.astype(jnp.bfloat16),
            (dims, ((), ())),
            preferred_element_type=jnp.float32,
        )

    beta = to_column(jax.nn.sigmoid(beta_ref[...].astype(jnp.float32)))
    logit = decay_ref[...].astype(jnp.float32)
    softplus = jnp.maximum(logit, 0.0) + jnp.log(1.0 + jnp.exp(-jnp.abs(logit)))
    decay = -jnp.exp(jnp.full((1, size), rate_ref[0], jnp.float32)) * softplus
    running = jnp.sum(jnp.where(causal, decay, 0.0), 1, keepdims=True)
    last = jnp.sum(decay, 1, keepdims=True)
    within = jnp.exp(jnp.where(causal, running - to_row(running), -1e30))
    query = q_ref[...].astype(jnp.float32)
    key = k_ref[...].astype(jnp.float32)
    value = v_ref[...].astype(jnp.float32)
    query_scale = lax.rsqrt(jnp.sum(query * query, 1, keepdims=True) + 1e-06) * size ** (-0.5)
    key_scale = lax.rsqrt(jnp.sum(key * key, 1, keepdims=True) + 1e-06)
    key_scale_row = to_row(key_scale)
    across = within * key_scale_row
    lower = jnp.where(
        col < row, dot(k_ref[...], k_ref[...], ((1,), (1,))) * across * (beta * key_scale), 0.0
    )
    scores = dot(q_ref[...], k_ref[...], ((1,), (1,))) * across * query_scale
    differ = row ^ col
    inverse = jnp.where(eye, 1.0, 0.0) - jnp.where(differ == 1, lower, 0.0)
    for level in range(1, 7):
        part = jnp.where((differ >> level) == 1, lower, 0.0)
        inverse = inverse - dot(dot(inverse, part), inverse)
    grown = jnp.exp(running)
    key = key * key_scale
    right = jnp.concatenate([key * (beta * grown), value * beta], 1)
    solved = dot(inverse, right)
    leaving = dot(key * jnp.exp(last - running), solved, ((0,), (0,)))
    passed = jnp.where(eye, jnp.exp(last), 0.0) - leaving[:, :size]
    both_ref[...] = jnp.concatenate([passed, leaving[:, size:]], 0).astype(both_ref.dtype)
    seen = dot(scores, solved)
    mix_ref[...] = query * (query_scale * grown) - seen[:, :size]
    out_ref[...] = seen[:, size:]
    for copy in copies:
        copy.wait()
    pack_parts(*bufs, part_bufs, outs, sems.at[3:])


def run_experts(rows_ref, *refs):
    out_ref, bufs, sems = refs[7], refs[8:15], refs[15]
    copies = [pltpu.make_async_copy(refs[k], bufs[k], sems.at[k]) for k in range(7)]
    for copy in (*copies[:2], *copies[3:], copies[2]):
        copy.start()
    gate_ref, up_ref, down_ref = bufs[:3]
    rows = rows_ref[...]
    width = rows.shape[1]
    half, lanes, blocks = (width // 2, LANES // 4, down_ref.shape[0] // LANES)

    def dot(a, b):
        return jnp.dot(a, b, preferred_element_type=jnp.float32)

    copies[0].wait()
    gate = dot(rows, gate_ref[...])
    copies[1].wait()
    inner = (jax.nn.silu(gate) * dot(rows, up_ref[...])).astype(jnp.bfloat16)
    place = lax.broadcasted_iota(jnp.int32, (rows.shape[0], LANES), 1) // lanes
    arrived = [jnp.zeros((rows.shape[0], LANES), jnp.float32)] * blocks
    for part, (copy, ref) in enumerate(zip(copies[3:], bufs[3:])):
        copy.wait()
        table = jnp.concatenate([ref[k * half : (k + 1) * half] for k in range(blocks)], 1)
        low, high = (dot(rows[:, :half], table), dot(rows[:, half:], table))
        for k in range(blocks):
            cut = slice(k * LANES, (k + 1) * LANES)
            sums = low[:, cut] + pltpu.roll(high[:, cut], LANES - lanes, 1)
            acts = jax.nn.silu(sums) * pltpu.roll(sums, LANES - 2 * lanes, 1)
            if part > 0:
                acts = pltpu.roll(acts, part * lanes, 1)
            arrived[k] = jnp.where(place == part, acts, arrived[k])
    arrived = jnp.concatenate(arrived, 1).astype(jnp.bfloat16)
    copies[2].wait()

    def down_block(k):
        row = blocks * (half + k * lanes)
        runs = [ref[row + b * lanes : row + (b + 1) * lanes] for b in range(blocks) for ref in bufs[3:]]
        return jnp.concatenate(runs, 0)

    for k in range(0, width // LANES, 2):
        cut = slice(k * LANES, (k + 2) * LANES)
        other = jnp.concatenate([down_block(k), down_block(k + 1)], 1)
        out_ref[:, cut] = (dot(inner, down_ref[:, cut]) + dot(arrived, other)).astype(out_ref.dtype)


def per_device(
    residual_in,
    queries,
    keys,
    values,
    out_gate,
    beta_logit,
    decay_logit,
    decay_log,
    head_gain,
    out_weight,
    norm_gain,
    final_gain,
    expert_index,
    route_weights,
    expert_gate,
    expert_up,
    expert_down,
):
    length, width = residual_in.shape

    vmem = pl.BlockSpec(memory_space=pltpu.VMEM)
    anywhere = pl.BlockSpec(memory_space=pl.ANY)
    split_count = lax.axis_size("tp")
    side = round(split_count**0.5)
    tables = (expert_gate[0], expert_up[0], expert_down[0])
    packed = (3 * tables[0].size // 4 // LANES, LANES)
    both, mix, local, *parts = pl.pallas_call(
        local_span,
        out_shape=(
            pltpu.VMEM((2 * HEAD_FEATURES, HEAD_FEATURES), jnp.bfloat16),
            pltpu.VMEM((length, HEAD_FEATURES), jnp.float32),
            pltpu.VMEM((length, HEAD_FEATURES), jnp.float32),
        )
        + (jax.ShapeDtypeStruct(packed, jnp.bfloat16),) * 4,
        in_specs=[vmem] * 5 + [pl.BlockSpec(memory_space=pltpu.SMEM)] + [anywhere] * 3,
        out_specs=(vmem,) * 3 + (anywhere,) * 4,
        scratch_shapes=[pltpu.VMEM(x.shape, x.dtype) for x in tables]
        + [pltpu.VMEM(packed, jnp.bfloat16)] * 4
        + [pltpu.SemaphoreType.DMA((19,))],
        name="local_span",
    )(queries, keys, values, beta_logit, decay_logit, decay_log, *tables)
    state, parts = entering(both, parts, side)
    mixed = local + mm(mix, state)
    normalized = mixed * lax.rsqrt(jnp.mean(mixed * mixed, -1, keepdims=True) + 1e-06) * head_gain
    gated = (normalized * jax.nn.silu(out_gate.astype(jnp.float32))).astype(jnp.bfloat16)
    expert_count = lax.axis_size(SP) * expert_gate.shape[0]
    rows = length // split_count
    first = lax.axis_index("tp") * rows
    projected = sum_at_owner(
        jnp.dot(gated, out_weight, preferred_element_type=jnp.float32).astype(jnp.bfloat16), "tp", 0
    )
    residual = lax.optimization_barrier(lax.dynamic_slice_in_dim(residual_in, first, rows, 0))
    routes = lax.dynamic_slice_in_dim(expert_index, first, rows, 0)
    weights = lax.dynamic_slice_in_dim(route_weights, first, rows, 0)
    hidden_in = layer_norm(
        residual_scale * residual.astype(jnp.float32) + projected, norm_gain
    ).astype(jnp.bfloat16)
    chips = lax.axis_size(Z)
    table = (routes[:, :, None] == jnp.arange(expert_count, dtype=jnp.int32)).astype(jnp.bfloat16)
    send = jnp.einsum(
        "rs,rd->sd", jnp.sum(table, 1), hidden_in, preferred_element_type=jnp.float32
    ).astype(jnp.bfloat16)

    def along_z(x):
        out = lax.all_to_all(x.reshape(chips, 2, width), Z, 0, 0, tiled=True)
        return out.reshape(chips, 2, width)

    def in_plane(x):
        return lax.all_to_all(x, PLANE, 0, 0, tiled=True)

    half = chips // 2
    arrived = along_z(send).transpose(1, 0, 2).reshape(2, 2, half, width)
    swapped = arrived[:, ::-1]
    turns = jnp.stack([arrived, swapped], 1)[:, None, :, None]
    turns = jnp.broadcast_to(turns, (2, side // 2, 2, side // 2, 2, half, width))
    piece = in_plane(turns.reshape(2 * split_count, half, width)).reshape(-1, width)
    tables += tuple(parts)
    partial_value = pl.pallas_call(
        run_experts,
        out_shape=pltpu.VMEM(piece.shape, jnp.bfloat16),
        in_specs=[vmem] + [anywhere] * 7,
        out_specs=vmem,
        scratch_shapes=[pltpu.VMEM(x.shape, x.dtype) for x in tables]
        + [pltpu.SemaphoreType.DMA((7,))],
        name="run_experts",
    )(held(piece), *tables)
    shares = in_plane(partial_value.reshape(2 * split_count, half, width))
    shares = shares.reshape(2, side // 2, 2, side // 2, 2, half, width).astype(jnp.float32)
    shares = jnp.sum(shares, axis=(1, 3))
    result = jnp.stack([shares[:, 0, 0] + shares[:, 1, 1], shares[:, 0, 1] + shares[:, 1, 0]], 1)
    result = result.reshape(2, chips, width).astype(jnp.bfloat16)
    back = along_z(result.transpose(1, 0, 2)).reshape(expert_count, width)
    gathered = jnp.einsum("rks,sd->rkd", table, back, preferred_element_type=jnp.float32)
    routed = jnp.sum(weights[..., None] * gathered, 1)
    layer_out = layer_norm(
        residual_scale * hidden_in.astype(jnp.float32) + routed, final_gain
    ).astype(jnp.bfloat16)
    layer_out = collect(layer_out, "tp", 0)
    return layer_out


def solution(mesh):
    split = Mesh(
        mesh.devices.reshape(8, 2, 2, mesh.shape["tp"]), ("zh", "zl", "c", "tp")
    )
    placed = (
        P(SP, None),
        P(SP, "tp"),
        P(SP, "tp"),
        P(SP, "tp"),
        P(SP, "tp"),
        P("tp", SP),
        P("tp", SP),
        P("tp"),
        P(),
        P("tp", None),
        P(),
        P(),
        P(SP, None),
        P(SP, None),
        P(SP, None, "tp"),
        P(SP, None, "tp"),
        P(SP, "tp", None),
    )

    return jax.shard_map(per_device, mesh=split, in_specs=placed, out_specs=P(SP, None), check_vma=False)
```

```python
import jax
import jax.numpy as jnp
from jax import lax
from jax.experimental import pallas as pl
from jax.experimental.pallas import tpu as pltpu
from jax.sharding import Mesh
from jax.sharding import PartitionSpec as P


HEAD_FEATURES = 128
LANES = 128
Z = ("zh", "zl")
SP = ("zh", "zl", "c")
PLANE = ("c", "tp")


highest_precision = lax.Precision.HIGHEST
residual_scale = 2.0**0.5


def held(x):
    return pltpu.with_memory_space_constraint(x, pltpu.VMEM)


def mm(a, b):
    return jnp.dot(a, b, precision=highest_precision)


def regroup(lanes):
    row = lax.broadcasted_iota(jnp.int32, (16 * lanes, 16 * lanes), 0)
    col = lax.broadcasted_iota(jnp.int32, (16 * lanes, 16 * lanes), 1)
    row_kind, row_part = (row // (4 * lanes), row // lanes % 4)
    col_part, col_kind = (col // (4 * lanes), col // lanes % 4)
    same = (row_kind == col_kind) & (row_part == col_part) & (row % lanes == col % lanes)
    return jnp.where(same, 1.0, 0.0).astype(jnp.bfloat16)


def pack_parts(gate_ref, up_ref, down_ref, bufs, outs, sems):
    depth, hidden = gate_ref.shape
    half, lanes, blocks = (depth // 2, LANES // 4, hidden // LANES)
    size = bufs[0].shape[0] // blocks
    early = size * (blocks - 1)
    copies = []
    for part, buf in enumerate(bufs):
        for block in range(blocks):
            first = block * LANES + part * lanes
            for k in range(depth // LANES):
                row = block * size + half + k * lanes
                buf[row : row + lanes] = down_ref[first : first + lanes, k * LANES : (k + 1) * LANES]
    order = regroup(lanes)
    for block in range(blocks):
        cut = slice(block * LANES, (block + 1) * LANES)
        kinds = [ref[k : k + half, cut] for ref in (gate_ref, up_ref) for k in (0, half)]
        parts = jnp.dot(jnp.concatenate(kinds, 1), order, preferred_element_type=jnp.float32)
        parts = parts.astype(jnp.bfloat16)
        for part, buf in enumerate(bufs):
            row = block * size
            buf[row : row + half] = parts[:, part * LANES : (part + 1) * LANES]
            last = row == early
            out = outs[part + 4] if last else outs[part].at[pl.ds(row, size)]
            copies.append(pltpu.make_async_copy(buf.at[pl.ds(row, size)], out, sems.at[len(copies)]))
            copies[-1].start()
    for copy in copies:
        copy.wait()


def spread(parts, side):
    out = []
    for part, (dy, dx) in zip(parts, ((0, 1), (0, side - 1), (1, 0), (side - 1, 0))):
        pairs = [
            (y * side + x, (y + dy) % side * side + (x + dx) % side)
            for y in range(side)
            for x in range(side)
        ]
        out.append(lax.ppermute(part, "tp", pairs))
    return out


def entering(own, parts, side):
    kind = jnp.bfloat16
    zh, zl, c = (lax.axis_index(axis) for axis in SP)
    near = lax.all_gather(own, ("zl", "c")).astype(jnp.float32)
    width = own.shape[-1]
    map_in, state_in = (jnp.eye(width, dtype=jnp.float32), jnp.zeros((width, width), jnp.float32))
    map_all, state_all = (near[0, :width], near[0, width:])
    for k in range(1, 4):
        inside = k == 2 * zl + c
        map_in = jnp.where(inside, map_all, map_in)
        state_in = jnp.where(inside, state_all, state_in)
        map_k, state_k = (near[k, :width], near[k, width:])
        state_all = mm(map_k, state_all) + state_k
        map_all = mm(map_k, map_all)
    group = jnp.concatenate([map_all, state_all], 0).astype(kind)
    quarter = lax.dynamic_slice_in_dim(group, (2 * zl + c) * (width // 2), width // 2, 0)
    count = lax.axis_size(Z)
    quarter, parts = lax.optimization_barrier((quarter, parts))
    parts = spread(parts, side)
    far = jnp.broadcast_to(quarter[None], (count, *quarter.shape))
    far = lax.all_to_all(far, Z, 0, 0, tiled=True)
    far = lax.all_gather(far, "c")
    far = far.reshape(2, count // 2, 2, width // 2, width).transpose(1, 2, 0, 3, 4)
    far = far.reshape(count // 2, 2 * width, width).astype(jnp.float32)
    state = jnp.zeros((width, width), jnp.float32)
    for k in range(count // 2 - 1):
        state = jnp.where(k < zh, mm(far[k, :width], state) + far[k, width:], state)
    return mm(map_in, state) + state_in, parts


def in_blocks(x, dim, length):
    shape = x.shape
    blocks = x.reshape(*shape[:dim], length, shape[dim] // length, *shape[dim + 1 :])
    return jnp.moveaxis(blocks, dim, 0)


def sum_at_owner(x, axis, dim):
    length = lax.axis_size(axis)
    blocks = lax.all_to_all(in_blocks(x, dim, length), axis, 0, 0, tiled=True)
    return jnp.sum(blocks.astype(jnp.float32), axis=0)


def copy_for_each(x, axis):
    length = lax.axis_size(axis)
    return lax.all_to_all(jnp.broadcast_to(x[None], (length, *x.shape)), axis, 0, 0, tiled=True)


def in_order(blocks, dim):
    shape = list(blocks.shape[1:])
    shape[dim] *= blocks.shape[0]
    return jnp.moveaxis(blocks, 0, dim).reshape(shape)


def collect(x, axis, dim):
    blocks = copy_for_each(x, axis)
    return in_order(blocks, dim)


def layer_norm(data, gain):
    center = data - jnp.mean(data, -1, keepdims=True)
    return center * lax.rsqrt(jnp.mean(center * center, -1, keepdims=True) + 1e-05) * gain


def local_span(q_ref, k_ref, v_ref, beta_ref, decay_ref, rate_ref, *refs):
    tables, (both_ref, mix_ref, out_ref), outs = refs[:3], refs[3:6], refs[6:14]
    bufs, part_bufs, sems = refs[14:17], refs[17:21], refs[21]
    copies = [pltpu.make_async_copy(x, y, sems.at[k]) for k, (x, y) in enumerate(zip(tables, bufs))]
    for copy in copies:
        copy.start()
    size = HEAD_FEATURES
    row = lax.broadcasted_iota(jnp.int32, (size, size), 0)
    col = lax.broadcasted_iota(jnp.int32, (size, size), 1)
    eye = row == col
    causal = col <= row

    def to_column(data):
        return jnp.sum(jnp.where(eye, data, 0.0), 1, keepdims=True)

    def to_row(data):
        return jnp.sum(jnp.where(eye, data, 0.0), 0, keepdims=True)

    def dot(a, b, dims=((1,), (0,))):
        return lax.dot_general(
            a.astype(jnp.bfloat16),
            b.astype(jnp.bfloat16),
            (dims, ((), ())),
            preferred_element_type=jnp.float32,
        )

    beta = to_column(jax.nn.sigmoid(beta_ref[...].astype(jnp.float32)))
    logit = decay_ref[...].astype(jnp.float32)
    softplus = jnp.maximum(logit, 0.0) + jnp.log(1.0 + jnp.exp(-jnp.abs(logit)))
    decay = -jnp.exp(jnp.full((1, size), rate_ref[0], jnp.float32)) * softplus
    running = jnp.sum(jnp.where(causal, decay, 0.0), 1, keepdims=True)
    last = jnp.sum(decay, 1, keepdims=True)
    within = jnp.exp(jnp.where(causal, running - to_row(running), -1e30))
    query = q_ref[...].astype(jnp.float32)
    key = k_ref[...].astype(jnp.float32)
    value = v_ref[...].astype(jnp.float32)
    query_scale = lax.rsqrt(jnp.sum(query * query, 1, keepdims=True) + 1e-06) * size ** (-0.5)
    key_scale = lax.rsqrt(jnp.sum(key * key, 1, keepdims=True) + 1e-06)
    key_scale_row = to_row(key_scale)
    across = within * key_scale_row
    lower = jnp.where(
        col < row, dot(k_ref[...], k_ref[...], ((1,), (1,))) * across * (beta * key_scale), 0.0
    )
    scores = dot(q_ref[...], k_ref[...], ((1,), (1,))) * across * query_scale
    differ = row ^ col
    inverse = jnp.where(eye, 1.0, 0.0) - jnp.where(differ == 1, lower, 0.0)
    for level in range(1, 7):
        part = jnp.where((differ >> level) == 1, lower, 0.0)
        inverse = inverse - dot(dot(inverse, part), inverse)
    grown = jnp.exp(running)
    key = key * key_scale
    right = jnp.concatenate([key * (beta * grown), value * beta], 1)
    solved = dot(inverse, right)
    leaving = dot(key * jnp.exp(last - running), solved, ((0,), (0,)))
    passed = jnp.where(eye, jnp.exp(last), 0.0) - leaving[:, :size]
    both_ref[...] = jnp.concatenate([passed, leaving[:, size:]], 0).astype(both_ref.dtype)
    seen = dot(scores, solved)
    mix_ref[...] = query * (query_scale * grown) - seen[:, :size]
    out_ref[...] = seen[:, size:]
    for copy in copies:
        copy.wait()
    pack_parts(*bufs, part_bufs, outs, sems.at[3:])


def run_experts(rows_ref, *refs):
    out_ref, bufs, sems = refs[11], refs[12:23], refs[23]
    copies = [pltpu.make_async_copy(refs[k], bufs[k], sems.at[k]) for k in range(11)]
    gate_ref, up_ref, down_ref = bufs[:3]
    rows = rows_ref[...]
    width = rows.shape[1]
    half, lanes, blocks = (width // 2, LANES // 4, down_ref.shape[0] // LANES)
    size = bufs[7].shape[0]

    def dot(a, b):
        return jnp.dot(a, b, preferred_element_type=jnp.float32)

    copies[0].start()
    copies[1].start()
    copies[0].wait()
    for k in range(3, 11):
        copies[k].start()
    gate = dot(rows, gate_ref[...])
    copies[1].wait()
    copies[2].start()
    inner = (jax.nn.silu(gate) * dot(rows, up_ref[...])).astype(jnp.bfloat16)
    place = lax.broadcasted_iota(jnp.int32, (rows.shape[0], LANES), 1) // lanes
    arrived = [jnp.zeros((rows.shape[0], LANES), jnp.float32)] * blocks

    def run(part, block, first, count):
        last = block == blocks - 1
        ref, row = (bufs[7 + part], first) if last else (bufs[3 + part], block * size + first)
        return ref[row : row + count]

    for part in range(4):
        copies[3 + part].wait()
        copies[7 + part].wait()
        table = jnp.concatenate([run(part, k, 0, half) for k in range(blocks)], 1)
        low, high = (dot(rows[:, :half], table), dot(rows[:, half:], table))
        for k in range(blocks):
            cut = slice(k * LANES, (k + 1) * LANES)
            sums = low[:, cut] + pltpu.roll(high[:, cut], LANES - lanes, 1)
            acts = jax.nn.silu(sums) * pltpu.roll(sums, LANES - 2 * lanes, 1)
            if part > 0:
                acts = pltpu.roll(acts, part * lanes, 1)
            arrived[k] = jnp.where(place == part, acts, arrived[k])
    arrived = jnp.concatenate(arrived, 1).astype(jnp.bfloat16)
    copies[2].wait()

    def down_block(k):
        first = half + k * lanes
        runs = [run(part, block, first, lanes) for block in range(blocks) for part in range(4)]
        return jnp.concatenate(runs, 0)

    for k in range(0, width // LANES, 2):
        cut = slice(k * LANES, (k + 2) * LANES)
        other = jnp.concatenate([down_block(k), down_block(k + 1)], 1)
        out_ref[:, cut] = (dot(inner, down_ref[:, cut]) + dot(arrived, other)).astype(out_ref.dtype)


def per_device(
    residual_in,
    queries,
    keys,
    values,
    out_gate,
    beta_logit,
    decay_logit,
    decay_log,
    head_gain,
    out_weight,
    norm_gain,
    final_gain,
    expert_index,
    route_weights,
    expert_gate,
    expert_up,
    expert_down,
):
    length, width = residual_in.shape

    vmem = pl.BlockSpec(memory_space=pltpu.VMEM)
    anywhere = pl.BlockSpec(memory_space=pl.ANY)
    split_count = lax.axis_size("tp")
    side = round(split_count**0.5)
    tables = (expert_gate[0], expert_up[0], expert_down[0])
    packed = (3 * tables[0].size // 4 // LANES, LANES)
    both, mix, local, *parts = pl.pallas_call(
        local_span,
        out_shape=(
            pltpu.VMEM((2 * HEAD_FEATURES, HEAD_FEATURES), jnp.bfloat16),
            pltpu.VMEM((length, HEAD_FEATURES), jnp.float32),
            pltpu.VMEM((length, HEAD_FEATURES), jnp.float32),
        )
        + (jax.ShapeDtypeStruct((packed[0] - packed[0] // 3, LANES), jnp.bfloat16),) * 4
        + (jax.ShapeDtypeStruct((packed[0] // 3, LANES), jnp.bfloat16),) * 4,
        in_specs=[vmem] * 5 + [pl.BlockSpec(memory_space=pltpu.SMEM)] + [anywhere] * 3,
        out_specs=(vmem,) * 3 + (anywhere,) * 8,
        scratch_shapes=[pltpu.VMEM(x.shape, x.dtype) for x in tables]
        + [pltpu.VMEM(packed, jnp.bfloat16)] * 4
        + [pltpu.SemaphoreType.DMA((15,))],
        name="local_span",
    )(queries, keys, values, beta_logit, decay_logit, decay_log, *tables)
    state, early = entering(both, parts[:4], side)
    mixed = local + mm(mix, state)
    normalized = mixed * lax.rsqrt(jnp.mean(mixed * mixed, -1, keepdims=True) + 1e-06) * head_gain
    gated = (normalized * jax.nn.silu(out_gate.astype(jnp.float32))).astype(jnp.bfloat16)
    expert_count = lax.axis_size(SP) * expert_gate.shape[0]
    rows = length // split_count
    first = lax.axis_index("tp") * rows
    projected = sum_at_owner(
        jnp.dot(gated, out_weight, preferred_element_type=jnp.float32).astype(jnp.bfloat16), "tp", 0
    )
    residual = lax.optimization_barrier(lax.dynamic_slice_in_dim(residual_in, first, rows, 0))
    routes = lax.dynamic_slice_in_dim(expert_index, first, rows, 0)
    weights = lax.dynamic_slice_in_dim(route_weights, first, rows, 0)
    hidden_in = layer_norm(
        residual_scale * residual.astype(jnp.float32) + projected, norm_gain
    ).astype(jnp.bfloat16)
    chips = lax.axis_size(Z)
    table = (routes[:, :, None] == jnp.arange(expert_count, dtype=jnp.int32)).astype(jnp.bfloat16)
    send = jnp.einsum(
        "rs,rd->sd", jnp.sum(table, 1), hidden_in, preferred_element_type=jnp.float32
    ).astype(jnp.bfloat16)

    def along_z(x):
        out = lax.all_to_all(x.reshape(chips, 2, width), Z, 0, 0, tiled=True)
        return out.reshape(chips, 2, width)

    def in_plane(x):
        return lax.all_to_all(x, PLANE, 0, 0, tiled=True)

    half = chips // 2
    send, late = lax.optimization_barrier((send, parts[4:]))
    late = spread(late, side)
    arrived = along_z(send)
    arrived = arrived.transpose(1, 0, 2).reshape(2, 2, half, width)
    swapped = arrived[:, ::-1]
    turns = jnp.stack([arrived, swapped], 1)[:, None, :, None]
    turns = jnp.broadcast_to(turns, (2, side // 2, 2, side // 2, 2, half, width))
    piece = in_plane(turns.reshape(2 * split_count, half, width)).reshape(-1, width)
    tables += tuple(early + late)
    partial_value = pl.pallas_call(
        run_experts,
        out_shape=pltpu.VMEM(piece.shape, jnp.bfloat16),
        in_specs=[vmem] + [anywhere] * 11,
        out_specs=vmem,
        scratch_shapes=[pltpu.VMEM(x.shape, x.dtype) for x in tables]
        + [pltpu.SemaphoreType.DMA((11,))],
        name="run_experts",
    )(held(piece), *tables)
    shares = in_plane(partial_value.reshape(2 * split_count, half, width))
    shares = shares.reshape(2, side // 2, 2, side // 2, 2, half, width).astype(jnp.float32)
    shares = jnp.sum(shares, axis=(1, 3))
    result = jnp.stack([shares[:, 0, 0] + shares[:, 1, 1], shares[:, 0, 1] + shares[:, 1, 0]], 1)
    result = result.reshape(2, chips, width).astype(jnp.bfloat16)
    back = along_z(result.transpose(1, 0, 2)).reshape(expert_count, width)
    gathered = jnp.einsum("rks,sd->rkd", table, back, preferred_element_type=jnp.float32)
    routed = jnp.sum(weights[..., None] * gathered, 1)
    layer_out = layer_norm(
        residual_scale * hidden_in.astype(jnp.float32) + routed, final_gain
    ).astype(jnp.bfloat16)
    layer_out = collect(layer_out, "tp", 0)
    return layer_out


def solution(mesh):
    split = Mesh(
        mesh.devices.reshape(8, 2, 2, mesh.shape["tp"]), ("zh", "zl", "c", "tp")
    )
    placed = (
        P(SP, None),
        P(SP, "tp"),
        P(SP, "tp"),
        P(SP, "tp"),
        P(SP, "tp"),
        P("tp", SP),
        P("tp", SP),
        P("tp"),
        P(),
        P("tp", None),
        P(),
        P(),
        P(SP, None),
        P(SP, None),
        P(SP, None, "tp"),
        P(SP, None, "tp"),
        P(SP, "tp", None),
    )

    return jax.shard_map(per_device, mesh=split, in_specs=placed, out_specs=P(SP, None), check_vma=False)
```

```python
import jax
import jax.numpy as jnp
from jax import lax
from jax.experimental import pallas as pl
from jax.experimental.pallas import tpu as pltpu
from jax.sharding import Mesh
from jax.sharding import PartitionSpec as P


HEAD_FEATURES = 128
LANES = 128
Z = ("zh", "zl")
SP = ("zh", "zl", "c")
PLANE = ("c", "tp")


highest_precision = lax.Precision.HIGHEST
residual_scale = 2.0**0.5


def held(x):
    return pltpu.with_memory_space_constraint(x, pltpu.VMEM)


def mm(a, b):
    return jnp.dot(a, b, precision=highest_precision)


def regroup(lanes):
    row = lax.broadcasted_iota(jnp.int32, (16 * lanes, 16 * lanes), 0)
    col = lax.broadcasted_iota(jnp.int32, (16 * lanes, 16 * lanes), 1)
    row_kind, row_part = (row // (4 * lanes), row // lanes % 4)
    col_part, col_kind = (col // (4 * lanes), col // lanes % 4)
    same = (row_kind == col_kind) & (row_part == col_part) & (row % lanes == col % lanes)
    return jnp.where(same, 1.0, 0.0).astype(jnp.bfloat16)


def pack_parts(gate_ref, up_ref, down_ref, bufs, outs, sems):
    depth, hidden = gate_ref.shape
    half, lanes, blocks = (depth // 2, LANES // 4, hidden // LANES)
    size = bufs[0].shape[0] // blocks
    early = size * (blocks - 1)
    copies = []
    for part, buf in enumerate(bufs):
        for block in range(blocks):
            first = block * LANES + part * lanes
            for k in range(depth // LANES):
                row = block * size + half + k * lanes
                buf[row : row + lanes] = down_ref[first : first + lanes, k * LANES : (k + 1) * LANES]
    order = regroup(lanes)
    for block in range(blocks):
        cut = slice(block * LANES, (block + 1) * LANES)
        kinds = [ref[k : k + half, cut] for ref in (gate_ref, up_ref) for k in (0, half)]
        parts = jnp.dot(jnp.concatenate(kinds, 1), order, preferred_element_type=jnp.float32)
        parts = parts.astype(jnp.bfloat16)
        for part, buf in enumerate(bufs):
            row = block * size
            buf[row : row + half] = parts[:, part * LANES : (part + 1) * LANES]
            late = row == early and part > 1
            out = outs[part + 2] if late else outs[part].at[pl.ds(row, size)]
            copies.append(pltpu.make_async_copy(buf.at[pl.ds(row, size)], out, sems.at[len(copies)]))
            copies[-1].start()
    for copy in copies:
        copy.wait()


def spread(parts, side, start=0):
    out = []
    ways = ((0, 1), (0, side - 1), (1, 0), (side - 1, 0))
    for part, (dy, dx) in zip(parts, ways[start:]):
        pairs = [
            (y * side + x, (y + dy) % side * side + (x + dx) % side)
            for y in range(side)
            for x in range(side)
        ]
        out.append(lax.ppermute(part, "tp", pairs))
    return out


def entering(own, parts, side):
    kind = jnp.bfloat16
    zh, zl, c = (lax.axis_index(axis) for axis in SP)
    near = lax.all_gather(own, ("zl", "c")).astype(jnp.float32)
    width = own.shape[-1]
    map_in, state_in = (jnp.eye(width, dtype=jnp.float32), jnp.zeros((width, width), jnp.float32))
    map_all, state_all = (near[0, :width], near[0, width:])
    for k in range(1, 4):
        inside = k == 2 * zl + c
        map_in = jnp.where(inside, map_all, map_in)
        state_in = jnp.where(inside, state_all, state_in)
        map_k, state_k = (near[k, :width], near[k, width:])
        state_all = mm(map_k, state_all) + state_k
        map_all = mm(map_k, map_all)
    group = jnp.concatenate([map_all, state_all], 0).astype(kind)
    quarter = lax.dynamic_slice_in_dim(group, (2 * zl + c) * (width // 2), width // 2, 0)
    count = lax.axis_size(Z)
    quarter, parts = lax.optimization_barrier((quarter, parts))
    parts = spread(parts, side)
    far = jnp.broadcast_to(quarter[None], (count, *quarter.shape))
    far = lax.all_to_all(far, Z, 0, 0, tiled=True)
    far = lax.all_gather(far, "c")
    far = far.reshape(2, count // 2, 2, width // 2, width).transpose(1, 2, 0, 3, 4)
    far = far.reshape(count // 2, 2 * width, width).astype(jnp.float32)
    state = jnp.zeros((width, width), jnp.float32)
    for k in range(count // 2 - 1):
        state = jnp.where(k < zh, mm(far[k, :width], state) + far[k, width:], state)
    return mm(map_in, state) + state_in, parts


def in_blocks(x, dim, length):
    shape = x.shape
    blocks = x.reshape(*shape[:dim], length, shape[dim] // length, *shape[dim + 1 :])
    return jnp.moveaxis(blocks, dim, 0)


def sum_at_owner(x, axis, dim):
    length = lax.axis_size(axis)
    blocks = lax.all_to_all(in_blocks(x, dim, length), axis, 0, 0, tiled=True)
    return jnp.sum(blocks.astype(jnp.float32), axis=0)


def copy_for_each(x, axis):
    length = lax.axis_size(axis)
    return lax.all_to_all(jnp.broadcast_to(x[None], (length, *x.shape)), axis, 0, 0, tiled=True)


def in_order(blocks, dim):
    shape = list(blocks.shape[1:])
    shape[dim] *= blocks.shape[0]
    return jnp.moveaxis(blocks, 0, dim).reshape(shape)


def collect(x, axis, dim):
    blocks = copy_for_each(x, axis)
    return in_order(blocks, dim)


def layer_norm(data, gain):
    center = data - jnp.mean(data, -1, keepdims=True)
    return center * lax.rsqrt(jnp.mean(center * center, -1, keepdims=True) + 1e-05) * gain


def local_span(q_ref, k_ref, v_ref, beta_ref, decay_ref, rate_ref, *refs):
    tables, (both_ref, mix_ref, out_ref), outs = refs[:3], refs[3:6], refs[6:12]
    bufs, part_bufs, sems = refs[12:15], refs[15:19], refs[19]
    copies = [pltpu.make_async_copy(x, y, sems.at[k]) for k, (x, y) in enumerate(zip(tables, bufs))]
    for copy in copies:
        copy.start()
    size = HEAD_FEATURES
    row = lax.broadcasted_iota(jnp.int32, (size, size), 0)
    col = lax.broadcasted_iota(jnp.int32, (size, size), 1)
    eye = row == col
    causal = col <= row

    def to_column(data):
        return jnp.sum(jnp.where(eye, data, 0.0), 1, keepdims=True)

    def to_row(data):
        return jnp.sum(jnp.where(eye, data, 0.0), 0, keepdims=True)

    def dot(a, b, dims=((1,), (0,))):
        return lax.dot_general(
            a.astype(jnp.bfloat16),
            b.astype(jnp.bfloat16),
            (dims, ((), ())),
            preferred_element_type=jnp.float32,
        )

    beta = to_column(jax.nn.sigmoid(beta_ref[...].astype(jnp.float32)))
    logit = decay_ref[...].astype(jnp.float32)
    softplus = jnp.maximum(logit, 0.0) + jnp.log(1.0 + jnp.exp(-jnp.abs(logit)))
    decay = -jnp.exp(jnp.full((1, size), rate_ref[0], jnp.float32)) * softplus
    running = jnp.sum(jnp.where(causal, decay, 0.0), 1, keepdims=True)
    last = jnp.sum(decay, 1, keepdims=True)
    within = jnp.exp(jnp.where(causal, running - to_row(running), -1e30))
    query = q_ref[...].astype(jnp.float32)
    key = k_ref[...].astype(jnp.float32)
    value = v_ref[...].astype(jnp.float32)
    query_scale = lax.rsqrt(jnp.sum(query * query, 1, keepdims=True) + 1e-06) * size ** (-0.5)
    key_scale = lax.rsqrt(jnp.sum(key * key, 1, keepdims=True) + 1e-06)
    key_scale_row = to_row(key_scale)
    across = within * key_scale_row
    lower = jnp.where(
        col < row, dot(k_ref[...], k_ref[...], ((1,), (1,))) * across * (beta * key_scale), 0.0
    )
    scores = dot(q_ref[...], k_ref[...], ((1,), (1,))) * across * query_scale
    differ = row ^ col
    inverse = jnp.where(eye, 1.0, 0.0) - jnp.where(differ == 1, lower, 0.0)
    for level in range(1, 7):
        part = jnp.where((differ >> level) == 1, lower, 0.0)
        inverse = inverse - dot(dot(inverse, part), inverse)
    grown = jnp.exp(running)
    key = key * key_scale
    right = jnp.concatenate([key * (beta * grown), value * beta], 1)
    solved = dot(inverse, right)
    leaving = dot(key * jnp.exp(last - running), solved, ((0,), (0,)))
    passed = jnp.where(eye, jnp.exp(last), 0.0) - leaving[:, :size]
    both_ref[...] = jnp.concatenate([passed, leaving[:, size:]], 0).astype(both_ref.dtype)
    seen = dot(scores, solved)
    mix_ref[...] = query * (query_scale * grown) - seen[:, :size]
    out_ref[...] = seen[:, size:]
    for copy in copies:
        copy.wait()
    pack_parts(*bufs, part_bufs, outs, sems.at[3:])


def run_experts(rows_ref, *refs):
    out_ref, bufs, sems = refs[9], refs[10:19], refs[19]
    copies = [pltpu.make_async_copy(refs[k], bufs[k], sems.at[k]) for k in range(9)]
    for copy in (*copies[:2], *copies[3:], copies[2]):
        copy.start()
    gate_ref, up_ref, down_ref = bufs[:3]
    rows = rows_ref[...]
    width = rows.shape[1]
    half, lanes, blocks = (width // 2, LANES // 4, down_ref.shape[0] // LANES)
    size = bufs[7].shape[0]

    def dot(a, b):
        return jnp.dot(a, b, preferred_element_type=jnp.float32)

    copies[0].wait()
    gate = dot(rows, gate_ref[...])
    copies[1].wait()
    inner = (jax.nn.silu(gate) * dot(rows, up_ref[...])).astype(jnp.bfloat16)
    place = lax.broadcasted_iota(jnp.int32, (rows.shape[0], LANES), 1) // lanes
    arrived = [jnp.zeros((rows.shape[0], LANES), jnp.float32)] * blocks

    def run(part, block, first, count):
        late = block == blocks - 1 and part > 1
        ref, row = (bufs[5 + part], first) if late else (bufs[3 + part], block * size + first)
        return ref[row : row + count]

    for part in range(4):
        copies[3 + part].wait()
        if part > 1:
            copies[5 + part].wait()
        table = jnp.concatenate([run(part, k, 0, half) for k in range(blocks)], 1)
        low, high = (dot(rows[:, :half], table), dot(rows[:, half:], table))
        for k in range(blocks):
            cut = slice(k * LANES, (k + 1) * LANES)
            sums = low[:, cut] + pltpu.roll(high[:, cut], LANES - lanes, 1)
            acts = jax.nn.silu(sums) * pltpu.roll(sums, LANES - 2 * lanes, 1)
            if part > 0:
                acts = pltpu.roll(acts, part * lanes, 1)
            arrived[k] = jnp.where(place == part, acts, arrived[k])
    arrived = jnp.concatenate(arrived, 1).astype(jnp.bfloat16)
    copies[2].wait()

    def down_block(k):
        first = half + k * lanes
        runs = [run(part, block, first, lanes) for block in range(blocks) for part in range(4)]
        return jnp.concatenate(runs, 0)

    for k in range(0, width // LANES, 2):
        cut = slice(k * LANES, (k + 2) * LANES)
        other = jnp.concatenate([down_block(k), down_block(k + 1)], 1)
        out_ref[:, cut] = (dot(inner, down_ref[:, cut]) + dot(arrived, other)).astype(out_ref.dtype)


def per_device(
    residual_in,
    queries,
    keys,
    values,
    out_gate,
    beta_logit,
    decay_logit,
    decay_log,
    head_gain,
    out_weight,
    norm_gain,
    final_gain,
    expert_index,
    route_weights,
    expert_gate,
    expert_up,
    expert_down,
):
    length, width = residual_in.shape

    vmem = pl.BlockSpec(memory_space=pltpu.VMEM)
    anywhere = pl.BlockSpec(memory_space=pl.ANY)
    split_count = lax.axis_size("tp")
    side = round(split_count**0.5)
    tables = (expert_gate[0], expert_up[0], expert_down[0])
    packed = (3 * tables[0].size // 4 // LANES, LANES)
    both, mix, local, *parts = pl.pallas_call(
        local_span,
        out_shape=(
            pltpu.VMEM((2 * HEAD_FEATURES, HEAD_FEATURES), jnp.bfloat16),
            pltpu.VMEM((length, HEAD_FEATURES), jnp.float32),
            pltpu.VMEM((length, HEAD_FEATURES), jnp.float32),
        )
        + (jax.ShapeDtypeStruct(packed, jnp.bfloat16),) * 2
        + (jax.ShapeDtypeStruct((packed[0] - packed[0] // 3, LANES), jnp.bfloat16),) * 2
        + (jax.ShapeDtypeStruct((packed[0] // 3, LANES), jnp.bfloat16),) * 2,
        in_specs=[vmem] * 5 + [pl.BlockSpec(memory_space=pltpu.SMEM)] + [anywhere] * 3,
        out_specs=(vmem,) * 3 + (anywhere,) * 6,
        scratch_shapes=[pltpu.VMEM(x.shape, x.dtype) for x in tables]
        + [pltpu.VMEM(packed, jnp.bfloat16)] * 4
        + [pltpu.SemaphoreType.DMA((15,))],
        name="local_span",
    )(queries, keys, values, beta_logit, decay_logit, decay_log, *tables)
    state, early = entering(both, parts[:4], side)
    mixed = local + mm(mix, state)
    normalized = mixed * lax.rsqrt(jnp.mean(mixed * mixed, -1, keepdims=True) + 1e-06) * head_gain
    gated = (normalized * jax.nn.silu(out_gate.astype(jnp.float32))).astype(jnp.bfloat16)
    expert_count = lax.axis_size(SP) * expert_gate.shape[0]
    rows = length // split_count
    first = lax.axis_index("tp") * rows
    projected = sum_at_owner(
        jnp.dot(gated, out_weight, preferred_element_type=jnp.float32).astype(jnp.bfloat16), "tp", 0
    )
    residual = lax.optimization_barrier(lax.dynamic_slice_in_dim(residual_in, first, rows, 0))
    routes = lax.dynamic_slice_in_dim(expert_index, first, rows, 0)
    weights = lax.dynamic_slice_in_dim(route_weights, first, rows, 0)
    hidden_in = layer_norm(
        residual_scale * residual.astype(jnp.float32) + projected, norm_gain
    ).astype(jnp.bfloat16)
    chips = lax.axis_size(Z)
    table = (routes[:, :, None] == jnp.arange(expert_count, dtype=jnp.int32)).astype(jnp.bfloat16)
    send = jnp.einsum(
        "rs,rd->sd", jnp.sum(table, 1), hidden_in, preferred_element_type=jnp.float32
    ).astype(jnp.bfloat16)

    def along_z(x):
        out = lax.all_to_all(x.reshape(chips, 2, width), Z, 0, 0, tiled=True)
        return out.reshape(chips, 2, width)

    def in_plane(x):
        return lax.all_to_all(x, PLANE, 0, 0, tiled=True)

    half = chips // 2
    send, late = lax.optimization_barrier((send, parts[4:]))
    late = spread(late, side, 2)
    arrived = along_z(send)
    arrived = arrived.transpose(1, 0, 2).reshape(2, 2, half, width)
    swapped = arrived[:, ::-1]
    turns = jnp.stack([arrived, swapped], 1)[:, None, :, None]
    turns = jnp.broadcast_to(turns, (2, side // 2, 2, side // 2, 2, half, width))
    piece = in_plane(turns.reshape(2 * split_count, half, width)).reshape(-1, width)
    tables += tuple(early + late)
    partial_value = pl.pallas_call(
        run_experts,
        out_shape=pltpu.VMEM(piece.shape, jnp.bfloat16),
        in_specs=[vmem] + [anywhere] * 9,
        out_specs=vmem,
        scratch_shapes=[pltpu.VMEM(x.shape, x.dtype) for x in tables]
        + [pltpu.SemaphoreType.DMA((9,))],
        name="run_experts",
    )(held(piece), *tables)
    shares = in_plane(partial_value.reshape(2 * split_count, half, width))
    shares = shares.reshape(2, side // 2, 2, side // 2, 2, half, width).astype(jnp.float32)
    shares = jnp.sum(shares, axis=(1, 3))
    result = jnp.stack([shares[:, 0, 0] + shares[:, 1, 1], shares[:, 0, 1] + shares[:, 1, 0]], 1)
    result = result.reshape(2, chips, width).astype(jnp.bfloat16)
    back = along_z(result.transpose(1, 0, 2)).reshape(expert_count, width)
    gathered = jnp.einsum("rks,sd->rkd", table, back, preferred_element_type=jnp.float32)
    routed = jnp.sum(weights[..., None] * gathered, 1)
    layer_out = layer_norm(
        residual_scale * hidden_in.astype(jnp.float32) + routed, final_gain
    ).astype(jnp.bfloat16)
    layer_out = collect(layer_out, "tp", 0)
    return layer_out


def solution(mesh):
    split = Mesh(
        mesh.devices.reshape(8, 2, 2, mesh.shape["tp"]), ("zh", "zl", "c", "tp")
    )
    placed = (
        P(SP, None),
        P(SP, "tp"),
        P(SP, "tp"),
        P(SP, "tp"),
        P(SP, "tp"),
        P("tp", SP),
        P("tp", SP),
        P("tp"),
        P(),
        P("tp", None),
        P(),
        P(),
        P(SP, None),
        P(SP, None),
        P(SP, None, "tp"),
        P(SP, None, "tp"),
        P(SP, "tp", None),
    )

    return jax.shard_map(per_device, mesh=split, in_specs=placed, out_specs=P(SP, None), check_vma=False)
```

```python
import jax
import jax.numpy as jnp
from jax import lax
from jax.experimental import pallas as pl
from jax.experimental.pallas import tpu as pltpu
from jax.sharding import Mesh
from jax.sharding import PartitionSpec as P


HEAD_FEATURES = 128
LANES = 128
Z = ("zh", "zl")
SP = ("zh", "zl", "c")
PLANE = ("c", "tp")


highest_precision = lax.Precision.HIGHEST
residual_scale = 2.0**0.5


def held(x):
    return pltpu.with_memory_space_constraint(x, pltpu.VMEM)


def mm(a, b):
    return jnp.dot(a, b, precision=highest_precision)


def regroup(lanes):
    row = lax.broadcasted_iota(jnp.int32, (16 * lanes, 16 * lanes), 0)
    col = lax.broadcasted_iota(jnp.int32, (16 * lanes, 16 * lanes), 1)
    row_kind, row_part = (row // (4 * lanes), row // lanes % 4)
    col_part, col_kind = (col // (4 * lanes), col // lanes % 4)
    same = (row_kind == col_kind) & (row_part == col_part) & (row % lanes == col % lanes)
    return jnp.where(same, 1.0, 0.0).astype(jnp.bfloat16)


def pack_parts(gate_ref, up_ref, down_ref, bufs, outs, sems):
    depth, hidden = gate_ref.shape
    half, lanes, blocks = (depth // 2, LANES // 4, hidden // LANES)
    size = bufs[0].shape[0] // blocks
    early = size * (blocks - 1)
    copies = []
    for part, buf in enumerate(bufs):
        for block in range(blocks):
            first = block * LANES + part * lanes
            for k in range(depth // LANES):
                row = block * size + half + k * lanes
                buf[row : row + lanes] = down_ref[first : first + lanes, k * LANES : (k + 1) * LANES]
    order = regroup(lanes)
    for block in range(blocks):
        cut = slice(block * LANES, (block + 1) * LANES)
        kinds = [ref[k : k + half, cut] for ref in (gate_ref, up_ref) for k in (0, half)]
        parts = jnp.dot(jnp.concatenate(kinds, 1), order, preferred_element_type=jnp.float32)
        parts = parts.astype(jnp.bfloat16)
        for part, buf in enumerate(bufs):
            row = block * size
            buf[row : row + half] = parts[:, part * LANES : (part + 1) * LANES]
            late = row == early and part > 1
            out = outs[part + 2] if late else outs[part].at[pl.ds(row, size)]
            copies.append(pltpu.make_async_copy(buf.at[pl.ds(row, size)], out, sems.at[len(copies)]))
            copies[-1].start()
    for copy in copies:
        copy.wait()


def spread(parts, side, start=0):
    out = []
    ways = ((0, 1), (0, side - 1), (1, 0), (side - 1, 0))
    for part, (dy, dx) in zip(parts, ways[start:]):
        pairs = [
            (y * side + x, (y + dy) % side * side + (x + dx) % side)
            for y in range(side)
            for x in range(side)
        ]
        out.append(lax.ppermute(part, "tp", pairs))
    return out


def entering(own, parts, side):
    kind = jnp.bfloat16
    zh, zl, c = (lax.axis_index(axis) for axis in SP)
    near = lax.all_gather(own, ("zl", "c")).astype(jnp.float32)
    width = own.shape[-1]
    map_in, state_in = (jnp.eye(width, dtype=jnp.float32), jnp.zeros((width, width), jnp.float32))
    map_all, state_all = (near[0, :width], near[0, width:])
    for k in range(1, 4):
        inside = k == 2 * zl + c
        map_in = jnp.where(inside, map_all, map_in)
        state_in = jnp.where(inside, state_all, state_in)
        map_k, state_k = (near[k, :width], near[k, width:])
        state_all = mm(map_k, state_all) + state_k
        map_all = mm(map_k, map_all)
    group = jnp.concatenate([map_all, state_all], 0).astype(kind)
    quarter = lax.dynamic_slice_in_dim(group, (2 * zl + c) * (width // 2), width // 2, 0)
    count = lax.axis_size(Z)
    quarter, parts = lax.optimization_barrier((quarter, parts))
    parts = spread(parts, side)
    far = jnp.broadcast_to(quarter[None], (count, *quarter.shape))
    far = lax.all_to_all(far, Z, 0, 0, tiled=True)
    far = lax.all_gather(far, "c")
    far = far.reshape(2, count // 2, 2, width // 2, width).transpose(1, 2, 0, 3, 4)
    far = far.reshape(count // 2, 2 * width, width).astype(jnp.float32)
    state = jnp.zeros((width, width), jnp.float32)
    for k in range(count // 2 - 1):
        state = jnp.where(k < zh, mm(far[k, :width], state) + far[k, width:], state)
    return mm(map_in, state) + state_in, parts


def in_blocks(x, dim, length):
    shape = x.shape
    blocks = x.reshape(*shape[:dim], length, shape[dim] // length, *shape[dim + 1 :])
    return jnp.moveaxis(blocks, dim, 0)


def copy_for_each(x, axis):
    length = lax.axis_size(axis)
    return lax.all_to_all(jnp.broadcast_to(x[None], (length, *x.shape)), axis, 0, 0, tiled=True)


def in_order(blocks, dim):
    shape = list(blocks.shape[1:])
    shape[dim] *= blocks.shape[0]
    return jnp.moveaxis(blocks, 0, dim).reshape(shape)


def collect(x, axis, dim):
    blocks = copy_for_each(x, axis)
    return in_order(blocks, dim)


def layer_norm(data, gain):
    center = data - jnp.mean(data, -1, keepdims=True)
    return center * lax.rsqrt(jnp.mean(center * center, -1, keepdims=True) + 1e-05) * gain


def local_span(q_ref, k_ref, v_ref, beta_ref, decay_ref, rate_ref, *refs):
    tables, (both_ref, mix_ref, out_ref), outs = refs[:3], refs[3:6], refs[6:12]
    bufs, part_bufs, sems = refs[12:15], refs[15:19], refs[19]
    copies = [pltpu.make_async_copy(x, y, sems.at[k]) for k, (x, y) in enumerate(zip(tables, bufs))]
    for copy in copies:
        copy.start()
    size = HEAD_FEATURES
    row = lax.broadcasted_iota(jnp.int32, (size, size), 0)
    col = lax.broadcasted_iota(jnp.int32, (size, size), 1)
    eye = row == col
    causal = col <= row

    def to_column(data):
        return jnp.sum(jnp.where(eye, data, 0.0), 1, keepdims=True)

    def to_row(data):
        return jnp.sum(jnp.where(eye, data, 0.0), 0, keepdims=True)

    def dot(a, b, dims=((1,), (0,))):
        return lax.dot_general(
            a.astype(jnp.bfloat16),
            b.astype(jnp.bfloat16),
            (dims, ((), ())),
            preferred_element_type=jnp.float32,
        )

    beta = to_column(jax.nn.sigmoid(beta_ref[...].astype(jnp.float32)))
    logit = decay_ref[...].astype(jnp.float32)
    softplus = jnp.maximum(logit, 0.0) + jnp.log(1.0 + jnp.exp(-jnp.abs(logit)))
    decay = -jnp.exp(jnp.full((1, size), rate_ref[0], jnp.float32)) * softplus
    running = jnp.sum(jnp.where(causal, decay, 0.0), 1, keepdims=True)
    last = jnp.sum(decay, 1, keepdims=True)
    within = jnp.exp(jnp.where(causal, running - to_row(running), -1e30))
    query = q_ref[...].astype(jnp.float32)
    key = k_ref[...].astype(jnp.float32)
    value = v_ref[...].astype(jnp.float32)
    query_scale = lax.rsqrt(jnp.sum(query * query, 1, keepdims=True) + 1e-06) * size ** (-0.5)
    key_scale = lax.rsqrt(jnp.sum(key * key, 1, keepdims=True) + 1e-06)
    key_scale_row = to_row(key_scale)
    across = within * key_scale_row
    lower = jnp.where(
        col < row, dot(k_ref[...], k_ref[...], ((1,), (1,))) * across * (beta * key_scale), 0.0
    )
    scores = dot(q_ref[...], k_ref[...], ((1,), (1,))) * across * query_scale
    differ = row ^ col
    inverse = jnp.where(eye, 1.0, 0.0) - jnp.where(differ == 1, lower, 0.0)
    for level in range(1, 7):
        part = jnp.where((differ >> level) == 1, lower, 0.0)
        inverse = inverse - dot(dot(inverse, part), inverse)
    grown = jnp.exp(running)
    key = key * key_scale
    right = jnp.concatenate([key * (beta * grown), value * beta], 1)
    solved = dot(inverse, right)
    leaving = dot(key * jnp.exp(last - running), solved, ((0,), (0,)))
    passed = jnp.where(eye, jnp.exp(last), 0.0) - leaving[:, :size]
    both_ref[...] = jnp.concatenate([passed, leaving[:, size:]], 0).astype(both_ref.dtype)
    seen = dot(scores, solved)
    mix_ref[...] = query * (query_scale * grown) - seen[:, :size]
    out_ref[...] = seen[:, size:]
    for copy in copies:
        copy.wait()
    pack_parts(*bufs, part_bufs, outs, sems.at[3:])


def run_experts(rows_ref, *refs):
    out_ref, bufs, sems = refs[9], refs[10:19], refs[19]
    copies = [pltpu.make_async_copy(refs[k], bufs[k], sems.at[k]) for k in range(9)]
    for copy in (*copies[:2], *copies[3:], copies[2]):
        copy.start()
    gate_ref, up_ref, down_ref = bufs[:3]
    rows = rows_ref[...]
    width = rows.shape[1]
    half, lanes, blocks = (width // 2, LANES // 4, down_ref.shape[0] // LANES)
    size = bufs[7].shape[0]

    def dot(a, b):
        return jnp.dot(a, b, preferred_element_type=jnp.float32)

    copies[0].wait()
    gate = dot(rows, gate_ref[...])
    copies[1].wait()
    inner = (jax.nn.silu(gate) * dot(rows, up_ref[...])).astype(jnp.bfloat16)
    place = lax.broadcasted_iota(jnp.int32, (rows.shape[0], LANES), 1) // lanes
    arrived = [jnp.zeros((rows.shape[0], LANES), jnp.float32)] * blocks

    def run(part, block, first, count):
        late = block == blocks - 1 and part > 1
        ref, row = (bufs[5 + part], first) if late else (bufs[3 + part], block * size + first)
        return ref[row : row + count]

    for part in range(4):
        copies[3 + part].wait()
        if part > 1:
            copies[5 + part].wait()
        table = jnp.concatenate([run(part, k, 0, half) for k in range(blocks)], 1)
        low, high = (dot(rows[:, :half], table), dot(rows[:, half:], table))
        for k in range(blocks):
            cut = slice(k * LANES, (k + 1) * LANES)
            sums = low[:, cut] + pltpu.roll(high[:, cut], LANES - lanes, 1)
            acts = jax.nn.silu(sums) * pltpu.roll(sums, LANES - 2 * lanes, 1)
            if part > 0:
                acts = pltpu.roll(acts, part * lanes, 1)
            arrived[k] = jnp.where(place == part, acts, arrived[k])
    arrived = jnp.concatenate(arrived, 1).astype(jnp.bfloat16)
    copies[2].wait()

    def down_block(k):
        first = half + k * lanes
        runs = [run(part, block, first, lanes) for block in range(blocks) for part in range(4)]
        return jnp.concatenate(runs, 0)

    for k in range(0, width // LANES, 2):
        cut = slice(k * LANES, (k + 2) * LANES)
        other = jnp.concatenate([down_block(k), down_block(k + 1)], 1)
        out_ref[:, cut] = (dot(inner, down_ref[:, cut]) + dot(arrived, other)).astype(out_ref.dtype)


def per_device(
    residual_in,
    queries,
    keys,
    values,
    out_gate,
    beta_logit,
    decay_logit,
    decay_log,
    head_gain,
    out_weight,
    norm_gain,
    final_gain,
    expert_index,
    route_weights,
    expert_gate,
    expert_up,
    expert_down,
):
    length, width = residual_in.shape

    vmem = pl.BlockSpec(memory_space=pltpu.VMEM)
    anywhere = pl.BlockSpec(memory_space=pl.ANY)
    split_count = lax.axis_size("tp")
    side = round(split_count**0.5)
    tables = (expert_gate[0], expert_up[0], expert_down[0])
    packed = (3 * tables[0].size // 4 // LANES, LANES)
    both, mix, local, *parts = pl.pallas_call(
        local_span,
        out_shape=(
            pltpu.VMEM((2 * HEAD_FEATURES, HEAD_FEATURES), jnp.bfloat16),
            pltpu.VMEM((length, HEAD_FEATURES), jnp.float32),
            pltpu.VMEM((length, HEAD_FEATURES), jnp.float32),
        )
        + (jax.ShapeDtypeStruct(packed, jnp.bfloat16),) * 2
        + (jax.ShapeDtypeStruct((packed[0] - packed[0] // 3, LANES), jnp.bfloat16),) * 2
        + (jax.ShapeDtypeStruct((packed[0] // 3, LANES), jnp.bfloat16),) * 2,
        in_specs=[vmem] * 5 + [pl.BlockSpec(memory_space=pltpu.SMEM)] + [anywhere] * 3,
        out_specs=(vmem,) * 3 + (anywhere,) * 6,
        scratch_shapes=[pltpu.VMEM(x.shape, x.dtype) for x in tables]
        + [pltpu.VMEM(packed, jnp.bfloat16)] * 4
        + [pltpu.SemaphoreType.DMA((15,))],
        name="local_span",
    )(queries, keys, values, beta_logit, decay_logit, decay_log, *tables)
    state, early = entering(both, parts[:4], side)
    mixed = local + mm(mix, state)
    normalized = mixed * lax.rsqrt(jnp.mean(mixed * mixed, -1, keepdims=True) + 1e-06) * head_gain
    gated = (normalized * jax.nn.silu(out_gate.astype(jnp.float32))).astype(jnp.bfloat16)
    expert_count = lax.axis_size(SP) * expert_gate.shape[0]
    rows = length // split_count
    first = lax.axis_index("tp") * rows
    product = jnp.dot(gated, out_weight, preferred_element_type=jnp.float32).astype(jnp.bfloat16)
    product, late = lax.optimization_barrier((product, parts[4:]))
    late = spread(late, side, 2)
    product = lax.all_to_all(in_blocks(product, 0, split_count), "tp", 0, 0, tiled=True)
    projected = jnp.sum(product.astype(jnp.float32), axis=0)
    residual = lax.optimization_barrier(lax.dynamic_slice_in_dim(residual_in, first, rows, 0))
    routes = lax.dynamic_slice_in_dim(expert_index, first, rows, 0)
    weights = lax.dynamic_slice_in_dim(route_weights, first, rows, 0)
    hidden_in = layer_norm(
        residual_scale * residual.astype(jnp.float32) + projected, norm_gain
    ).astype(jnp.bfloat16)
    chips = lax.axis_size(Z)
    table = (routes[:, :, None] == jnp.arange(expert_count, dtype=jnp.int32)).astype(jnp.bfloat16)
    send = jnp.einsum(
        "rs,rd->sd", jnp.sum(table, 1), hidden_in, preferred_element_type=jnp.float32
    ).astype(jnp.bfloat16)

    def along_z(x):
        out = lax.all_to_all(x.reshape(chips, 2, width), Z, 0, 0, tiled=True)
        return out.reshape(chips, 2, width)

    def in_plane(x):
        return lax.all_to_all(x, PLANE, 0, 0, tiled=True)

    half = chips // 2
    arrived = lax.all_to_all(send.reshape(chips, 16, width // 8), Z, 0, 0, tiled=True)
    arrived = arrived.reshape(chips, 2, width).transpose(1, 0, 2).reshape(2, 2, half, width)
    swapped = arrived[:, ::-1]
    turns = jnp.stack([arrived, swapped], 1)[:, None, :, None]
    turns = jnp.broadcast_to(turns, (2, side // 2, 2, side // 2, 2, half, width))
    piece = in_plane(turns.reshape(2 * split_count, half, width)).reshape(-1, width)
    tables += tuple(early + late)
    partial_value = pl.pallas_call(
        run_experts,
        out_shape=pltpu.VMEM(piece.shape, jnp.bfloat16),
        in_specs=[vmem] + [anywhere] * 9,
        out_specs=vmem,
        scratch_shapes=[pltpu.VMEM(x.shape, x.dtype) for x in tables]
        + [pltpu.SemaphoreType.DMA((9,))],
        name="run_experts",
    )(held(piece), *tables)
    shares = in_plane(partial_value.reshape(2 * split_count, half, width))
    shares = shares.reshape(2, side // 2, 2, side // 2, 2, half, width).astype(jnp.float32)
    shares = jnp.sum(shares, axis=(1, 3))
    result = jnp.stack([shares[:, 0, 0] + shares[:, 1, 1], shares[:, 0, 1] + shares[:, 1, 0]], 1)
    result = result.reshape(2, chips, width).astype(jnp.bfloat16)
    back = along_z(result.transpose(1, 0, 2)).reshape(expert_count, width)
    gathered = jnp.einsum("rks,sd->rkd", table, back, preferred_element_type=jnp.float32)
    routed = jnp.sum(weights[..., None] * gathered, 1)
    layer_out = layer_norm(
        residual_scale * hidden_in.astype(jnp.float32) + routed, final_gain
    ).astype(jnp.bfloat16)
    layer_out = collect(layer_out, "tp", 0)
    return layer_out


def solution(mesh):
    split = Mesh(
        mesh.devices.reshape(8, 2, 2, mesh.shape["tp"]), ("zh", "zl", "c", "tp")
    )
    placed = (
        P(SP, None),
        P(SP, "tp"),
        P(SP, "tp"),
        P(SP, "tp"),
        P(SP, "tp"),
        P("tp", SP),
        P("tp", SP),
        P("tp"),
        P(),
        P("tp", None),
        P(),
        P(),
        P(SP, None),
        P(SP, None),
        P(SP, None, "tp"),
        P(SP, None, "tp"),
        P(SP, "tp", None),
    )

    return jax.shard_map(per_device, mesh=split, in_specs=placed, out_specs=P(SP, None), check_vma=False)
```

```python
import jax
import jax.numpy as jnp
from jax import lax
from jax.experimental import pallas as pl
from jax.experimental.pallas import tpu as pltpu
from jax.sharding import Mesh
from jax.sharding import PartitionSpec as P


HEAD_FEATURES = 128
LANES = 128
Z = ("zh", "zl")
SP = ("zh", "zl", "c")
PLANE = ("c", "tp")


highest_precision = lax.Precision.HIGHEST
residual_scale = 2.0**0.5


def held(x):
    return pltpu.with_memory_space_constraint(x, pltpu.VMEM)


def mm(a, b):
    return jnp.dot(a, b, precision=highest_precision)


def regroup(lanes):
    row = lax.broadcasted_iota(jnp.int32, (16 * lanes, 16 * lanes), 0)
    col = lax.broadcasted_iota(jnp.int32, (16 * lanes, 16 * lanes), 1)
    row_kind, row_part = (row // (4 * lanes), row // lanes % 4)
    col_part, col_kind = (col // (4 * lanes), col // lanes % 4)
    same = (row_kind == col_kind) & (row_part == col_part) & (row % lanes == col % lanes)
    return jnp.where(same, 1.0, 0.0).astype(jnp.bfloat16)


def pack_parts(gate_ref, up_ref, down_ref, bufs, outs, sems):
    depth, hidden = gate_ref.shape
    half, lanes, blocks = (depth // 2, LANES // 4, hidden // LANES)
    size = bufs[0].shape[0] // blocks
    copies = []
    for part, buf in enumerate(bufs):
        for block in range(blocks):
            first = block * LANES + part * lanes
            for k in range(depth // LANES):
                row = block * size + half + k * lanes
                buf[row : row + lanes] = down_ref[first : first + lanes, k * LANES : (k + 1) * LANES]
    order = regroup(lanes)
    for block in range(blocks):
        cut = slice(block * LANES, (block + 1) * LANES)
        kinds = [ref[k : k + half, cut] for ref in (gate_ref, up_ref) for k in (0, half)]
        parts = jnp.dot(jnp.concatenate(kinds, 1), order, preferred_element_type=jnp.float32)
        parts = parts.astype(jnp.bfloat16)
        for part, buf in enumerate(bufs):
            row = block * size
            buf[row : row + half] = parts[:, part * LANES : (part + 1) * LANES]
            run = pl.ds(row, size)
            copies.append(pltpu.make_async_copy(buf.at[run], outs[part].at[run], sems.at[len(copies)]))
            copies[-1].start()
    for copy in copies:
        copy.wait()


def spread(parts, side, start=0):
    out = []
    ways = ((0, 1), (0, side - 1), (1, 0), (side - 1, 0))
    for part, (dy, dx) in zip(parts, ways[start:]):
        pairs = [
            (y * side + x, (y + dy) % side * side + (x + dx) % side)
            for y in range(side)
            for x in range(side)
        ]
        out.append(lax.ppermute(part, "tp", pairs))
    return out


def entering(own, parts, side):
    kind = jnp.bfloat16
    zh, zl, c = (lax.axis_index(axis) for axis in SP)
    near = lax.all_gather(own, ("zl", "c")).astype(jnp.float32)
    width = own.shape[-1]
    map_in, state_in = (jnp.eye(width, dtype=jnp.float32), jnp.zeros((width, width), jnp.float32))
    map_all, state_all = (near[0, :width], near[0, width:])
    for k in range(1, 4):
        inside = k == 2 * zl + c
        map_in = jnp.where(inside, map_all, map_in)
        state_in = jnp.where(inside, state_all, state_in)
        map_k, state_k = (near[k, :width], near[k, width:])
        state_all = mm(map_k, state_all) + state_k
        map_all = mm(map_k, map_all)
    group = jnp.concatenate([map_all, state_all], 0).astype(kind)
    quarter = lax.dynamic_slice_in_dim(group, (2 * zl + c) * (width // 2), width // 2, 0)
    count = lax.axis_size(Z)
    quarter, parts = lax.optimization_barrier((quarter, parts))
    parts = spread(parts, side)
    far = jnp.broadcast_to(quarter[None], (count, *quarter.shape))
    far = lax.all_to_all(far, Z, 0, 0, tiled=True)
    far = lax.all_gather(far, "c")
    far = far.reshape(2, count // 2, 2, width // 2, width).transpose(1, 2, 0, 3, 4)
    far = far.reshape(count // 2, 2 * width, width).astype(jnp.float32)
    state = jnp.zeros((width, width), jnp.float32)
    for k in range(count // 2 - 1):
        state = jnp.where(k < zh, mm(far[k, :width], state) + far[k, width:], state)
    return mm(map_in, state) + state_in, parts


def in_blocks(x, dim, length):
    shape = x.shape
    blocks = x.reshape(*shape[:dim], length, shape[dim] // length, *shape[dim + 1 :])
    return jnp.moveaxis(blocks, dim, 0)


def copy_for_each(x, axis):
    length = lax.axis_size(axis)
    return lax.all_to_all(jnp.broadcast_to(x[None], (length, *x.shape)), axis, 0, 0, tiled=True)


def in_order(blocks, dim):
    shape = list(blocks.shape[1:])
    shape[dim] *= blocks.shape[0]
    return jnp.moveaxis(blocks, 0, dim).reshape(shape)


def collect(x, axis, dim):
    blocks = copy_for_each(x, axis)
    return in_order(blocks, dim)


def layer_norm(data, gain):
    center = data - jnp.mean(data, -1, keepdims=True)
    return center * lax.rsqrt(jnp.mean(center * center, -1, keepdims=True) + 1e-05) * gain


def local_span(q_ref, k_ref, v_ref, beta_ref, decay_ref, rate_ref, *refs):
    tables, (both_ref, mix_ref, out_ref), outs = refs[:3], refs[3:6], refs[6:10]
    bufs, part_bufs, sems = refs[10:13], refs[13:17], refs[17]
    copies = [pltpu.make_async_copy(x, y, sems.at[k]) for k, (x, y) in enumerate(zip(tables, bufs))]
    for copy in copies:
        copy.start()
    size = HEAD_FEATURES
    row = lax.broadcasted_iota(jnp.int32, (size, size), 0)
    col = lax.broadcasted_iota(jnp.int32, (size, size), 1)
    eye = row == col
    causal = col <= row

    def to_column(data):
        return jnp.sum(jnp.where(eye, data, 0.0), 1, keepdims=True)

    def to_row(data):
        return jnp.sum(jnp.where(eye, data, 0.0), 0, keepdims=True)

    def dot(a, b, dims=((1,), (0,))):
        return lax.dot_general(
            a.astype(jnp.bfloat16),
            b.astype(jnp.bfloat16),
            (dims, ((), ())),
            preferred_element_type=jnp.float32,
        )

    beta = to_column(jax.nn.sigmoid(beta_ref[...].astype(jnp.float32)))
    logit = decay_ref[...].astype(jnp.float32)
    softplus = jnp.maximum(logit, 0.0) + jnp.log(1.0 + jnp.exp(-jnp.abs(logit)))
    decay = -jnp.exp(jnp.full((1, size), rate_ref[0], jnp.float32)) * softplus
    running = jnp.sum(jnp.where(causal, decay, 0.0), 1, keepdims=True)
    last = jnp.sum(decay, 1, keepdims=True)
    within = jnp.exp(jnp.where(causal, running - to_row(running), -1e30))
    query = q_ref[...].astype(jnp.float32)
    key = k_ref[...].astype(jnp.float32)
    value = v_ref[...].astype(jnp.float32)
    query_scale = lax.rsqrt(jnp.sum(query * query, 1, keepdims=True) + 1e-06) * size ** (-0.5)
    key_scale = lax.rsqrt(jnp.sum(key * key, 1, keepdims=True) + 1e-06)
    key_scale_row = to_row(key_scale)
    across = within * key_scale_row
    lower = jnp.where(
        col < row, dot(k_ref[...], k_ref[...], ((1,), (1,))) * across * (beta * key_scale), 0.0
    )
    scores = dot(q_ref[...], k_ref[...], ((1,), (1,))) * across * query_scale
    differ = row ^ col
    inverse = jnp.where(eye, 1.0, 0.0) - jnp.where(differ == 1, lower, 0.0)
    for level in range(1, 7):
        part = jnp.where((differ >> level) == 1, lower, 0.0)
        inverse = inverse - dot(dot(inverse, part), inverse)
    grown = jnp.exp(running)
    key = key * key_scale
    right = jnp.concatenate([key * (beta * grown), value * beta], 1)
    solved = dot(inverse, right)
    leaving = dot(key * jnp.exp(last - running), solved, ((0,), (0,)))
    passed = jnp.where(eye, jnp.exp(last), 0.0) - leaving[:, :size]
    both_ref[...] = jnp.concatenate([passed, leaving[:, size:]], 0).astype(both_ref.dtype)
    seen = dot(scores, solved)
    mix_ref[...] = query * (query_scale * grown) - seen[:, :size]
    out_ref[...] = seen[:, size:]
    for copy in copies:
        copy.wait()
    pack_parts(*bufs, part_bufs, outs, sems.at[3:])


def run_experts(rows_ref, *refs):
    out_ref, bufs, sems = refs[7], refs[8:15], refs[15]
    copies = [pltpu.make_async_copy(refs[k], bufs[k], sems.at[k]) for k in range(7)]
    for copy in (*copies[:2], *copies[3:], copies[2]):
        copy.start()
    gate_ref, up_ref, down_ref = bufs[:3]
    rows = rows_ref[...]
    width = rows.shape[1]
    half, lanes, blocks = (width // 2, LANES // 4, down_ref.shape[0] // LANES)
    size = bufs[3].shape[0] // blocks

    def dot(a, b):
        return jnp.dot(a, b, preferred_element_type=jnp.float32)

    copies[0].wait()
    gate = dot(rows, gate_ref[...])
    copies[1].wait()
    inner = (jax.nn.silu(gate) * dot(rows, up_ref[...])).astype(jnp.bfloat16)
    place = lax.broadcasted_iota(jnp.int32, (rows.shape[0], LANES), 1) // lanes
    arrived = [jnp.zeros((rows.shape[0], LANES), jnp.float32)] * blocks

    def run(part, block, first, count):
        row = block * size + first
        return bufs[3 + part][row : row + count]

    for part in range(4):
        copies[3 + part].wait()
        table = jnp.concatenate([run(part, k, 0, half) for k in range(blocks)], 1)
        low, high = (dot(rows[:, :half], table), dot(rows[:, half:], table))
        for k in range(blocks):
            cut = slice(k * LANES, (k + 1) * LANES)
            sums = low[:, cut] + pltpu.roll(high[:, cut], LANES - lanes, 1)
            acts = jax.nn.silu(sums) * pltpu.roll(sums, LANES - 2 * lanes, 1)
            if part > 0:
                acts = pltpu.roll(acts, part * lanes, 1)
            arrived[k] = jnp.where(place == part, acts, arrived[k])
    arrived = jnp.concatenate(arrived, 1).astype(jnp.bfloat16)
    copies[2].wait()

    def down_block(k):
        first = half + k * lanes
        runs = [run(part, block, first, lanes) for block in range(blocks) for part in range(4)]
        return jnp.concatenate(runs, 0)

    for k in range(0, width // LANES, 2):
        cut = slice(k * LANES, (k + 2) * LANES)
        other = jnp.concatenate([down_block(k), down_block(k + 1)], 1)
        out_ref[:, cut] = (dot(inner, down_ref[:, cut]) + dot(arrived, other)).astype(out_ref.dtype)


def per_device(
    residual_in,
    queries,
    keys,
    values,
    out_gate,
    beta_logit,
    decay_logit,
    decay_log,
    head_gain,
    out_weight,
    norm_gain,
    final_gain,
    expert_index,
    route_weights,
    expert_gate,
    expert_up,
    expert_down,
):
    length, width = residual_in.shape

    vmem = pl.BlockSpec(memory_space=pltpu.VMEM)
    anywhere = pl.BlockSpec(memory_space=pl.ANY)
    split_count = lax.axis_size("tp")
    side = round(split_count**0.5)
    tables = (expert_gate[0], expert_up[0], expert_down[0])
    packed = (3 * tables[0].size // 4 // LANES, LANES)
    both, mix, local, *parts = pl.pallas_call(
        local_span,
        out_shape=(
            pltpu.VMEM((2 * HEAD_FEATURES, HEAD_FEATURES), jnp.bfloat16),
            pltpu.VMEM((length, HEAD_FEATURES), jnp.float32),
            pltpu.VMEM((length, HEAD_FEATURES), jnp.float32),
        )
        + (jax.ShapeDtypeStruct(packed, jnp.bfloat16),) * 4,
        in_specs=[vmem] * 5 + [pl.BlockSpec(memory_space=pltpu.SMEM)] + [anywhere] * 3,
        out_specs=(vmem,) * 3 + (anywhere,) * 4,
        scratch_shapes=[pltpu.VMEM(x.shape, x.dtype) for x in tables]
        + [pltpu.VMEM(packed, jnp.bfloat16)] * 4
        + [pltpu.SemaphoreType.DMA((15,))],
        name="local_span",
    )(queries, keys, values, beta_logit, decay_logit, decay_log, *tables)
    state, early = entering(both, parts[:2], side)
    mixed = local + mm(mix, state)
    normalized = mixed * lax.rsqrt(jnp.mean(mixed * mixed, -1, keepdims=True) + 1e-06) * head_gain
    gated = (normalized * jax.nn.silu(out_gate.astype(jnp.float32))).astype(jnp.bfloat16)
    expert_count = lax.axis_size(SP) * expert_gate.shape[0]
    rows = length // split_count
    first = lax.axis_index("tp") * rows
    product = jnp.dot(gated, out_weight, preferred_element_type=jnp.float32).astype(jnp.bfloat16)
    product, late = lax.optimization_barrier((product, parts[2:]))
    late = spread(late, side, 2)
    product = lax.all_to_all(in_blocks(product, 0, split_count), "tp", 0, 0, tiled=True)
    projected = jnp.sum(product.astype(jnp.float32), axis=0)
    residual = lax.optimization_barrier(lax.dynamic_slice_in_dim(residual_in, first, rows, 0))
    routes = lax.dynamic_slice_in_dim(expert_index, first, rows, 0)
    weights = lax.dynamic_slice_in_dim(route_weights, first, rows, 0)
    hidden_in = layer_norm(
        residual_scale * residual.astype(jnp.float32) + projected, norm_gain
    ).astype(jnp.bfloat16)
    chips = lax.axis_size(Z)
    table = (routes[:, :, None] == jnp.arange(expert_count, dtype=jnp.int32)).astype(jnp.bfloat16)
    send = jnp.einsum(
        "rs,rd->sd", jnp.sum(table, 1), hidden_in, preferred_element_type=jnp.float32
    ).astype(jnp.bfloat16)

    def along_z(x):
        out = lax.all_to_all(x.reshape(chips, 2, width), Z, 0, 0, tiled=True)
        return out.reshape(chips, 2, width)

    def in_plane(x):
        return lax.all_to_all(x, PLANE, 0, 0, tiled=True)

    half = chips // 2
    arrived = lax.all_to_all(send.reshape(chips, 16, width // 8), Z, 0, 0, tiled=True)
    arrived = arrived.reshape(chips, 2, width).transpose(1, 0, 2).reshape(2, 2, half, width)
    swapped = arrived[:, ::-1]
    turns = jnp.stack([arrived, swapped], 1)[:, None, :, None]
    turns = jnp.broadcast_to(turns, (2, side // 2, 2, side // 2, 2, half, width))
    piece = in_plane(turns.reshape(2 * split_count, half, width)).reshape(-1, width)
    tables += tuple(early + late)
    partial_value = pl.pallas_call(
        run_experts,
        out_shape=pltpu.VMEM(piece.shape, jnp.bfloat16),
        in_specs=[vmem] + [anywhere] * 7,
        out_specs=vmem,
        scratch_shapes=[pltpu.VMEM(x.shape, x.dtype) for x in tables]
        + [pltpu.SemaphoreType.DMA((7,))],
        name="run_experts",
    )(held(piece), *tables)
    shares = in_plane(partial_value.reshape(2 * split_count, half, width))
    shares = shares.reshape(2, side // 2, 2, side // 2, 2, half, width).astype(jnp.float32)
    shares = jnp.sum(shares, axis=(1, 3))
    result = jnp.stack([shares[:, 0, 0] + shares[:, 1, 1], shares[:, 0, 1] + shares[:, 1, 0]], 1)
    result = result.reshape(2, chips, width).astype(jnp.bfloat16)
    back = along_z(result.transpose(1, 0, 2)).reshape(expert_count, width)
    gathered = jnp.einsum("rks,sd->rkd", table, back, preferred_element_type=jnp.float32)
    routed = jnp.sum(weights[..., None] * gathered, 1)
    layer_out = layer_norm(
        residual_scale * hidden_in.astype(jnp.float32) + routed, final_gain
    ).astype(jnp.bfloat16)
    layer_out = collect(layer_out, "tp", 0)
    return layer_out


def solution(mesh):
    split = Mesh(
        mesh.devices.reshape(8, 2, 2, mesh.shape["tp"]), ("zh", "zl", "c", "tp")
    )
    placed = (
        P(SP, None),
        P(SP, "tp"),
        P(SP, "tp"),
        P(SP, "tp"),
        P(SP, "tp"),
        P("tp", SP),
        P("tp", SP),
        P("tp"),
        P(),
        P("tp", None),
        P(),
        P(),
        P(SP, None),
        P(SP, None),
        P(SP, None, "tp"),
        P(SP, None, "tp"),
        P(SP, "tp", None),
    )

    return jax.shard_map(per_device, mesh=split, in_specs=placed, out_specs=P(SP, None), check_vma=False)
```

```python
import jax
import jax.numpy as jnp
from jax import lax
from jax.experimental import pallas as pl
from jax.experimental.pallas import tpu as pltpu
from jax.sharding import Mesh
from jax.sharding import PartitionSpec as P


HEAD_FEATURES = 128
LANES = 128
Z = ("zh", "zl")
SP = ("zh", "zl", "c")
PLANE = ("c", "tp")


highest_precision = lax.Precision.HIGHEST
residual_scale = 2.0**0.5


def held(x):
    return pltpu.with_memory_space_constraint(x, pltpu.VMEM)


def mm(a, b):
    return jnp.dot(a, b, precision=highest_precision)


def regroup(lanes):
    row = lax.broadcasted_iota(jnp.int32, (16 * lanes, 16 * lanes), 0)
    col = lax.broadcasted_iota(jnp.int32, (16 * lanes, 16 * lanes), 1)
    row_kind, row_part = (row // (4 * lanes), row // lanes % 4)
    col_part, col_kind = (col // (4 * lanes), col // lanes % 4)
    same = (row_kind == col_kind) & (row_part == col_part) & (row % lanes == col % lanes)
    return jnp.where(same, 1.0, 0.0).astype(jnp.bfloat16)


def pack_parts(gate_ref, up_ref, down_ref, bufs, outs, sems):
    depth, hidden = gate_ref.shape
    half, lanes, blocks = (depth // 2, LANES // 4, hidden // LANES)
    size = bufs[0].shape[0] // blocks
    copies = []
    for part, buf in enumerate(bufs):
        for block in range(blocks):
            first = block * LANES + part * lanes
            for k in range(depth // LANES):
                row = block * size + half + k * lanes
                buf[row : row + lanes] = down_ref[first : first + lanes, k * LANES : (k + 1) * LANES]
    order = regroup(lanes)
    for block in range(blocks):
        cut = slice(block * LANES, (block + 1) * LANES)
        kinds = [ref[k : k + half, cut] for ref in (gate_ref, up_ref) for k in (0, half)]
        parts = jnp.dot(jnp.concatenate(kinds, 1), order, preferred_element_type=jnp.float32)
        parts = parts.astype(jnp.bfloat16)
        for part, buf in enumerate(bufs):
            row = block * size
            buf[row : row + half] = parts[:, part * LANES : (part + 1) * LANES]
            run = pl.ds(row, size)
            copies.append(pltpu.make_async_copy(buf.at[run], outs[part].at[run], sems.at[len(copies)]))
            copies[-1].start()
    for copy in copies:
        copy.wait()


def pack_experts(*refs):
    tables, outs, bufs, part_bufs, sems = refs[:3], refs[3:7], refs[7:10], refs[10:14], refs[14]
    copies = [pltpu.make_async_copy(x, y, sems.at[k]) for k, (x, y) in enumerate(zip(tables, bufs))]
    for copy in copies:
        copy.start()
    for copy in copies:
        copy.wait()
    pack_parts(*bufs, part_bufs, outs, sems.at[3:])


def packed_parts(tables):
    packed = (3 * tables[0].size // 4 // LANES, LANES)
    anywhere = pl.BlockSpec(memory_space=pl.ANY)
    return pl.pallas_call(
        pack_experts,
        out_shape=(jax.ShapeDtypeStruct(packed, jnp.bfloat16),) * 4,
        in_specs=[anywhere] * 3,
        out_specs=(anywhere,) * 4,
        scratch_shapes=[pltpu.VMEM(x.shape, x.dtype) for x in tables]
        + [pltpu.VMEM(packed, jnp.bfloat16)] * 4
        + [pltpu.SemaphoreType.DMA((15,))],
        name="pack_experts",
    )(*tables)


def spread(parts, side, start=0):
    out = []
    ways = ((0, 1), (0, side - 1), (1, 0), (side - 1, 0))
    for part, (dy, dx) in zip(parts, ways[start:]):
        pairs = [
            (y * side + x, (y + dy) % side * side + (x + dx) % side)
            for y in range(side)
            for x in range(side)
        ]
        out.append(lax.ppermute(part, "tp", pairs))
    return out


def entering(own, tables, side):
    kind = jnp.bfloat16
    zh, zl, c = (lax.axis_index(axis) for axis in SP)
    near = lax.all_gather(own, ("zl", "c")).astype(jnp.float32)
    width = own.shape[-1]
    map_in, state_in = (jnp.eye(width, dtype=jnp.float32), jnp.zeros((width, width), jnp.float32))
    map_all, state_all = (near[0, :width], near[0, width:])
    for k in range(1, 4):
        inside = k == 2 * zl + c
        map_in = jnp.where(inside, map_all, map_in)
        state_in = jnp.where(inside, state_all, state_in)
        map_k, state_k = (near[k, :width], near[k, width:])
        state_all = mm(map_k, state_all) + state_k
        map_all = mm(map_k, map_all)
    group = jnp.concatenate([map_all, state_all], 0).astype(kind)
    quarter = lax.dynamic_slice_in_dim(group, (2 * zl + c) * (width // 2), width // 2, 0)
    count = lax.axis_size(Z)
    quarter, tables = lax.optimization_barrier((quarter, tables))
    parts = packed_parts(tables)
    early = spread(parts[:1], side)
    far = jnp.broadcast_to(quarter[None], (count, *quarter.shape))
    far = lax.all_to_all(far, Z, 0, 0, tiled=True)
    far = lax.all_gather(far, "c")
    far = far.reshape(2, count // 2, 2, width // 2, width).transpose(1, 2, 0, 3, 4)
    far = far.reshape(count // 2, 2 * width, width).astype(jnp.float32)
    state = jnp.zeros((width, width), jnp.float32)
    for k in range(count // 2 - 1):
        state = jnp.where(k < zh, mm(far[k, :width], state) + far[k, width:], state)
    return mm(map_in, state) + state_in, early, parts[1:]


def in_blocks(x, dim, length):
    shape = x.shape
    blocks = x.reshape(*shape[:dim], length, shape[dim] // length, *shape[dim + 1 :])
    return jnp.moveaxis(blocks, dim, 0)


def copy_for_each(x, axis):
    length = lax.axis_size(axis)
    return lax.all_to_all(jnp.broadcast_to(x[None], (length, *x.shape)), axis, 0, 0, tiled=True)


def in_order(blocks, dim):
    shape = list(blocks.shape[1:])
    shape[dim] *= blocks.shape[0]
    return jnp.moveaxis(blocks, 0, dim).reshape(shape)


def collect(x, axis, dim):
    blocks = copy_for_each(x, axis)
    return in_order(blocks, dim)


def layer_norm(data, gain):
    center = data - jnp.mean(data, -1, keepdims=True)
    return center * lax.rsqrt(jnp.mean(center * center, -1, keepdims=True) + 1e-05) * gain


def local_span(q_ref, k_ref, v_ref, beta_ref, decay_ref, rate_ref, both_ref, mix_ref, out_ref):
    size = HEAD_FEATURES
    row = lax.broadcasted_iota(jnp.int32, (size, size), 0)
    col = lax.broadcasted_iota(jnp.int32, (size, size), 1)
    eye = row == col
    causal = col <= row

    def to_column(data):
        return jnp.sum(jnp.where(eye, data, 0.0), 1, keepdims=True)

    def to_row(data):
        return jnp.sum(jnp.where(eye, data, 0.0), 0, keepdims=True)

    def dot(a, b, dims=((1,), (0,))):
        return lax.dot_general(
            a.astype(jnp.bfloat16),
            b.astype(jnp.bfloat16),
            (dims, ((), ())),
            preferred_element_type=jnp.float32,
        )

    beta = to_column(jax.nn.sigmoid(beta_ref[...].astype(jnp.float32)))
    logit = decay_ref[...].astype(jnp.float32)
    softplus = jnp.maximum(logit, 0.0) + jnp.log(1.0 + jnp.exp(-jnp.abs(logit)))
    decay = -jnp.exp(jnp.full((1, size), rate_ref[0], jnp.float32)) * softplus
    running = jnp.sum(jnp.where(causal, decay, 0.0), 1, keepdims=True)
    last = jnp.sum(decay, 1, keepdims=True)
    within = jnp.exp(jnp.where(causal, running - to_row(running), -1e30))
    query = q_ref[...].astype(jnp.float32)
    key = k_ref[...].astype(jnp.float32)
    value = v_ref[...].astype(jnp.float32)
    query_scale = lax.rsqrt(jnp.sum(query * query, 1, keepdims=True) + 1e-06) * size ** (-0.5)
    key_scale = lax.rsqrt(jnp.sum(key * key, 1, keepdims=True) + 1e-06)
    key_scale_row = to_row(key_scale)
    across = within * key_scale_row
    lower = jnp.where(
        col < row, dot(k_ref[...], k_ref[...], ((1,), (1,))) * across * (beta * key_scale), 0.0
    )
    scores = dot(q_ref[...], k_ref[...], ((1,), (1,))) * across * query_scale
    differ = row ^ col
    inverse = jnp.where(eye, 1.0, 0.0) - jnp.where(differ == 1, lower, 0.0)
    for level in range(1, 7):
        part = jnp.where((differ >> level) == 1, lower, 0.0)
        inverse = inverse - dot(dot(inverse, part), inverse)
    grown = jnp.exp(running)
    key = key * key_scale
    right = jnp.concatenate([key * (beta * grown), value * beta], 1)
    solved = dot(inverse, right)
    leaving = dot(key * jnp.exp(last - running), solved, ((0,), (0,)))
    passed = jnp.where(eye, jnp.exp(last), 0.0) - leaving[:, :size]
    both_ref[...] = jnp.concatenate([passed, leaving[:, size:]], 0).astype(both_ref.dtype)
    seen = dot(scores, solved)
    mix_ref[...] = query * (query_scale * grown) - seen[:, :size]
    out_ref[...] = seen[:, size:]


def run_experts(rows_ref, *refs):
    out_ref, bufs, sems = refs[7], refs[8:15], refs[15]
    copies = [pltpu.make_async_copy(refs[k], bufs[k], sems.at[k]) for k in range(7)]
    for copy in (*copies[:2], *copies[3:], copies[2]):
        copy.start()
    gate_ref, up_ref, down_ref = bufs[:3]
    rows = rows_ref[...]
    width = rows.shape[1]
    half, lanes, blocks = (width // 2, LANES // 4, down_ref.shape[0] // LANES)
    size = bufs[3].shape[0] // blocks

    def dot(a, b):
        return jnp.dot(a, b, preferred_element_type=jnp.float32)

    copies[0].wait()
    gate = dot(rows, gate_ref[...])
    copies[1].wait()
    inner = (jax.nn.silu(gate) * dot(rows, up_ref[...])).astype(jnp.bfloat16)
    place = lax.broadcasted_iota(jnp.int32, (rows.shape[0], LANES), 1) // lanes
    arrived = [jnp.zeros((rows.shape[0], LANES), jnp.float32)] * blocks

    def run(part, block, first, count):
        row = block * size + first
        return bufs[3 + part][row : row + count]

    for part in range(4):
        copies[3 + part].wait()
        table = jnp.concatenate([run(part, k, 0, half) for k in range(blocks)], 1)
        low, high = (dot(rows[:, :half], table), dot(rows[:, half:], table))
        for k in range(blocks):
            cut = slice(k * LANES, (k + 1) * LANES)
            sums = low[:, cut] + pltpu.roll(high[:, cut], LANES - lanes, 1)
            acts = jax.nn.silu(sums) * pltpu.roll(sums, LANES - 2 * lanes, 1)
            if part > 0:
                acts = pltpu.roll(acts, part * lanes, 1)
            arrived[k] = jnp.where(place == part, acts, arrived[k])
    arrived = jnp.concatenate(arrived, 1).astype(jnp.bfloat16)
    copies[2].wait()

    def down_block(k):
        first = half + k * lanes
        runs = [run(part, block, first, lanes) for block in range(blocks) for part in range(4)]
        return jnp.concatenate(runs, 0)

    for k in range(0, width // LANES, 2):
        cut = slice(k * LANES, (k + 2) * LANES)
        other = jnp.concatenate([down_block(k), down_block(k + 1)], 1)
        out_ref[:, cut] = (dot(inner, down_ref[:, cut]) + dot(arrived, other)).astype(out_ref.dtype)


def per_device(
    residual_in,
    queries,
    keys,
    values,
    out_gate,
    beta_logit,
    decay_logit,
    decay_log,
    head_gain,
    out_weight,
    norm_gain,
    final_gain,
    expert_index,
    route_weights,
    expert_gate,
    expert_up,
    expert_down,
):
    length, width = residual_in.shape

    vmem = pl.BlockSpec(memory_space=pltpu.VMEM)
    anywhere = pl.BlockSpec(memory_space=pl.ANY)
    split_count = lax.axis_size("tp")
    side = round(split_count**0.5)
    tables = (expert_gate[0], expert_up[0], expert_down[0])
    both, mix, local = pl.pallas_call(
        local_span,
        out_shape=(
            pltpu.VMEM((2 * HEAD_FEATURES, HEAD_FEATURES), jnp.bfloat16),
            pltpu.VMEM((length, HEAD_FEATURES), jnp.float32),
            pltpu.VMEM((length, HEAD_FEATURES), jnp.float32),
        ),
        in_specs=[vmem] * 5 + [pl.BlockSpec(memory_space=pltpu.SMEM)],
        out_specs=(vmem,) * 3,
        name="local_span",
    )(queries, keys, values, beta_logit, decay_logit, decay_log)
    state, early, late = entering(both, tables, side)
    mixed = local + mm(mix, state)
    normalized = mixed * lax.rsqrt(jnp.mean(mixed * mixed, -1, keepdims=True) + 1e-06) * head_gain
    gated = (normalized * jax.nn.silu(out_gate.astype(jnp.float32))).astype(jnp.bfloat16)
    expert_count = lax.axis_size(SP) * expert_gate.shape[0]
    rows = length // split_count
    first = lax.axis_index("tp") * rows
    product = jnp.dot(gated, out_weight, preferred_element_type=jnp.float32).astype(jnp.bfloat16)
    product, late = lax.optimization_barrier((product, late))
    late = spread(late, side, 1)
    product = lax.all_to_all(in_blocks(product, 0, split_count), "tp", 0, 0, tiled=True)
    projected = jnp.sum(product.astype(jnp.float32), axis=0)
    residual = lax.optimization_barrier(lax.dynamic_slice_in_dim(residual_in, first, rows, 0))
    routes = lax.dynamic_slice_in_dim(expert_index, first, rows, 0)
    weights = lax.dynamic_slice_in_dim(route_weights, first, rows, 0)
    hidden_in = layer_norm(
        residual_scale * residual.astype(jnp.float32) + projected, norm_gain
    ).astype(jnp.bfloat16)
    chips = lax.axis_size(Z)
    table = (routes[:, :, None] == jnp.arange(expert_count, dtype=jnp.int32)).astype(jnp.bfloat16)
    send = jnp.einsum(
        "rs,rd->sd", jnp.sum(table, 1), hidden_in, preferred_element_type=jnp.float32
    ).astype(jnp.bfloat16)

    def along_z(x):
        out = lax.all_to_all(x.reshape(chips, 2, width), Z, 0, 0, tiled=True)
        return out.reshape(chips, 2, width)

    def in_plane(x):
        return lax.all_to_all(x, PLANE, 0, 0, tiled=True)

    half = chips // 2
    arrived = lax.all_to_all(send.reshape(chips, 16, width // 8), Z, 0, 0, tiled=True)
    arrived = arrived.reshape(chips, 2, width).transpose(1, 0, 2).reshape(2, 2, half, width)
    swapped = arrived[:, ::-1]
    turns = jnp.stack([arrived, swapped], 1)[:, None, :, None]
    turns = jnp.broadcast_to(turns, (2, side // 2, 2, side // 2, 2, half, width))
    piece = in_plane(turns.reshape(2 * split_count, half, width)).reshape(-1, width)
    tables += tuple(early + late)
    partial_value = pl.pallas_call(
        run_experts,
        out_shape=pltpu.VMEM(piece.shape, jnp.bfloat16),
        in_specs=[vmem] + [anywhere] * 7,
        out_specs=vmem,
        scratch_shapes=[pltpu.VMEM(x.shape, x.dtype) for x in tables]
        + [pltpu.SemaphoreType.DMA((7,))],
        name="run_experts",
    )(held(piece), *tables)
    shares = in_plane(partial_value.reshape(2 * split_count, half, width))
    shares = shares.reshape(2, side // 2, 2, side // 2, 2, half, width).astype(jnp.float32)
    shares = jnp.sum(shares, axis=(1, 3))
    result = jnp.stack([shares[:, 0, 0] + shares[:, 1, 1], shares[:, 0, 1] + shares[:, 1, 0]], 1)
    result = result.reshape(2, chips, width).astype(jnp.bfloat16)
    back = along_z(result.transpose(1, 0, 2)).reshape(expert_count, width)
    gathered = jnp.einsum("rks,sd->rkd", table, back, preferred_element_type=jnp.float32)
    routed = jnp.sum(weights[..., None] * gathered, 1)
    layer_out = layer_norm(
        residual_scale * hidden_in.astype(jnp.float32) + routed, final_gain
    ).astype(jnp.bfloat16)
    layer_out = collect(layer_out, "tp", 0)
    return layer_out


def solution(mesh):
    split = Mesh(
        mesh.devices.reshape(8, 2, 2, mesh.shape["tp"]), ("zh", "zl", "c", "tp")
    )
    placed = (
        P(SP, None),
        P(SP, "tp"),
        P(SP, "tp"),
        P(SP, "tp"),
        P(SP, "tp"),
        P("tp", SP),
        P("tp", SP),
        P("tp"),
        P(),
        P("tp", None),
        P(),
        P(),
        P(SP, None),
        P(SP, None),
        P(SP, None, "tp"),
        P(SP, None, "tp"),
        P(SP, "tp", None),
    )

    return jax.shard_map(per_device, mesh=split, in_specs=placed, out_specs=P(SP, None), check_vma=False)
```

```python
import jax
import jax.numpy as jnp
from jax import lax
from jax.experimental import pallas as pl
from jax.experimental.pallas import tpu as pltpu
from jax.sharding import Mesh
from jax.sharding import PartitionSpec as P


HEAD_FEATURES = 128
LANES = 128
Z = ("zh", "zl")
SP = ("zh", "zl", "c")
PLANE = ("c", "tp")


highest_precision = lax.Precision.HIGHEST
residual_scale = 2.0**0.5


def held(x):
    return pltpu.with_memory_space_constraint(x, pltpu.VMEM)


def mm(a, b):
    return jnp.dot(a, b, precision=highest_precision)


def regroup(lanes):
    row = lax.broadcasted_iota(jnp.int32, (16 * lanes, 16 * lanes), 0)
    col = lax.broadcasted_iota(jnp.int32, (16 * lanes, 16 * lanes), 1)
    row_kind, row_part = (row // (4 * lanes), row // lanes % 4)
    col_part, col_kind = (col // (4 * lanes), col // lanes % 4)
    same = (row_kind == col_kind) & (row_part == col_part) & (row % lanes == col % lanes)
    return jnp.where(same, 1.0, 0.0).astype(jnp.bfloat16)


def pack_parts(gate_ref, up_ref, down_ref, bufs, outs, sems):
    depth, hidden = gate_ref.shape
    half, lanes, blocks = (depth // 2, LANES // 4, hidden // LANES)
    size = bufs[0].shape[0] // blocks
    copies = []
    for part, buf in enumerate(bufs):
        for block in range(blocks):
            first = block * LANES + part * lanes
            for k in range(depth // LANES):
                row = block * size + half + k * lanes
                buf[row : row + lanes] = down_ref[first : first + lanes, k * LANES : (k + 1) * LANES]
    order = regroup(lanes)
    for block in range(blocks):
        cut = slice(block * LANES, (block + 1) * LANES)
        kinds = [ref[k : k + half, cut] for ref in (gate_ref, up_ref) for k in (0, half)]
        parts = jnp.dot(jnp.concatenate(kinds, 1), order, preferred_element_type=jnp.float32)
        parts = parts.astype(jnp.bfloat16)
        for part, buf in enumerate(bufs):
            row = block * size
            buf[row : row + half] = parts[:, part * LANES : (part + 1) * LANES]
            run = pl.ds(row, size)
            copies.append(pltpu.make_async_copy(buf.at[run], outs[part].at[run], sems.at[len(copies)]))
            copies[-1].start()
    for copy in copies:
        copy.wait()


def pack_experts(*refs):
    tables, outs, bufs, part_bufs, sems = refs[:3], refs[3:7], refs[7:10], refs[10:14], refs[14]
    copies = [pltpu.make_async_copy(x, y, sems.at[k]) for k, (x, y) in enumerate(zip(tables, bufs))]
    for copy in copies:
        copy.start()
    for copy in copies:
        copy.wait()
    pack_parts(*bufs, part_bufs, outs, sems.at[3:])


def packed_parts(tables):
    packed = (3 * tables[0].size // 4 // LANES, LANES)
    anywhere = pl.BlockSpec(memory_space=pl.ANY)
    return pl.pallas_call(
        pack_experts,
        out_shape=(jax.ShapeDtypeStruct(packed, jnp.bfloat16),) * 4,
        in_specs=[anywhere] * 3,
        out_specs=(anywhere,) * 4,
        scratch_shapes=[pltpu.VMEM(x.shape, x.dtype) for x in tables]
        + [pltpu.VMEM(packed, jnp.bfloat16)] * 4
        + [pltpu.SemaphoreType.DMA((15,))],
        name="pack_experts",
    )(*tables)


def spread(parts, side, start=0):
    out = []
    ways = ((0, 1), (0, side - 1), (1, 0), (side - 1, 0))
    for part, (dy, dx) in zip(parts, ways[start:]):
        pairs = [
            (y * side + x, (y + dy) % side * side + (x + dx) % side)
            for y in range(side)
            for x in range(side)
        ]
        out.append(lax.ppermute(part, "tp", pairs))
    return out


def entering(own, tables, side):
    kind = jnp.bfloat16
    zh, zl, c = (lax.axis_index(axis) for axis in SP)
    near = lax.all_gather(own, ("zl", "c")).astype(jnp.float32)
    width = own.shape[-1]
    map_in, state_in = (jnp.eye(width, dtype=jnp.float32), jnp.zeros((width, width), jnp.float32))
    map_all, state_all = (near[0, :width], near[0, width:])
    for k in range(1, 4):
        inside = k == 2 * zl + c
        map_in = jnp.where(inside, map_all, map_in)
        state_in = jnp.where(inside, state_all, state_in)
        map_k, state_k = (near[k, :width], near[k, width:])
        state_all = mm(map_k, state_all) + state_k
        map_all = mm(map_k, map_all)
    group = jnp.concatenate([map_all, state_all], 0).astype(kind)
    quarter = lax.dynamic_slice_in_dim(group, (2 * zl + c) * (width // 2), width // 2, 0)
    count = lax.axis_size(Z)
    quarter, tables = lax.optimization_barrier((quarter, tables))
    parts = packed_parts(tables)
    early = spread(parts[:2], side)
    far = jnp.broadcast_to(quarter[None], (count, *quarter.shape))
    far = lax.all_to_all(far, Z, 0, 0, tiled=True)
    far = lax.all_gather(far, "c")
    far = far.reshape(2, count // 2, 2, width // 2, width).transpose(1, 2, 0, 3, 4)
    far = far.reshape(count // 2, 2 * width, width).astype(jnp.float32)
    state = jnp.zeros((width, width), jnp.float32)
    for k in range(count // 2 - 1):
        state = jnp.where(k < zh, mm(far[k, :width], state) + far[k, width:], state)
    return mm(map_in, state) + state_in, early, parts[2:]


def in_blocks(x, dim, length):
    shape = x.shape
    blocks = x.reshape(*shape[:dim], length, shape[dim] // length, *shape[dim + 1 :])
    return jnp.moveaxis(blocks, dim, 0)


def copy_for_each(x, axis):
    length = lax.axis_size(axis)
    return lax.all_to_all(jnp.broadcast_to(x[None], (length, *x.shape)), axis, 0, 0, tiled=True)


def in_order(blocks, dim):
    shape = list(blocks.shape[1:])
    shape[dim] *= blocks.shape[0]
    return jnp.moveaxis(blocks, 0, dim).reshape(shape)


def collect(x, axis, dim):
    blocks = copy_for_each(x, axis)
    return in_order(blocks, dim)


def layer_norm(data, gain):
    center = data - jnp.mean(data, -1, keepdims=True)
    return center * lax.rsqrt(jnp.mean(center * center, -1, keepdims=True) + 1e-05) * gain


def local_span(q_ref, k_ref, v_ref, beta_ref, decay_ref, rate_ref, both_ref, mix_ref, out_ref):
    size = HEAD_FEATURES
    row = lax.broadcasted_iota(jnp.int32, (size, size), 0)
    col = lax.broadcasted_iota(jnp.int32, (size, size), 1)
    eye = row == col
    causal = col <= row

    def to_column(data):
        return jnp.sum(jnp.where(eye, data, 0.0), 1, keepdims=True)

    def to_row(data):
        return jnp.sum(jnp.where(eye, data, 0.0), 0, keepdims=True)

    def dot(a, b, dims=((1,), (0,))):
        return lax.dot_general(
            a.astype(jnp.bfloat16),
            b.astype(jnp.bfloat16),
            (dims, ((), ())),
            preferred_element_type=jnp.float32,
        )

    beta = to_column(jax.nn.sigmoid(beta_ref[...].astype(jnp.float32)))
    logit = decay_ref[...].astype(jnp.float32)
    softplus = jnp.maximum(logit, 0.0) + jnp.log(1.0 + jnp.exp(-jnp.abs(logit)))
    decay = -jnp.exp(jnp.full((1, size), rate_ref[0], jnp.float32)) * softplus
    running = jnp.sum(jnp.where(causal, decay, 0.0), 1, keepdims=True)
    last = jnp.sum(decay, 1, keepdims=True)
    within = jnp.exp(jnp.where(causal, running - to_row(running), -1e30))
    query = q_ref[...].astype(jnp.float32)
    key = k_ref[...].astype(jnp.float32)
    value = v_ref[...].astype(jnp.float32)
    query_scale = lax.rsqrt(jnp.sum(query * query, 1, keepdims=True) + 1e-06) * size ** (-0.5)
    key_scale = lax.rsqrt(jnp.sum(key * key, 1, keepdims=True) + 1e-06)
    key_scale_row = to_row(key_scale)
    across = within * key_scale_row
    lower = jnp.where(
        col < row, dot(k_ref[...], k_ref[...], ((1,), (1,))) * across * (beta * key_scale), 0.0
    )
    scores = dot(q_ref[...], k_ref[...], ((1,), (1,))) * across * query_scale
    differ = row ^ col
    inverse = jnp.where(eye, 1.0, 0.0) - jnp.where(differ == 1, lower, 0.0)
    for level in range(1, 7):
        part = jnp.where((differ >> level) == 1, lower, 0.0)
        inverse = inverse - dot(dot(inverse, part), inverse)
    grown = jnp.exp(running)
    key = key * key_scale
    right = jnp.concatenate([key * (beta * grown), value * beta], 1)
    solved = dot(inverse, right)
    leaving = dot(key * jnp.exp(last - running), solved, ((0,), (0,)))
    passed = jnp.where(eye, jnp.exp(last), 0.0) - leaving[:, :size]
    both_ref[...] = jnp.concatenate([passed, leaving[:, size:]], 0).astype(both_ref.dtype)
    seen = dot(scores, solved)
    mix_ref[...] = query * (query_scale * grown) - seen[:, :size]
    out_ref[...] = seen[:, size:]


def run_experts(rows_ref, *refs):
    out_ref, bufs, sems = refs[7], refs[8:15], refs[15]
    copies = [pltpu.make_async_copy(refs[k], bufs[k], sems.at[k]) for k in range(7)]
    for copy in (*copies[:2], *copies[3:], copies[2]):
        copy.start()
    gate_ref, up_ref, down_ref = bufs[:3]
    rows = rows_ref[...]
    width = rows.shape[1]
    half, lanes, blocks = (width // 2, LANES // 4, down_ref.shape[0] // LANES)
    size = bufs[3].shape[0] // blocks

    def dot(a, b):
        return jnp.dot(a, b, preferred_element_type=jnp.float32)

    copies[0].wait()
    gate = dot(rows, gate_ref[...])
    copies[1].wait()
    inner = (jax.nn.silu(gate) * dot(rows, up_ref[...])).astype(jnp.bfloat16)
    place = lax.broadcasted_iota(jnp.int32, (rows.shape[0], LANES), 1) // lanes
    arrived = [jnp.zeros((rows.shape[0], LANES), jnp.float32)] * blocks

    def run(part, block, first, count):
        row = block * size + first
        return bufs[3 + part][row : row + count]

    for part in range(4):
        copies[3 + part].wait()
        table = jnp.concatenate([run(part, k, 0, half) for k in range(blocks)], 1)
        low, high = (dot(rows[:, :half], table), dot(rows[:, half:], table))
        for k in range(blocks):
            cut = slice(k * LANES, (k + 1) * LANES)
            sums = low[:, cut] + pltpu.roll(high[:, cut], LANES - lanes, 1)
            acts = jax.nn.silu(sums) * pltpu.roll(sums, LANES - 2 * lanes, 1)
            if part > 0:
                acts = pltpu.roll(acts, part * lanes, 1)
            arrived[k] = jnp.where(place == part, acts, arrived[k])
    arrived = jnp.concatenate(arrived, 1).astype(jnp.bfloat16)
    copies[2].wait()

    def down_block(k):
        first = half + k * lanes
        runs = [run(part, block, first, lanes) for block in range(blocks) for part in range(4)]
        return jnp.concatenate(runs, 0)

    for k in range(0, width // LANES, 2):
        cut = slice(k * LANES, (k + 2) * LANES)
        other = jnp.concatenate([down_block(k), down_block(k + 1)], 1)
        out_ref[:, cut] = (dot(inner, down_ref[:, cut]) + dot(arrived, other)).astype(out_ref.dtype)


def per_device(
    residual_in,
    queries,
    keys,
    values,
    out_gate,
    beta_logit,
    decay_logit,
    decay_log,
    head_gain,
    out_weight,
    norm_gain,
    final_gain,
    expert_index,
    route_weights,
    expert_gate,
    expert_up,
    expert_down,
):
    length, width = residual_in.shape

    vmem = pl.BlockSpec(memory_space=pltpu.VMEM)
    anywhere = pl.BlockSpec(memory_space=pl.ANY)
    split_count = lax.axis_size("tp")
    side = round(split_count**0.5)
    tables = (expert_gate[0], expert_up[0], expert_down[0])
    both, mix, local = pl.pallas_call(
        local_span,
        out_shape=(
            pltpu.VMEM((2 * HEAD_FEATURES, HEAD_FEATURES), jnp.bfloat16),
            pltpu.VMEM((length, HEAD_FEATURES), jnp.float32),
            pltpu.VMEM((length, HEAD_FEATURES), jnp.float32),
        ),
        in_specs=[vmem] * 5 + [pl.BlockSpec(memory_space=pltpu.SMEM)],
        out_specs=(vmem,) * 3,
        name="local_span",
    )(queries, keys, values, beta_logit, decay_logit, decay_log)
    state, early, late = entering(both, tables, side)
    mixed = local + mm(mix, state)
    normalized = mixed * lax.rsqrt(jnp.mean(mixed * mixed, -1, keepdims=True) + 1e-06) * head_gain
    gated = (normalized * jax.nn.silu(out_gate.astype(jnp.float32))).astype(jnp.bfloat16)
    expert_count = lax.axis_size(SP) * expert_gate.shape[0]
    rows = length // split_count
    first = lax.axis_index("tp") * rows
    product = jnp.dot(gated, out_weight, preferred_element_type=jnp.float32).astype(jnp.bfloat16)
    product, late = lax.optimization_barrier((product, late))
    late = spread(late, side, 2)
    product = lax.all_to_all(in_blocks(product, 0, split_count), "tp", 0, 0, tiled=True)
    projected = jnp.sum(product.astype(jnp.float32), axis=0)
    residual = lax.optimization_barrier(lax.dynamic_slice_in_dim(residual_in, first, rows, 0))
    routes = lax.dynamic_slice_in_dim(expert_index, first, rows, 0)
    weights = lax.dynamic_slice_in_dim(route_weights, first, rows, 0)
    hidden_in = layer_norm(
        residual_scale * residual.astype(jnp.float32) + projected, norm_gain
    ).astype(jnp.bfloat16)
    chips = lax.axis_size(Z)
    table = (routes[:, :, None] == jnp.arange(expert_count, dtype=jnp.int32)).astype(jnp.bfloat16)
    send = jnp.einsum(
        "rs,rd->sd", jnp.sum(table, 1), hidden_in, preferred_element_type=jnp.float32
    ).astype(jnp.bfloat16)

    def along_z(x):
        out = lax.all_to_all(x.reshape(chips, 2, width), Z, 0, 0, tiled=True)
        return out.reshape(chips, 2, width)

    def in_plane(x):
        return lax.all_to_all(x, PLANE, 0, 0, tiled=True)

    half = chips // 2
    arrived = lax.all_to_all(send.reshape(chips, 16, width // 8), Z, 0, 0, tiled=True)
    arrived = arrived.reshape(chips, 2, width).transpose(1, 0, 2).reshape(2, 2, half, width)
    swapped = arrived[:, ::-1]
    turns = jnp.stack([arrived, swapped], 1)[:, None, :, None]
    turns = jnp.broadcast_to(turns, (2, side // 2, 2, side // 2, 2, half, width))
    piece = in_plane(turns.reshape(2 * split_count, half, width)).reshape(-1, width)
    tables += tuple(early + late)
    partial_value = pl.pallas_call(
        run_experts,
        out_shape=pltpu.VMEM(piece.shape, jnp.bfloat16),
        in_specs=[vmem] + [anywhere] * 7,
        out_specs=vmem,
        scratch_shapes=[pltpu.VMEM(x.shape, x.dtype) for x in tables]
        + [pltpu.SemaphoreType.DMA((7,))],
        name="run_experts",
    )(held(piece), *tables)
    shares = in_plane(partial_value.reshape(2 * split_count, half, width))
    shares = shares.reshape(2, side // 2, 2, side // 2, 2, half, width).astype(jnp.float32)
    shares = jnp.sum(shares, axis=(1, 3))
    result = jnp.stack([shares[:, 0, 0] + shares[:, 1, 1], shares[:, 0, 1] + shares[:, 1, 0]], 1)
    result = result.reshape(2, chips, width).astype(jnp.bfloat16)
    back = along_z(result.transpose(1, 0, 2)).reshape(expert_count, width)
    gathered = jnp.einsum("rks,sd->rkd", table, back, preferred_element_type=jnp.float32)
    routed = jnp.sum(weights[..., None] * gathered, 1)
    layer_out = layer_norm(
        residual_scale * hidden_in.astype(jnp.float32) + routed, final_gain
    ).astype(jnp.bfloat16)
    layer_out = collect(layer_out, "tp", 0)
    return layer_out


def solution(mesh):
    split = Mesh(
        mesh.devices.reshape(8, 2, 2, mesh.shape["tp"]), ("zh", "zl", "c", "tp")
    )
    placed = (
        P(SP, None),
        P(SP, "tp"),
        P(SP, "tp"),
        P(SP, "tp"),
        P(SP, "tp"),
        P("tp", SP),
        P("tp", SP),
        P("tp"),
        P(),
        P("tp", None),
        P(),
        P(),
        P(SP, None),
        P(SP, None),
        P(SP, None, "tp"),
        P(SP, None, "tp"),
        P(SP, "tp", None),
    )

    return jax.shard_map(per_device, mesh=split, in_specs=placed, out_specs=P(SP, None), check_vma=False)
```
